256 devices in a mesh: grp: 2 (over y), st: 32 (over z, core), tp: 4 (over x).
Axes of the slice: x: 4, y: 2, z: 16, core: 2. Of those that a mesh axis runs over, the one named last changes fastest.
The devices are a block of a 4x16x16 slice.
Arguments:
- tokens: bfloat16 [32768, 2048], P(('grp', 'st')), parts along dimension 0, may hold values from -6 to 6
- owners: int32 [512, 4], P(('grp', 'st')), parts along dimension 0, may hold values from 0 to 31, all different within a row; in each aligned block of 8 rows (0 to 7, 8 to 15, ...) at most 2 rows name the same one
- entries: int32 [512, 4], P(('grp', 'st')), parts along dimension 0, may hold values from 0 to 15
- store: bfloat16 [1024, 64, 2048], P(('grp', 'st')), parts along dimension 0, may hold values from -600 to 600
- mixer_query_weight: bfloat16 [2048, 1024], P(None, 'tp'), may hold values from -0.125 to 0.125
- mixer_key_weight: bfloat16 [2048, 1024], P(None, 'tp'), may hold values from -0.125 to 0.125
- mixer_value_weight: bfloat16 [2048, 1024], P(None, 'tp'), may hold values from -0.125 to 0.125
- strength_weight: bfloat16 [2048, 8], P(None, 'tp'), may hold values from -0.125 to 0.125
- decay_weight: bfloat16 [2048, 8], P(None, 'tp'), may hold values from -0.125 to 0.125
- head_decay_rate: float32 [8], P('tp'), may hold values from 0.003 to 0.15
- extra_forgetting_exponent: float32 [32768, 8], P(('grp', 'st'), 'tp'), parts along dimension 0, may hold values from -0.7 to 0
- output_norm_gain: float32 [128], replicated, may hold values from 0.1 to 1.9
- retrieval_query_weight: bfloat16 [2048, 1024], P(None, 'tp'), may hold values from -0.125 to 0.125
- passage_key_weight: bfloat16 [2048, 1024], P(None, 'tp'), may hold values from -0.125 to 0.125
- passage_value_weight: bfloat16 [2048, 1024], P(None, 'tp'), may hold values from -0.125 to 0.125
- retrieval_gate_weight: bfloat16 [2048, 8], P(None, 'tp'), may hold values from -0.125 to 0.125
Outputs:
- mixed: bfloat16 [32768, 1024], P(('grp', 'st'), 'tp'), parts along dimension 0
The draws below stay inside these ranges and needn't reach their ends.
There are 2 independent parts, one for each index of `grp`. The reference program is written for one: setup_inputs(seed, part) draws one part's arguments, and reference() takes and returns one part's arrays. A program takes and returns all parts, laid end to end along the dimension named above; an argument that names none is the same for every part. Nothing has to cross between parts.
Inputs may be any that keep to these rules, and one draw needn't show every extreme that they name: `owners`: each row names 4 different values; the rows of one device name no value more than 2 times, a bound that some device reaches; every value is named by some row.
All inputs are finite; a program needn't handle non-finite values.
Results may differ from the reference program's by a relative error of at most 0.015.
The reference program's roundings to bfloat16 on the way count: a program that leaves them out, or rounds other values in their place, can miss the bound.
Values may be sent and summed in bfloat16 or wider, within the bound.
No kernel may reach another device: no remote copies, remote signals or barrier semaphores. Data moves between devices by JAX's collectives and lax.ppermute only.
A program may use at most 128 MiB of HBM per device.

```python
import math
import jax
import jax.numpy as jnp
import numpy as np
from jax import lax

D = 2048
ATTENTION_GROUPS = 8
FEATURE_WIDTH = 128
STREAM_LENGTH = 512
PASS_DEV = 16
BLOCK_TOKENS = 64
PER_BLOCK = 4
PASS_LEN = 64
POSITIONS_ALL = 16384
BLK_DEV = 8
BLOCKS = 256
PASSAGES = 512
CAP = 2
N_ST = 32


def draw_store(key, part):
    base_key = jax.random.fold_in(key, 0)
    shape = (PASSAGES, PASS_LEN, D)
    values = jnp.clip(jax.random.normal(base_key, shape, jnp.float32), -6.0, 6.0)
    return values.astype(jnp.bfloat16)


def draw_extra_forgetting_exponent(key, part):
    where_key, depth_key = jax.random.split(key, 2)
    shape = (POSITIONS_ALL, ATTENTION_GROUPS)
    struck = jax.random.uniform(where_key, shape, jnp.float32) < 1.0 / 128.0
    depth = jnp.log(jax.random.uniform(depth_key, shape, jnp.float32, 0.5, 0.8))
    return jnp.where(struck, depth, 0.0).astype(jnp.float32)


def touch_ends(values, key, low, largest):
    longest = values.shape.index(max(values.shape))
    spots = []
    for shift in (0, 1):
        where = [jax.random.randint(jax.random.fold_in(key, axis), (), 0, length) for axis, length in enumerate(values.shape)]
        where[longest] = (where[longest] + shift) % values.shape[longest]
        spots.append(tuple(where))
    return values.at[spots[0]].set(low).at[spots[1]].set(largest)


def block_scale(rng, extent, cuts, least, top_value):
    loudness = 1.0
    for position, blocks in cuts:
        steps = jax.random.uniform(jax.random.fold_in(jax.random.fold_in(rng, 6), position), (blocks,), jnp.float32, least / len(cuts), top_value / len(cuts))
        loudness = loudness * jnp.repeat(jnp.exp(steps), extent[position] // blocks).reshape((-1,) + (1,) * (len(extent) - 1 - position))
    return loudness


def deal_out(key, own, number, rows, number_of, top, most, lean):
    sequence = jax.random.permutation(key, number_of)
    heavy_load, common = portions_of(number_of, rows * top, most, lean, True), portions_of(number_of, rows * top, most, lean, False)
    places = jnp.arange(number_of)

    def named(tallies, offset_by):
        used = int((tallies > 0).sum())
        fixed = max(1, used // 4)
        moved = fixed + (places - fixed + offset_by * (used - fixed)) % max(1, number_of - fixed)
        return jnp.zeros((number_of,), jnp.int32).at[sequence[jnp.where(places < fixed, places, moved)]].set(jnp.asarray(tallies, jnp.int32))

    tallies = jnp.where(number % 4 == 0, named(heavy_load, number // 4), named(common, number - number // 4 - 1))
    mixed = jax.random.permutation(jax.random.fold_in(own, 3), number_of)
    donor, taker = mixed[0:number_of // 2 * 2:2], mixed[1:number_of // 2 * 2:2]
    room = jnp.minimum(tallies[donor] - 1, most - tallies[taker]) // 2
    room = jnp.where((donor == sequence[0]) | (taker == sequence[0]) | (tallies[taker] == 0), 0, jnp.maximum(room, 0))
    moved = jax.random.randint(jax.random.fold_in(own, 4), (number_of // 2,), 0, 1 << 20) % (room + 1)
    tallies = tallies.at[donor].add(-moved).at[taker].add(moved)
    members = jnp.searchsorted(jnp.cumsum(tallies), jnp.arange(rows * top), side="right").astype(jnp.int32)
    listing = members.reshape(top, rows).T
    listing = listing[jax.random.permutation(jax.random.fold_in(own, 1), rows)]
    offset_by = jax.random.randint(jax.random.fold_in(own, 2), (rows, 1), 0, top)
    return jnp.take_along_axis(listing, (jnp.arange(top)[None, :] + offset_by) % top, axis=1)


def portions_of(number_of, total, bound, lean, full):
    loads = [(1 << 20) // math.isqrt(standing ** lean) + 1 for standing in range(1, number_of + 1)]
    largest = bound if full else min(bound, max(-(-total // number_of), total * loads[0] // sum(loads)))
    least = 1 if total - largest >= number_of - 1 else 0
    counts, rest = [largest] + [least] * (number_of - 1), total - largest - least * (number_of - 1)
    while rest > 0:
        candidates = [i for i in range(1, number_of) if counts[i] < largest] or [i for i in range(1, number_of) if counts[i] < bound]
        pool, remaining = sum([loads[i] for i in candidates]), rest
        for i in candidates:
            addition = min(bound - counts[i], max(1, remaining * loads[i] // pool), rest)
            counts[i] = counts[i] + addition
            rest = rest - addition
    return np.array(counts)


def scatter_about(stream_key, extent, deviation, reach, shards=(), kind=jnp.bfloat16):
    gain = block_scale(stream_key, extent, shards, -0.22, 0.18) if shards else 1.0
    values = jax.random.normal(stream_key, extent, jnp.float32) * deviation * gain
    return jnp.minimum(jnp.maximum(values, -reach), reach).astype(kind)


def setup_inputs(seed: int = 0, part: int = 0) -> dict:
    keys = jax.random.split(jax.random.key(seed), 17)
    own_keys = jax.random.split(jax.random.fold_in(keys[16], part), 17)
    tokens = scatter_about(own_keys[0], (POSITIONS_ALL, D), 1.0, 6.0, ((0, 32),))
    owners_keys = jax.random.split(jax.random.fold_in(own_keys[1], 1), BLOCKS // BLK_DEV)
    owners_turns = jax.random.permutation(jax.random.fold_in(own_keys[1], 3), BLOCKS // BLK_DEV)
    owners = jax.vmap(lambda own, number: deal_out(jax.random.fold_in(own_keys[1], 2), own, number, BLK_DEV, N_ST, PER_BLOCK, CAP, 2))(owners_keys, owners_turns).reshape((BLOCKS, PER_BLOCK))
    entries = touch_ends(jax.random.randint(own_keys[2], (BLOCKS, PER_BLOCK), 0, PASS_DEV), jax.random.fold_in(own_keys[2], 1), 0, PASS_DEV - 1).astype(jnp.int32)
    store = draw_store(jax.random.fold_in(jax.random.fold_in(keys[16], part), 71), part)
    mixer_query_weight = scatter_about(keys[4], (D, ATTENTION_GROUPS * FEATURE_WIDTH), D ** -0.5, 0.125, ((1, 4),))
    mixer_key_weight = scatter_about(keys[5], (D, ATTENTION_GROUPS * FEATURE_WIDTH), D ** -0.5, 0.125, ((1, 4),))
    mixer_value_weight = scatter_about(keys[6], (D, ATTENTION_GROUPS * FEATURE_WIDTH), D ** -0.5, 0.125, ((1, 4),))
    strength_weight = scatter_about(keys[7], (D, ATTENTION_GROUPS), D ** -0.5, 0.125, ((1, 4),))
    decay_weight = scatter_about(keys[8], (D, ATTENTION_GROUPS), D ** -0.5, 0.125, ((1, 4),))
    head_decay_rate = jnp.clip(jnp.exp(math.log(0.15) - 3.912023 * jax.random.uniform(keys[9], (ATTENTION_GROUPS,), jnp.float32) ** block_scale(keys[9], (ATTENTION_GROUPS,), ((0, 4),), -0.2, 0.2)), 0.003, 0.15)
    extra_forgetting_exponent = draw_extra_forgetting_exponent(jax.random.fold_in(jax.random.fold_in(keys[16], part), 71), part)
    output_norm_gain = jnp.clip(1.0 + 0.18 * jax.random.normal(keys[11], (FEATURE_WIDTH,), jnp.float32), 0.1, 1.9)
    retrieval_query_weight = scatter_about(keys[12], (D, ATTENTION_GROUPS * FEATURE_WIDTH), D ** -0.5, 0.125, ((1, 4),))
    passage_key_weight = scatter_about(keys[13], (D, ATTENTION_GROUPS * FEATURE_WIDTH), D ** -0.5, 0.125, ((1, 4),))
    passage_value_weight = scatter_about(keys[14], (D, ATTENTION_GROUPS * FEATURE_WIDTH), D ** -0.5, 0.125, ((1, 4),))
    retrieval_gate_weight = scatter_about(keys[15], (D, ATTENTION_GROUPS), D ** -0.5, 0.125, ((1, 4),))
    return {"tokens": tokens, "owners": owners, "entries": entries, "store": store, "mixer_query_weight": mixer_query_weight, "mixer_key_weight": mixer_key_weight, "mixer_value_weight": mixer_value_weight, "strength_weight": strength_weight, "decay_weight": decay_weight, "head_decay_rate": head_decay_rate, "extra_forgetting_exponent": extra_forgetting_exponent, "output_norm_gain": output_norm_gain, "retrieval_query_weight": retrieval_query_weight, "passage_key_weight": passage_key_weight, "passage_value_weight": passage_value_weight, "retrieval_gate_weight": retrieval_gate_weight}


eps = 1e-06

def matmul_high(left, right):
    return jnp.einsum('...ij,...jk->...ik', left, right, precision=lax.Precision.HIGHEST)

def unit_lower_inverse(strict_part):
    size = strict_part.shape[-1]
    ident = jnp.eye(size, dtype=jnp.float32)
    inverse = ident - strict_part
    power = strict_part
    for level in range(size.bit_length() - 2):
        power = matmul_high(power, power)
        inverse = matmul_high(inverse, ident + power)
    return inverse

def delta_rule(queries, keys_in, values_in, decay_logarithm, strength, block_slice):
    length, heads, width = queries.shape
    count = length // block_slice

    def split(array):
        return array.reshape(count, block_slice, heads, array.shape[-1]).transpose(0, 2, 1, 3)
    q_blk = split(queries)
    k_blk = split(keys_in)
    v_blk = split(values_in)
    decay_blk = decay_logarithm.reshape(count, block_slice, heads).transpose(0, 2, 1)
    beta_blk = strength.reshape(count, block_slice, heads).transpose(0, 2, 1)
    cumul = jnp.cumsum(decay_blk, axis=-1)
    lower = jnp.tril(jnp.ones((block_slice, block_slice), bool))
    strict = jnp.tril(jnp.ones((block_slice, block_slice), bool), -1)
    spread = cumul[..., :, None] - cumul[..., None, :]
    damping = jnp.where(lower, jnp.exp(jnp.where(lower, spread, 0.0)), 0.0)
    k_beta = k_blk * beta_blk[..., None]
    inner = jnp.where(strict, matmul_high(k_beta, jnp.swapaxes(k_blk, -1, -2)) * damping, 0.0)
    inverse = unit_lower_inverse(inner)
    fresh_base = matmul_high(inverse, v_blk * beta_blk[..., None])
    key_mix = matmul_high(inverse, k_beta * jnp.exp(cumul)[..., None])
    within = jnp.where(lower, matmul_high(q_blk, jnp.swapaxes(k_blk, -1, -2)) * damping, 0.0)
    q_decayed = q_blk * jnp.exp(cumul)[..., None]
    k_tail = k_blk * jnp.exp(cumul[..., -1:] - cumul)[..., None]
    carry_decay = jnp.exp(cumul[..., -1])

    def advance(state, pieces):
        q_part, k_part, base_part, mix_part, within_part, decay_part = pieces
        fresh = base_part - matmul_high(mix_part, state)
        result = matmul_high(q_part, state) + matmul_high(within_part, fresh)
        state = state * decay_part[:, None, None] + matmul_high(jnp.swapaxes(k_part, -1, -2), fresh)
        return (state, result)
    start = jnp.zeros((heads, width, values_in.shape[-1]), jnp.float32)
    final, outputs = lax.scan(advance, start, (q_decayed, k_tail, fresh_base, key_mix, within, carry_decay))
    return outputs.transpose(0, 2, 1, 3).reshape(length, heads, values_in.shape[-1])

def mixer_head_outputs(tokens, mixer_query_weight, mixer_key_weight, mixer_value_weight, strength_weight, decay_weight, head_decay_rate, extra_forgetting_exponent, output_norm_gain, block_slice):
    heads = head_decay_rate.shape[0]
    head_dim = output_norm_gain.shape[0]
    length = tokens.shape[0]

    def project(weight):
        rounded = jnp.dot(tokens, weight, preferred_element_type=jnp.float32).astype(jnp.bfloat16)
        return lax.optimization_barrier(rounded).astype(jnp.float32).reshape(length, heads, head_dim)

    def unit_rows(array):
        return array * lax.rsqrt(lax.optimization_barrier(jnp.sum(array * array, axis=-1, keepdims=True)) + eps)
    queries = unit_rows(project(mixer_query_weight)) * head_dim ** (-0.5)
    keys_in = unit_rows(project(mixer_key_weight))
    values_in = project(mixer_value_weight)
    strength = jax.nn.sigmoid(jnp.dot(tokens, strength_weight, preferred_element_type=jnp.float32))
    decay_logarithm = -head_decay_rate[None, :] * jax.nn.softplus(jnp.dot(tokens, decay_weight, preferred_element_type=jnp.float32)) + extra_forgetting_exponent
    recur = delta_rule(queries, keys_in, values_in, decay_logarithm, strength, block_slice)
    return recur * lax.rsqrt(lax.optimization_barrier(jnp.mean(recur * recur, axis=-1, keepdims=True)) + eps) * output_norm_gain

def reference(tokens, owners, entries, store, mixer_query_weight, mixer_key_weight, mixer_value_weight, strength_weight, decay_weight, head_decay_rate, extra_forgetting_exponent, output_norm_gain, retrieval_query_weight, passage_key_weight, passage_value_weight, retrieval_gate_weight):
    stream_group = tokens.reshape(N_ST, STREAM_LENGTH, D)
    forgetting_spikes = extra_forgetting_exponent.reshape(N_ST, STREAM_LENGTH, ATTENTION_GROUPS)

    def lone_stream(pair):
        return mixer_head_outputs(pair[0], mixer_query_weight, mixer_key_weight, mixer_value_weight, strength_weight, decay_weight, head_decay_rate, pair[1], output_norm_gain, BLOCK_TOKENS)
    rescaled_result = lax.map(lone_stream, (stream_group, forgetting_spikes)).reshape(POSITIONS_ALL, ATTENTION_GROUPS, FEATURE_WIDTH)
    flat_store = store.reshape(PASSAGES * PASS_LEN, D)
    pass_key = jnp.dot(flat_store, passage_key_weight, preferred_element_type=jnp.float32).astype(jnp.bfloat16).reshape(PASSAGES, PASS_LEN, ATTENTION_GROUPS * FEATURE_WIDTH)
    pass_value = jnp.dot(flat_store, passage_value_weight, preferred_element_type=jnp.float32).astype(jnp.bfloat16).reshape(PASSAGES, PASS_LEN, ATTENTION_GROUPS * FEATURE_WIDTH)
    passage = (owners.astype(jnp.int32) * PASS_DEV + entries.astype(jnp.int32)).astype(jnp.int32)
    keys_read = pass_key[passage].reshape(BLOCKS, PER_BLOCK * PASS_LEN, ATTENTION_GROUPS, FEATURE_WIDTH)
    values_read = pass_value[passage].reshape(BLOCKS, PER_BLOCK * PASS_LEN, ATTENTION_GROUPS, FEATURE_WIDTH)
    rquery = jnp.dot(tokens, retrieval_query_weight, preferred_element_type=jnp.float32).astype(jnp.bfloat16).reshape(BLOCKS, BLOCK_TOKENS, ATTENTION_GROUPS, FEATURE_WIDTH)
    scores = jnp.einsum('bqhd,bkhd->bhqk', rquery.astype(jnp.float32), keys_read.astype(jnp.float32)) * FEATURE_WIDTH ** (-0.5)
    peak = lax.optimization_barrier(jnp.max(scores, axis=-1, keepdims=True))
    expo = jnp.exp(scores - peak)
    weights = (expo / lax.optimization_barrier(jnp.sum(expo, axis=-1, keepdims=True))).astype(jnp.bfloat16)
    retrieved = jnp.einsum('bhqk,bkhd->bqhd', weights.astype(jnp.float32), values_read.astype(jnp.float32)).reshape(POSITIONS_ALL, ATTENTION_GROUPS, FEATURE_WIDTH)
    rgate = jax.nn.sigmoid(jnp.dot(tokens, retrieval_gate_weight, preferred_element_type=jnp.float32))
    mixed = rescaled_result + rgate[..., None] * retrieved
    return mixed.reshape(POSITIONS_ALL, ATTENTION_GROUPS * FEATURE_WIDTH).astype(jnp.bfloat16)
```

```python
import functools

import jax
import jax.numpy as jnp
from jax import lax
from jax.experimental import pallas as pl
from jax.experimental.pallas import tpu as pltpu
from jax.sharding import PartitionSpec as P

BLOCK = 64
SLOTS = 4
EPS = 1e-06
NONE = -1e30
MIB = 1024 * 1024
F32 = jnp.float32
BF16 = jnp.bfloat16
VMEM = pltpu.VMEM


def nt(left, right):
    return lax.dot_general(left, right, (((1,), (1,)), ((), ())), preferred_element_type=F32)


def nn(left, right):
    return jnp.dot(left, right, preferred_element_type=F32)


def tn(left, right):
    return lax.dot_general(left, right, (((0,), (0,)), ((), ())), preferred_element_type=F32)


def tie(value, *after):
    return lax.optimization_barrier((value,) + after)[0]


def params(limit, **more):
    return pltpu.CompilerParams(vmem_limit_bytes=limit * MIB, **more)


def cost(flops, size, trans=0):
    return pl.CostEstimate(flops=flops, bytes_accessed=size, transcendentals=trans)


def stack_heads(rows, out_ref):
    for b in range(rows.shape[0] // BLOCK):
        for h in range(2):
            out_ref[b, h * BLOCK : (h + 1) * BLOCK, :] = rows[
                b * BLOCK : (b + 1) * BLOCK, h * 128 : (h + 1) * 128
            ]


def project_body(x_ref, w_ref, out_ref):
    stack_heads(nn(x_ref[...], w_ref[...]).astype(BF16), out_ref)


def project(x, w, steps=2):
    rows, depth = x.shape
    tile = rows // steps
    return pl.pallas_call(
        project_body,
        grid=(steps,),
        in_specs=[
            pl.BlockSpec((tile, depth), lambda i: (i, 0)),
            pl.BlockSpec(w.shape, lambda i: (0, 0)),
        ],
        out_specs=pl.BlockSpec((tile // BLOCK, 128, 128), lambda i: (i, 0, 0)),
        out_shape=jax.ShapeDtypeStruct((rows // BLOCK, 128, 128), BF16),
        compiler_params=params(16),
        cost_estimate=cost(2 * rows * depth * 256, 2 * (rows * depth + depth * 256 + rows * 256)),
        name="project",
    )(x, w)


def gates_body(x_ref, w_ref, out_ref):
    out_ref[...] = nn(x_ref[...], w_ref[...])


def gate_logits(x, w, steps=2):
    rows, depth = x.shape
    tile = rows // steps
    return pl.pallas_call(
        gates_body,
        grid=(steps,),
        in_specs=[
            pl.BlockSpec((tile, depth), lambda i: (i, 0)),
            pl.BlockSpec(w.shape, lambda i: (0, 0)),
        ],
        out_specs=pl.BlockSpec((tile, w.shape[1]), lambda i: (i, 0)),
        out_shape=jax.ShapeDtypeStruct((rows, w.shape[1]), F32),
        compiler_params=params(16),
        cost_estimate=cost(2 * rows * depth * 128, 2 * rows * depth),
        name="gates",
    )(x, w)


def passages_body(store_ref, wk_ref, wv_ref, out_ref):
    count, rows, depth = store_ref.shape
    flat = store_ref[...].reshape(count * rows, depth)
    keys = nn(flat, wk_ref[...]).astype(BF16)
    values = nn(flat, wv_ref[...]).astype(BF16).astype(F32)
    for p in range(count):
        span = slice(p * rows, (p + 1) * rows)
        for h in range(2):
            out_ref[p, h * rows : (h + 1) * rows, :] = keys[span, h * 128 : (h + 1) * 128]
        stacked = jnp.concatenate([values[span, :128], values[span, 128:]], axis=0)
        out_ref[p, 128:256, :] = stacked.T.astype(BF16)


def project_passages(store, wk, wv, first, number, per_step=2):
    _, rows, depth = store.shape
    skip = first // per_step
    return pl.pallas_call(
        passages_body,
        grid=(number // per_step,),
        in_specs=[
            pl.BlockSpec((per_step, rows, depth), lambda i: (i + skip, 0, 0)),
            pl.BlockSpec(wk.shape, lambda i: (0, 0)),
            pl.BlockSpec(wv.shape, lambda i: (0, 0)),
        ],
        out_specs=pl.BlockSpec((per_step, 256, 128), lambda i: (i, 0, 0)),
        out_shape=jax.ShapeDtypeStruct((number, 256, 128), BF16),
        compiler_params=params(16),
        cost_estimate=cost(2 * number * rows * depth * 512, 2 * number * rows * depth),
        name="passages",
    )(store, wk, wv)


def mixer_body(q_ref, k_ref, v_ref, lg_ref, ex_ref, rate_ref, gain_ref, s_ref, out_ref, s_out_ref):
    ri = lax.broadcasted_iota(jnp.int32, (128, 128), 0)
    ci = lax.broadcasted_iota(jnp.int32, (128, 128), 1)
    same = (ri >= BLOCK) == (ci >= BLOCK)
    lower = same & (ri >= ci)
    strict = same & (ri > ci)
    upper = same & (ri <= ci)
    diag = ri == ci
    top = lax.broadcasted_iota(jnp.int32, (128, 1), 0) < BLOCK
    rate = jnp.where(top, rate_ref[0], rate_ref[1])
    pieces = []
    for n in range(q_ref.shape[0]):
        lg = lg_ref[n * BLOCK : (n + 1) * BLOCK, :]
        ex = ex_ref[n * BLOCK : (n + 1) * BLOCK, :]
        beta = jax.nn.sigmoid(jnp.concatenate([lg[:, 0:1], lg[:, 1:2]], axis=0))
        pre = jnp.concatenate([lg[:, 2:3], lg[:, 3:4]], axis=0)
        extra = jnp.concatenate([ex[:, 0:1], ex[:, 1:2]], axis=0)
        soft = jnp.maximum(pre, 0.0) + jnp.log1p(jnp.exp(-jnp.abs(pre)))
        g = extra - rate * soft
        g_row = jnp.sum(jnp.where(diag, g, 0.0), axis=0, keepdims=True)
        c = jnp.sum(jnp.where(lower, g_row, 0.0), axis=1, keepdims=True)
        total = jnp.sum(jnp.where(same, g_row, 0.0), axis=1, keepdims=True)
        c_row = jnp.sum(jnp.where(upper, g, 0.0), axis=0, keepdims=True)
        damping = jnp.where(lower, jnp.exp(jnp.where(lower, c - c_row, 0.0)), 0.0)
        q = q_ref[n].astype(F32)
        k = k_ref[n].astype(F32)
        v = v_ref[n].astype(F32)
        q = q * (lax.rsqrt(jnp.sum(q * q, axis=1, keepdims=True) + EPS) * 128**-0.5)
        k = k * lax.rsqrt(jnp.sum(k * k, axis=1, keepdims=True) + EPS)
        kb = k * beta
        decay = jnp.exp(c)
        k16 = k.astype(BF16)
        power = jnp.where(strict, nt(kb.astype(BF16), k16) * damping, 0.0)
        within = (nt(q.astype(BF16), k16) * damping).astype(BF16)
        inverse = jnp.where(diag, 1.0, 0.0) - power
        p16 = power.astype(BF16)
        for _ in range(5):
            p16 = nn(p16, p16).astype(BF16)
            inverse = inverse + nn(inverse.astype(BF16), p16)
        inv16 = inverse.astype(BF16)
        mix = nn(inv16, (kb * decay).astype(BF16)).astype(BF16)
        base = nn(inv16, (v * beta).astype(BF16))
        q_dec = (q * decay).astype(BF16)
        k_tail = (k * jnp.exp(total - c)).astype(BF16)
        pieces.append((mix, base, within, q_dec, k_tail, jnp.exp(total)))
    state = [s_ref[0], s_ref[1]]
    for n, (mix, base, within, q_dec, k_tail, keep) in enumerate(pieces):
        fresh, far = [], []
        for h in range(2):
            rows = slice(h * BLOCK, (h + 1) * BLOCK)
            both = nn(jnp.concatenate([mix[rows], q_dec[rows]], axis=0), state[h].astype(BF16))
            fresh.append(base[rows] - both[:BLOCK])
            far.append(both[BLOCK:])
        f16 = jnp.concatenate(fresh, axis=0).astype(BF16)
        recur = jnp.concatenate(far, axis=0) + nn(within, f16)
        for h in range(2):
            rows = slice(h * BLOCK, (h + 1) * BLOCK)
            state[h] = state[h] * keep[h * BLOCK : h * BLOCK + 1] + tn(k_tail[rows], f16[rows])
        scale = lax.rsqrt(jnp.mean(recur * recur, axis=1, keepdims=True) + EPS)
        out_ref[n] = recur * scale * gain_ref[...]
    s_out_ref[0] = state[0]
    s_out_ref[1] = state[1]


def mixer(q, k, v, logits, extra, rate, gain, state, first, number):
    at = first // number
    return pl.pallas_call(
        mixer_body,
        grid=(1,),
        in_specs=[
            pl.BlockSpec((number, 128, 128), lambda i: (at, 0, 0)),
            pl.BlockSpec((number, 128, 128), lambda i: (at, 0, 0)),
            pl.BlockSpec((number, 128, 128), lambda i: (at, 0, 0)),
            pl.BlockSpec((number * BLOCK, logits.shape[1]), lambda i: (at, 0)),
            pl.BlockSpec((number * BLOCK, 2), lambda i: (at, 0)),
            pl.BlockSpec(memory_space=pltpu.SMEM),
            pl.BlockSpec((1, 128), lambda i: (0, 0)),
            pl.BlockSpec((2, 128, 128), lambda i: (0, 0, 0)),
        ],
        out_specs=[
            pl.BlockSpec((number, 128, 128), lambda i: (0, 0, 0)),
            pl.BlockSpec((2, 128, 128), lambda i: (0, 0, 0)),
        ],
        out_shape=[
            jax.ShapeDtypeStruct((number, 128, 128), F32),
            jax.ShapeDtypeStruct((2, 128, 128), F32),
        ],
        compiler_params=params(16),
        cost_estimate=cost(number * 1000 * MIB // 2, number * 300 * 1024),
        name="mixer",
    )(q, k, v, logits, extra, rate, gain, state)


def split3(x):
    high = x.astype(BF16)
    rest = x - high.astype(F32)
    mid = rest.astype(BF16)
    low = (rest - mid.astype(F32)).astype(BF16)
    return high.astype(F32), mid.astype(F32), low.astype(F32)


def attend_body(step, empty, list_ref, q_ref, kv_ref, *refs):
    if empty:
        (out_ref, q_buf, kv_buf, sems) = refs
    else:
        (msg_ref, out_ref, q_buf, kv_buf, sems) = refs
    row = ((step * list_ref[0]) & 31) * SLOTS + 8
    codes = [list_ref[row + r] for r in range(SLOTS)]
    valid = [code > 0 for code in codes]
    block = [jnp.maximum(code - 1, 0) >> 5 for code in codes]
    entry = [jnp.maximum(code - 1, 0) & 31 for code in codes]
    copies = []
    for r in range(SLOTS):
        copies.append(pltpu.make_async_copy(q_ref.at[block[r]], q_buf.at[r], sems.at[0, r]))
        copies.append(pltpu.make_async_copy(kv_ref.at[entry[r]], kv_buf.at[r], sems.at[1, r]))
    for copy in copies:
        copy.start()
    if empty:
        pad = lax.broadcasted_iota(jnp.int32, (8, 128), 0)
        start = jnp.where(pad == 0, NONE, 0.0)
        for b in range(out_ref.shape[0]):
            out_ref[b, 0:128, :] = jnp.zeros((128, 128), BF16)
            out_ref[b, 128:136, :] = start.astype(BF16)
    else:
        out_ref[...] = msg_ref[...]
    for copy in copies:
        copy.wait()
    left = lax.broadcasted_iota(jnp.int32, (BLOCK, 128), 1) < BLOCK
    parts = []
    for r in range(SLOTS):
        both = nt(kv_buf[r, 0:128, :], q_buf[r])
        scores = jnp.where(left, both[:BLOCK], both[BLOCK:]) * 128**-0.5
        scores = jnp.where(valid[r], scores, NONE)
        peak = jnp.max(scores, axis=0, keepdims=True)
        expo = jnp.exp(scores - peak)
        denom = jnp.sum(expo, axis=0, keepdims=True)
        apart = jnp.concatenate(
            [jnp.where(left, expo, 0.0), jnp.where(left, 0.0, expo)], axis=0
        ).astype(BF16)
        parts.append((peak, denom, nn(kv_buf[r, 128:256, :], apart)))
    for r in range(SLOTS):
        peak, denom, sums = parts[r]
        b = block[r]
        stats = out_ref[b, 128:136, :].astype(F32)
        m_old = stats[0:1] + stats[1:2] + stats[2:3]
        l_old = stats[3:4] + stats[4:5] + stats[5:6]
        m_new = jnp.maximum(m_old, peak)
        keep = jnp.exp(m_old - m_new)
        gain = jnp.where(valid[r], jnp.exp(peak - m_new), 0.0)
        l_new = l_old * keep + denom * gain
        zero = jnp.zeros((2, 128), F32)
        fresh = jnp.concatenate(split3(m_new) + split3(l_new) + (zero,), axis=0)
        out_ref[b, 128:136, :] = fresh.astype(BF16)
        out_ref[b, 0:128, :] = (out_ref[b, 0:128, :].astype(F32) * keep + sums * gain).astype(BF16)


def attend(step, lists, q, kv, msg=None):
    blocks = q.shape[0]
    shape = (blocks, 136, 128)
    whole = pl.BlockSpec(memory_space=VMEM)
    anywhere = pl.BlockSpec(memory_space=pl.ANY)
    more = () if msg is None else (msg,)
    return pl.pallas_call(
        functools.partial(attend_body, step, msg is None),
        in_specs=[pl.BlockSpec(memory_space=pltpu.SMEM), anywhere, anywhere] + [whole] * len(more),
        out_specs=whole,
        out_shape=jax.ShapeDtypeStruct(shape, BF16),
        scratch_shapes=[
            VMEM((SLOTS, 128, 128), BF16),
            VMEM((SLOTS, 256, 128), BF16),
            pltpu.SemaphoreType.DMA((2, SLOTS)),
        ],
        compiler_params=params(8),
        cost_estimate=cost(600 * MIB, 1000 * 1024),
        name="attend",
    )(lists, q, kv, *more)


def finish_body(a_ref, b_ref, lg_ref, *refs):
    normed, out_ref = refs[:-1], refs[-1]
    per = normed[0].shape[0]
    for b in range(a_ref.shape[0]):
        sa = a_ref[b, 128:136, :].astype(F32)
        sb = b_ref[b, 128:136, :].astype(F32)
        ma, mb = (s[0:1] + s[1:2] + s[2:3] for s in (sa, sb))
        la, lb = (s[3:4] + s[4:5] + s[5:6] for s in (sa, sb))
        peak = jnp.maximum(ma, mb)
        ga, gb = jnp.exp(ma - peak), jnp.exp(mb - peak)
        denom = la * ga + lb * gb
        sums = a_ref[b, 0:128, :].astype(F32) * ga + b_ref[b, 0:128, :].astype(F32) * gb
        retrieved = (sums / denom).T
        lg = lg_ref[b * BLOCK : (b + 1) * BLOCK, :]
        gate = jax.nn.sigmoid(jnp.concatenate([lg[:, 4:5], lg[:, 5:6]], axis=0))
        mixed = (normed[b // per][b % per] + gate * retrieved).astype(BF16)
        for h in range(2):
            out_ref[b * BLOCK : (b + 1) * BLOCK, h * 128 : (h + 1) * 128] = mixed[
                h * BLOCK : (h + 1) * BLOCK
            ]


def finish(a, b, logits, normed):
    rows = logits.shape[0]
    return pl.pallas_call(
        finish_body,
        out_shape=jax.ShapeDtypeStruct((rows, 256), BF16),
        compiler_params=params(16),
        cost_estimate=cost(100 * MIB, 2 * MIB),
        name="finish",
    )(a, b, logits, *normed)


def per_device(
    tokens,
    owners,
    entries,
    store,
    mixer_query_weight,
    mixer_key_weight,
    mixer_value_weight,
    strength_weight,
    decay_weight,
    head_decay_rate,
    extra_forgetting_exponent,
    output_norm_gain,
    retrieval_query_weight,
    passage_key_weight,
    passage_value_weight,
    retrieval_gate_weight,
):
    devices = lax.axis_size("st")
    me = lax.axis_index("st")
    core = lax.rem(me, 2)
    side = 1 - 2 * core
    reach = devices // 4
    blocks, per_block = owners.shape
    requests = blocks * per_block
    passages = store.shape[0]

    out_pairs = [(i, (i + (2 if i % 2 == 0 else -2)) % devices) for i in range(devices)]
    back_pairs = [(j, i) for i, j in out_pairs]
    mate_pairs = [(i, i ^ 1) for i in range(devices)]

    def out(x):
        return lax.ppermute(x, "st", out_pairs)

    def back(x):
        return lax.ppermute(x, "st", back_pairs)

    def mate(x):
        return lax.ppermute(x, "st", mate_pairs)

    query = project(tokens, retrieval_query_weight)
    own = {0: query}
    other = {}

    table = jnp.concatenate([owners.reshape(1, requests), entries.reshape(1, requests)], axis=1)
    known = 1
    while known < devices:
        shift = [(i, (i + known) % devices) for i in range(devices)]
        table = jnp.concatenate([table, lax.ppermute(table, "st", shift)], axis=0)
        known *= 2
    name, place = table[:, :requests], table[:, requests:]
    hit = (name // 2) == (me // 2)
    earlier = jnp.arange(requests)[:, None] < jnp.arange(requests)[None, :]
    rank = jnp.dot(hit.astype(BF16), earlier.astype(BF16), preferred_element_type=F32)
    rank = rank.astype(jnp.int32)
    entry = jnp.where(name % 2 == core, 0, passages) + place
    code = (jnp.arange(requests, dtype=jnp.int32) // per_block)[None, :] * 32 + entry + 1
    listed = jnp.stack(
        [jnp.sum(jnp.where(hit & (rank == r), code, 0), axis=1) for r in range(SLOTS)], axis=1
    )
    lists = jnp.concatenate(
        [jnp.full((8,), 1, jnp.int32) * side, listed.reshape(devices * SLOTS)]
    )

    gate_weight = jnp.concatenate([strength_weight, decay_weight, retrieval_gate_weight], axis=1)
    gain = output_norm_gain.reshape(1, 128)

    work = {}

    def keys_low(dep):
        work["kv0"] = project_passages(
            tie(store, dep), passage_key_weight, passage_value_weight, 0, passages // 2
        )
        return work["kv0"]

    def keys_high(dep):
        work["kv1"] = project_passages(
            tie(store, dep), passage_key_weight, passage_value_weight, passages // 2, passages // 2
        )
        return work["kv1"]

    def proj(key, weight):
        def run(dep):
            work[key] = project(tie(tokens, dep), weight)
            return work[key]

        return run

    def gates(dep):
        work["lg"] = gate_logits(tie(tokens, dep), gate_weight)
        return work["lg"]

    normed = []
    number = 2
    work["s"] = jnp.zeros((2, 128, 128), F32)

    def chunk(n):
        def run(dep):
            result, work["s"] = mixer(
                work["q"],
                work["k"],
                work["v"],
                work["lg"],
                extra_forgetting_exponent,
                head_decay_rate,
                gain,
                tie(work["s"], dep),
                n * number,
                number,
            )
            normed.append(result)
            return work["s"]

        return run

    pieces = [
        keys_low,
        keys_high,
        proj("q", mixer_query_weight),
        proj("k", mixer_key_weight),
        proj("v", mixer_value_weight),
        gates,
    ] + [chunk(n) for n in range(blocks // number)]

    own[1] = out(query)
    other[0] = mate(query)
    other[1] = out(other[0])
    last = other[0]
    for h in range(1, reach):
        for lane in (own, other):
            arrived = lane[h]
            if pieces:
                done = pieces.pop(0)(last)
                arrived = tie(arrived, done)
            lane[h] = arrived
            last = arrived
            if h + 1 < reach or lane is own:
                lane[h + 1] = out(arrived)
    while pieces:
        last = pieces.pop(0)(last)

    kv_own = jnp.concatenate([work["kv0"], work["kv1"]], axis=0)
    kv = jnp.concatenate([kv_own, mate(kv_own)], axis=0)

    far_other = attend(2 * (reach - 1) - 1, lists, other[reach - 1], kv)
    msg_other = back(far_other)
    far_own = attend(2 * reach, lists, own[reach], kv)
    msg_own = back(tie(far_own, far_other))
    last = far_own
    for h in range(reach - 2, 0, -1):
        last = attend(2 * h - 1, lists, other[h], kv, tie(msg_other, last))
        msg_other = back(last)
        last = attend(2 * (h + 1), lists, own[h + 1], kv, tie(msg_own, last))
        msg_own = back(last)
    msg_other = mate(tie(msg_other, last))
    last = attend(2, lists, own[1], kv, msg_own)
    msg_own = back(last)
    msg_own = attend(0, lists, own[0], kv, msg_own)
    return finish(msg_own, msg_other, work["lg"], normed)


def solution(mesh):
    return jax.shard_map(
        per_device,
        mesh=mesh,
        in_specs=(
            P(("grp", "st"), None),
            P(("grp", "st"), None),
            P(("grp", "st"), None),
            P(("grp", "st"), None, None),
            P(None, "tp"),
            P(None, "tp"),
            P(None, "tp"),
            P(None, "tp"),
            P(None, "tp"),
            P("tp"),
            P(("grp", "st"), "tp"),
            P(),
            P(None, "tp"),
            P(None, "tp"),
            P(None, "tp"),
            P(None, "tp"),
        ),
        out_specs=P(("grp", "st"), "tp"),
        check_vma=False,
    )
```

```python
import functools

import jax
import jax.numpy as jnp
from jax import lax
from jax.experimental import pallas as pl
from jax.experimental.pallas import tpu as pltpu
from jax.sharding import PartitionSpec as P

BLOCK = 64
SLOTS = 4
EPS = 1e-06
NONE = -1e30
MIB = 1024 * 1024
F32 = jnp.float32
BF16 = jnp.bfloat16
VMEM = pltpu.VMEM


def nt(left, right):
    return lax.dot_general(left, right, (((1,), (1,)), ((), ())), preferred_element_type=F32)


def nn(left, right):
    return jnp.dot(left, right, preferred_element_type=F32)


def tn(left, right):
    return lax.dot_general(left, right, (((0,), (0,)), ((), ())), preferred_element_type=F32)


def tie(value, *after):
    return lax.optimization_barrier((value,) + after)[0]


def params(limit, **more):
    return pltpu.CompilerParams(vmem_limit_bytes=limit * MIB, **more)


def cost(flops, size, trans=0):
    return pl.CostEstimate(flops=flops, bytes_accessed=size, transcendentals=trans)


def query_body(x_hbm, w_hbm, owners_ref, entries_ref, out_ref, x_buf, w_buf, sems):
    tiles, rows, _ = x_buf.shape
    load_w = pltpu.make_async_copy(w_hbm, w_buf, sems.at[tiles])
    loads = [
        pltpu.make_async_copy(x_hbm.at[pl.ds(i * rows, rows)], x_buf.at[i], sems.at[i])
        for i in range(tiles)
    ]
    load_w.start()
    for load in loads:
        load.start()
    per, count = owners_ref.shape
    blocks = tiles * rows // BLOCK
    names = jnp.concatenate([owners_ref[...], entries_ref[...]], axis=0).astype(F32)
    out_ref[blocks * 128 :, :] = jnp.zeros((2 * per, 128), BF16)
    out_ref[blocks * 128 :, 0:count] = names.astype(BF16)
    load_w.wait()
    for i in range(tiles):
        loads[i].wait()
        q = nn(x_buf[i], w_buf[...]).astype(BF16)
        for n in range(rows // BLOCK):
            at = (i * rows // BLOCK + n) * 128
            for h in range(2):
                out_ref[at + h * BLOCK : at + (h + 1) * BLOCK, :] = q[
                    n * BLOCK : (n + 1) * BLOCK, h * 128 : (h + 1) * 128
                ]


def query_message(x, w, owners, entries, tiles=4):
    rows, depth = x.shape
    hbm = pl.BlockSpec(memory_space=pltpu.HBM)
    whole = pl.BlockSpec(memory_space=VMEM)
    return pl.pallas_call(
        query_body,
        in_specs=[hbm, hbm, whole, whole],
        out_specs=whole,
        out_shape=jax.ShapeDtypeStruct((rows * 2 + 8, 128), BF16),
        scratch_shapes=[
            VMEM((tiles, rows // tiles, depth), BF16),
            VMEM(w.shape, BF16),
            pltpu.SemaphoreType.DMA((tiles + 1,)),
        ],
        compiler_params=params(12),
        cost_estimate=cost(2 * rows * depth * 256, 2 * (rows * depth + depth * 256)),
        name="query",
    )(x, w, owners, entries)


def mixed_body(x_hbm, wq_hbm, wk_hbm, wv_hbm, ga_ref, gb_ref, gc_ref, q_ref, k_ref, v_ref, lg_ref, x_buf, w_buf, sems):
    load_x = pltpu.make_async_copy(x_hbm, x_buf, sems.at[3])
    loads = [
        pltpu.make_async_copy(w, w_buf.at[i], sems.at[i])
        for i, w in enumerate((wq_hbm, wk_hbm, wv_hbm))
    ]
    load_x.start()
    for load in loads:
        load.start()
    depth = x_buf.shape[1]
    none = jnp.zeros((2, depth), BF16)
    gates = jnp.concatenate([ga_ref[...], gb_ref[...], gc_ref[...], none], axis=0)
    load_x.wait()
    lg_ref[...] = nt(x_buf[...], gates)
    for i, out_ref in enumerate((q_ref, k_ref, v_ref)):
        loads[i].wait()

        def tile(t, _):
            rows = nn(x_buf[pl.ds(t * 128, 128), :], w_buf[i]).astype(BF16)
            for n in range(2):
                for h in range(2):
                    out_ref[2 * t + n, h * BLOCK : (h + 1) * BLOCK, :] = rows[
                        n * BLOCK : (n + 1) * BLOCK, h * 128 : (h + 1) * 128
                    ]
            return 0

        lax.fori_loop(0, x_buf.shape[0] // 128, tile, 0)


def mixer_inputs(x, wq, wk, wv, ga, gb, gc):
    rows, depth = x.shape
    hbm = pl.BlockSpec(memory_space=pltpu.HBM)
    whole = pl.BlockSpec(memory_space=VMEM)
    stacked = jax.ShapeDtypeStruct((rows // BLOCK, 128, 128), BF16)
    return pl.pallas_call(
        mixed_body,
        in_specs=[hbm] * 4 + [whole] * 3,
        out_specs=[whole] * 4,
        out_shape=[stacked] * 3 + [jax.ShapeDtypeStruct((rows, 8), F32)],
        scratch_shapes=[
            VMEM(x.shape, BF16),
            VMEM((3,) + wq.shape, BF16),
            pltpu.SemaphoreType.DMA((4,)),
        ],
        compiler_params=params(16),
        cost_estimate=cost(2 * rows * depth * 768, 2 * (rows * depth + depth * 768)),
        name="mixer_inputs",
    )(x, wq, wk, wv, ga, gb, gc)


def passages_body(store_ref, wk_ref, wv_ref, out_ref):
    count, rows, depth = store_ref.shape
    flat = store_ref[...].reshape(count * rows, depth)
    keys = nn(flat, wk_ref[...]).astype(BF16)
    values = nn(flat, wv_ref[...]).astype(BF16).astype(F32)
    for p in range(count):
        span = slice(p * rows, (p + 1) * rows)
        for h in range(2):
            out_ref[p, h * rows : (h + 1) * rows, :] = keys[span, h * 128 : (h + 1) * 128]
        stacked = jnp.concatenate([values[span, :128], values[span, 128:]], axis=0)
        out_ref[p, 128:256, :] = stacked.T.astype(BF16)


def project_passages(store, wk, wv, first, number, per_step=2):
    _, rows, depth = store.shape
    skip = first // per_step
    return pl.pallas_call(
        passages_body,
        grid=(number // per_step,),
        in_specs=[
            pl.BlockSpec((per_step, rows, depth), lambda i: (i + skip, 0, 0)),
            pl.BlockSpec(wk.shape, lambda i: (0, 0)),
            pl.BlockSpec(wv.shape, lambda i: (0, 0)),
        ],
        out_specs=pl.BlockSpec((per_step, 256, 128), lambda i: (i, 0, 0)),
        out_shape=jax.ShapeDtypeStruct((number, 256, 128), BF16),
        compiler_params=params(16),
        cost_estimate=cost(2 * number * rows * depth * 512, 2 * number * rows * depth),
        name="passages",
    )(store, wk, wv)


def mixer_body(first, q_ref, k_ref, v_ref, lg_ref, ex_ref, rate_ref, gain_ref, s_ref, out_ref, s_out_ref):
    ri = lax.broadcasted_iota(jnp.int32, (128, 128), 0)
    ci = lax.broadcasted_iota(jnp.int32, (128, 128), 1)
    same = (ri >= BLOCK) == (ci >= BLOCK)
    lower = same & (ri >= ci)
    strict = same & (ri > ci)
    upper = same & (ri <= ci)
    diag = ri == ci
    top = lax.broadcasted_iota(jnp.int32, (128, 1), 0) < BLOCK
    rate = jnp.where(top, rate_ref[0], rate_ref[1])
    pieces = []
    for n in range(q_ref.shape[0]):
        lg = lg_ref[n * BLOCK : (n + 1) * BLOCK, :]
        at = (first + n) * BLOCK
        ex = jnp.concatenate([ex_ref[0:1, at : at + BLOCK], ex_ref[1:2, at : at + BLOCK]], axis=1)
        beta = jax.nn.sigmoid(jnp.concatenate([lg[:, 0:1], lg[:, 1:2]], axis=0))
        pre = jnp.concatenate([lg[:, 2:3], lg[:, 3:4]], axis=0)
        extra = jnp.sum(jnp.where(diag, ex, 0.0), axis=1, keepdims=True)
        soft = jnp.maximum(pre, 0.0) + jnp.log1p(jnp.exp(-jnp.abs(pre)))
        g = extra - rate * soft
        g_row = jnp.sum(jnp.where(diag, g, 0.0), axis=0, keepdims=True)
        c = jnp.sum(jnp.where(lower, g_row, 0.0), axis=1, keepdims=True)
        total = jnp.sum(jnp.where(same, g_row, 0.0), axis=1, keepdims=True)
        c_row = jnp.sum(jnp.where(upper, g, 0.0), axis=0, keepdims=True)
        damping = jnp.where(lower, jnp.exp(jnp.where(lower, c - c_row, 0.0)), 0.0)
        q = q_ref[n].astype(F32)
        k = k_ref[n].astype(F32)
        v = v_ref[n].astype(F32)
        q = q * (lax.rsqrt(jnp.sum(q * q, axis=1, keepdims=True) + EPS) * 128**-0.5)
        k = k * lax.rsqrt(jnp.sum(k * k, axis=1, keepdims=True) + EPS)
        kb = k * beta
        decay = jnp.exp(c)
        k16 = k.astype(BF16)
        power = jnp.where(strict, nt(kb.astype(BF16), k16) * damping, 0.0)
        within = (nt(q.astype(BF16), k16) * damping).astype(BF16)
        inverse = jnp.where(diag, 1.0, 0.0) - power
        p16 = power.astype(BF16)
        for _ in range(5):
            p16 = nn(p16, p16).astype(BF16)
            inverse = inverse + nn(inverse.astype(BF16), p16)
        inv16 = inverse.astype(BF16)
        mix = nn(inv16, (kb * decay).astype(BF16)).astype(BF16)
        base = nn(inv16, (v * beta).astype(BF16))
        q_dec = (q * decay).astype(BF16)
        k_tail = (k * jnp.exp(total - c)).astype(BF16)
        pieces.append((mix, base, within, q_dec, k_tail, jnp.exp(total)))
    state = [s_ref[0], s_ref[1]]
    for n, (mix, base, within, q_dec, k_tail, keep) in enumerate(pieces):
        fresh, far = [], []
        for h in range(2):
            rows = slice(h * BLOCK, (h + 1) * BLOCK)
            both = nn(jnp.concatenate([mix[rows], q_dec[rows]], axis=0), state[h].astype(BF16))
            fresh.append(base[rows] - both[:BLOCK])
            far.append(both[BLOCK:])
        f16 = jnp.concatenate(fresh, axis=0).astype(BF16)
        recur = jnp.concatenate(far, axis=0) + nn(within, f16)
        for h in range(2):
            rows = slice(h * BLOCK, (h + 1) * BLOCK)
            state[h] = state[h] * keep[h * BLOCK : h * BLOCK + 1] + tn(k_tail[rows], f16[rows])
        scale = lax.rsqrt(jnp.mean(recur * recur, axis=1, keepdims=True) + EPS)
        out_ref[n] = recur * scale * gain_ref[...]
    s_out_ref[0] = state[0]
    s_out_ref[1] = state[1]


def mixer(q, k, v, logits, extra, rate, gain, state, first, number):
    at = first // number
    return pl.pallas_call(
        functools.partial(mixer_body, first),
        grid=(1,),
        in_specs=[
            pl.BlockSpec((number, 128, 128), lambda i: (at, 0, 0)),
            pl.BlockSpec((number, 128, 128), lambda i: (at, 0, 0)),
            pl.BlockSpec((number, 128, 128), lambda i: (at, 0, 0)),
            pl.BlockSpec((number * BLOCK, logits.shape[1]), lambda i: (at, 0)),
            pl.BlockSpec(extra.shape, lambda i: (0, 0)),
            pl.BlockSpec(memory_space=pltpu.SMEM),
            pl.BlockSpec((1, 128), lambda i: (0, 0)),
            pl.BlockSpec((2, 128, 128), lambda i: (0, 0, 0)),
        ],
        out_specs=[
            pl.BlockSpec((number, 128, 128), lambda i: (0, 0, 0)),
            pl.BlockSpec((2, 128, 128), lambda i: (0, 0, 0)),
        ],
        out_shape=[
            jax.ShapeDtypeStruct((number, 128, 128), F32),
            jax.ShapeDtypeStruct((2, 128, 128), F32),
        ],
        compiler_params=params(16),
        cost_estimate=cost(number * 1000 * MIB // 2, number * 300 * 1024),
        name="mixer",
    )(q, k, v, logits, extra, rate, gain, state)


def parts_body(count, own_ref, *refs):
    messages, refs = refs[:count], refs[count:]
    (kv_ref, mate_ref, sums_ref, stats_ref, codes_ref, names, wide, codes, q_buf, kv_buf, sems, one) = refs
    chip, core = own_ref[0], own_ref[1]
    rows = messages[0].shape[0]
    tables = [
        pltpu.make_async_copy(m.at[pl.ds(rows - 8, 8)], names.at[n], one.at[n])
        for n, m in enumerate(messages)
    ]
    for table in tables:
        table.start()
    row = lax.broadcasted_iota(jnp.int32, (8, 128), 0)
    lane = lax.broadcasted_iota(jnp.int32, (8, 128), 1)
    before = (
        lax.broadcasted_iota(jnp.int32, (128, 128), 0) < lax.broadcasted_iota(jnp.int32, (128, 128), 1)
    )
    before = jnp.where(before, 1.0, 0.0).astype(BF16)
    blocks = (rows - 8) // 128
    found = jnp.zeros((8, 128), F32)
    for n in range(count):
        tables[n].wait()
        table = names[n].astype(F32)
        entry = jnp.concatenate([table[4:8], table[4:8]], axis=0)
        name = table.astype(jnp.int32)
        hit = ((name >> 1) == chip) & (row < 4) & (lane < blocks)
        ones = jnp.where(hit, 1.0, 0.0)
        rank = nn(ones.astype(BF16), before)
        sums = jnp.sum(ones, axis=1, keepdims=True)
        first, second, third = sums[0:1], sums[1:2], sums[2:3]
        rank = rank + jnp.where(row > 0, first, 0.0)
        rank = rank + jnp.where(row > 1, second, 0.0)
        rank = rank + jnp.where(row > 2, third, 0.0)
        far = jnp.where((name & 1) == core, 0.0, 16.0)
        code = lane.astype(F32) * 32.0 + far + entry + 1.0
        for r in range(SLOTS):
            value = jnp.where(hit & (rank == float(r)), code, 0.0)
            value = jnp.sum(jnp.sum(value, axis=1, keepdims=True), axis=0, keepdims=True)
            found = jnp.where((row == n) & (lane == r), value, found)
    wide[...] = found.astype(jnp.int32)
    to_scalar = pltpu.make_async_copy(wide, codes, one.at[count])
    to_scalar.start()
    to_scalar.wait()
    for n in range(count):
        for r in range(SLOTS):
            i = n * SLOTS + r
            code = codes[n, r]
            codes_ref[i] = code
            spot = jnp.maximum(code - 1, 0)
            at = pl.multiple_of((spot >> 5) * 128, 128)
            pltpu.make_async_copy(messages[n].at[pl.ds(at, 128)], q_buf.at[i], sems.at[0, i]).start()

            @pl.when((spot & 16) == 0)
            def _():
                pltpu.make_async_copy(kv_ref.at[spot & 15], kv_buf.at[i], sems.at[1, i]).start()

            @pl.when((spot & 16) != 0)
            def _():
                pltpu.make_async_copy(mate_ref.at[spot & 15], kv_buf.at[i], sems.at[1, i]).start()

    left = lax.broadcasted_iota(jnp.int32, (BLOCK, 128), 1) < BLOCK
    for n in range(count):
        for r in range(SLOTS):
            i = n * SLOTS + r
            pltpu.make_async_copy(messages[n].at[pl.ds(0, 128)], q_buf.at[i], sems.at[0, i]).wait()
            pltpu.make_async_copy(kv_ref.at[0], kv_buf.at[i], sems.at[1, i]).wait()
        for r in range(SLOTS):
            i = n * SLOTS + r
            both = nt(kv_buf[i, 0:128, :], q_buf[i])
            scores = jnp.where(left, both[:BLOCK], both[BLOCK:]) * 128**-0.5
            peak = jnp.max(scores, axis=0, keepdims=True)
            expo = jnp.exp(scores - peak)
            denom = jnp.sum(expo, axis=0, keepdims=True)
            apart = jnp.concatenate(
                [jnp.where(left, expo, 0.0), jnp.where(left, 0.0, expo)], axis=0
            ).astype(BF16)
            sums_ref[i] = nn(kv_buf[i, 128:256, :], apart)
            stats_ref[i] = jnp.where(row == 0, peak, denom)


def parts(own, messages, kv, kv_mate):
    count = len(messages)
    total = count * SLOTS
    anywhere = pl.BlockSpec(memory_space=pl.ANY)
    whole = pl.BlockSpec(memory_space=VMEM)
    scalars = pl.BlockSpec(memory_space=pltpu.SMEM)
    return pl.pallas_call(
        functools.partial(parts_body, count),
        in_specs=[scalars] + [anywhere] * (count + 2),
        out_specs=[whole, whole, scalars],
        out_shape=[
            jax.ShapeDtypeStruct((total, 128, 128), F32),
            jax.ShapeDtypeStruct((total, 8, 128), F32),
            jax.ShapeDtypeStruct((total,), jnp.int32),
        ],
        scratch_shapes=[
            VMEM((count, 8, 128), BF16),
            VMEM((8, 128), jnp.int32),
            pltpu.SMEM((8, 128), jnp.int32),
            VMEM((total, 128, 128), BF16),
            VMEM((total, 256, 128), BF16),
            pltpu.SemaphoreType.DMA((2, total)),
            pltpu.SemaphoreType.DMA((count + 1,)),
        ],
        compiler_params=params(12),
        cost_estimate=cost(count * 400 * MIB, count * 500 * 1024),
        name="parts",
    )(own, *messages, kv, kv_mate)


def split3(x):
    high = x.astype(BF16)
    rest = x - high.astype(F32)
    mid = rest.astype(BF16)
    low = (rest - mid.astype(F32)).astype(BF16)
    return high.astype(F32), mid.astype(F32), low.astype(F32)


def merge_body(first, empty, codes_ref, sums_ref, stats_ref, *refs):
    if empty:
        (out_ref,) = refs
        pad = lax.broadcasted_iota(jnp.int32, (8, 128), 0)
        start = jnp.where(pad == 0, NONE, 0.0).astype(BF16)
        for b in range(out_ref.shape[0]):
            out_ref[b, 0:128, :] = jnp.zeros((128, 128), BF16)
            out_ref[b, 128:136, :] = start
    else:
        msg_ref, out_ref = refs
        out_ref[...] = msg_ref[...]
    for r in range(SLOTS):
        code = codes_ref[first + r]

        @pl.when(code > 0)
        def _():
            b = (code - 1) >> 5
            peak, denom = stats_ref[r, 0:1, :], stats_ref[r, 1:2, :]
            stats = out_ref[b, 128:136, :].astype(F32)
            m_old = stats[0:1] + stats[1:2] + stats[2:3]
            l_old = stats[3:4] + stats[4:5] + stats[5:6]
            m_new = jnp.maximum(m_old, peak)
            keep = jnp.exp(m_old - m_new)
            gain = jnp.exp(peak - m_new)
            l_new = l_old * keep + denom * gain
            zero = jnp.zeros((2, 128), F32)
            fresh = jnp.concatenate(split3(m_new) + split3(l_new) + (zero,), axis=0)
            out_ref[b, 128:136, :] = fresh.astype(BF16)
            mixed = out_ref[b, 0:128, :].astype(F32) * keep + sums_ref[r] * gain
            out_ref[b, 0:128, :] = mixed.astype(BF16)


def merge(part, blocks, msg=None):
    (sums, stats, codes), n = part
    whole = pl.BlockSpec(memory_space=VMEM)
    scalars = pl.BlockSpec(memory_space=pltpu.SMEM)
    more = () if msg is None else (msg,)
    return pl.pallas_call(
        functools.partial(merge_body, n * SLOTS, msg is None),
        grid=(1,),
        in_specs=[
            scalars,
            pl.BlockSpec((SLOTS, 128, 128), lambda i: (n, 0, 0)),
            pl.BlockSpec((SLOTS, 8, 128), lambda i: (n, 0, 0)),
        ]
        + [pl.BlockSpec((blocks, 136, 128), lambda i: (0, 0, 0))] * len(more),
        out_specs=pl.BlockSpec((blocks, 136, 128), lambda i: (0, 0, 0)),
        out_shape=jax.ShapeDtypeStruct((blocks, 136, 128), BF16),
        compiler_params=params(8),
        cost_estimate=cost(100 * MIB, 900 * 1024),
        name="merge",
    )(codes, sums, stats, *more)


def finish_body(a_ref, b_ref, lg_ref, *refs):
    normed, out_ref = refs[:-1], refs[-1]
    per = normed[0].shape[0]
    for b in range(a_ref.shape[0]):
        sa = a_ref[b, 128:136, :].astype(F32)
        sb = b_ref[b, 128:136, :].astype(F32)
        ma, mb = (s[0:1] + s[1:2] + s[2:3] for s in (sa, sb))
        la, lb = (s[3:4] + s[4:5] + s[5:6] for s in (sa, sb))
        peak = jnp.maximum(ma, mb)
        ga, gb = jnp.exp(ma - peak), jnp.exp(mb - peak)
        denom = la * ga + lb * gb
        sums = a_ref[b, 0:128, :].astype(F32) * ga + b_ref[b, 0:128, :].astype(F32) * gb
        retrieved = (sums / denom).T
        lg = lg_ref[b * BLOCK : (b + 1) * BLOCK, :]
        gate = jax.nn.sigmoid(jnp.concatenate([lg[:, 4:5], lg[:, 5:6]], axis=0))
        mixed = (normed[b // per][b % per] + gate * retrieved).astype(BF16)
        for h in range(2):
            out_ref[b * BLOCK : (b + 1) * BLOCK, h * 128 : (h + 1) * 128] = mixed[
                h * BLOCK : (h + 1) * BLOCK
            ]


def finish(a, b, logits, normed):
    rows = logits.shape[0]
    return pl.pallas_call(
        finish_body,
        out_shape=jax.ShapeDtypeStruct((rows, 256), BF16),
        compiler_params=params(16),
        cost_estimate=cost(100 * MIB, 2 * MIB),
        name="finish",
    )(a, b, logits, *normed)


def per_device(
    tokens,
    owners,
    entries,
    store,
    mixer_query_weight,
    mixer_key_weight,
    mixer_value_weight,
    strength_weight,
    decay_weight,
    head_decay_rate,
    extra_forgetting_exponent,
    output_norm_gain,
    retrieval_query_weight,
    passage_key_weight,
    passage_value_weight,
    retrieval_gate_weight,
):
    devices = lax.axis_size("st")
    me = lax.axis_index("st")
    core = lax.rem(me, 2)
    reach = devices // 4
    blocks = owners.shape[0]
    passages = store.shape[0]

    out_pairs = [(i, (i + (2 if i % 2 == 0 else -2)) % devices) for i in range(devices)]
    back_pairs = [(j, i) for i, j in out_pairs]
    mate_pairs = [(i, i ^ 1) for i in range(devices)]

    def out(x):
        return lax.ppermute(x, "st", out_pairs)

    def back(x):
        return lax.ppermute(x, "st", back_pairs)

    def mate(x):
        return lax.ppermute(x, "st", mate_pairs)

    query = query_message(tokens, retrieval_query_weight, owners.T, entries.T)
    own = {0: query}
    other = {}
    gain = output_norm_gain.reshape(1, 128)
    extra = extra_forgetting_exponent.T
    where_own = jnp.stack([me // 2, core])
    part = {}

    def compute_parts(names, after):
        messages = [(own if lane == "own" else other)[h] for lane, h in names]
        messages[-1] = tie(messages[-1], after)
        result = parts(where_own, messages, kv_own, kv_mate)
        for n, name in enumerate(names):
            part[name] = (result, n)
        return result[1]

    own[1] = out(query)
    other[0] = mate(query)
    kv_own = project_passages(
        tie(store, own[0]), passage_key_weight, passage_value_weight, 0, passages
    )
    other[1] = out(other[0])
    own[1] = tie(own[1], kv_own)
    kv_mate = mate(kv_own)
    q, k, v, logits = mixer_inputs(
        tie(tokens, kv_own),
        mixer_query_weight,
        mixer_key_weight,
        mixer_value_weight,
        strength_weight.T,
        decay_weight.T,
        retrieval_gate_weight.T,
    )
    last = logits
    plan = {
        ("other", 1): None,
        ("own", 3): [("own", 0), ("own", 1), ("other", 1), ("own", 2)],
        ("own", 5): [("other", 2), ("own", 3), ("other", 3), ("own", 4)],
        ("own", 7): [("other", 4), ("own", 5), ("other", 5), ("own", 6)],
    }
    for h in range(1, reach):
        for key, lane in (("own", own), ("other", other)):
            arrived = lane[h]
            if (key, h) == ("other", 1):
                arrived = tie(arrived, last)
            lane[h] = arrived
            if h + 1 < reach or lane is own:
                lane[h + 1] = out(arrived)
            if (key, h) in plan and plan[(key, h)]:
                last = compute_parts(plan[(key, h)], last)
                if h + 1 < reach or lane is own:
                    lane[h + 1] = tie(lane[h + 1], last)
    last = compute_parts([("other", reach - 2), ("own", reach - 1)], last)
    last = compute_parts([("other", reach - 1)], last)

    normed = []
    number = 2
    state = jnp.zeros((2, 128, 128), F32)

    def mixer_step(after):
        nonlocal state
        n = len(normed)
        if n * number >= blocks:
            return after
        result, state = mixer(
            q, k, v, logits, extra, head_decay_rate, gain, tie(state, after), n * number, number
        )
        normed.append(result)
        return state

    last = merge(part[("other", reach - 1)], blocks)
    msg_other = back(last)
    last = compute_parts([("own", reach)], last)
    last = merge(part[("own", reach)], blocks)
    msg_own = back(last)
    for h in range(reach - 2, 0, -1):
        last = merge(part[("other", h)], blocks, tie(msg_other, last))
        msg_other = back(last)
        last = merge(part[("own", h + 1)], blocks, tie(msg_own, last))
        msg_own = back(last)
        last = mixer_step(last)
    while len(normed) * number < blocks:
        last = mixer_step(last)
    msg_other = mate(tie(msg_other, last))
    last = merge(part[("own", 1)], blocks, msg_own)
    msg_own = back(last)
    msg_own = merge(part[("own", 0)], blocks, msg_own)
    return finish(msg_own, msg_other, logits, normed)


def solution(mesh):
    return jax.shard_map(
        per_device,
        mesh=mesh,
        in_specs=(
            P(("grp", "st"), None),
            P(("grp", "st"), None),
            P(("grp", "st"), None),
            P(("grp", "st"), None, None),
            P(None, "tp"),
            P(None, "tp"),
            P(None, "tp"),
            P(None, "tp"),
            P(None, "tp"),
            P("tp"),
            P(("grp", "st"), "tp"),
            P(),
            P(None, "tp"),
            P(None, "tp"),
            P(None, "tp"),
            P(None, "tp"),
        ),
        out_specs=P(("grp", "st"), "tp"),
        check_vma=False,
    )
```

```python
import functools

import jax
import jax.numpy as jnp
from jax import lax
from jax.experimental import pallas as pl
from jax.experimental.pallas import tpu as pltpu
from jax.sharding import PartitionSpec as P


BLOCK = 64
SLOTS = 4
EPS = 1e-06
NONE = -1e30
MIB = 1024 * 1024
F32 = jnp.float32
BF16 = jnp.bfloat16
VMEM = pltpu.VMEM


def nt(left, right):
    return lax.dot_general(left, right, (((1,), (1,)), ((), ())), preferred_element_type=F32)


def nn(left, right):
    return jnp.dot(left, right, preferred_element_type=F32)


def tn(left, right):
    return lax.dot_general(left, right, (((0,), (0,)), ((), ())), preferred_element_type=F32)


def params(limit, **more):
    return pltpu.CompilerParams(vmem_limit_bytes=limit * MIB, **more)


def cost(flops, size, trans=0):
    return pl.CostEstimate(flops=flops, bytes_accessed=size, transcendentals=trans)


def query_body(x_hbm, w_hbm, owners_ref, entries_ref, out_ref, x_buf, w_buf, sems):
    tiles, rows, _ = x_buf.shape
    load_w = pltpu.make_async_copy(w_hbm, w_buf, sems.at[tiles])
    loads = [
        pltpu.make_async_copy(x_hbm.at[pl.ds(i * rows, rows)], x_buf.at[i], sems.at[i])
        for i in range(tiles)
    ]
    load_w.start()
    for load in loads:
        load.start()
    per, count = owners_ref.shape
    blocks = tiles * rows // BLOCK
    names = jnp.concatenate([owners_ref[...], entries_ref[...]], axis=0).astype(F32)
    out_ref[blocks * 128 :, :] = jnp.zeros((2 * per, 128), BF16)
    out_ref[blocks * 128 :, 0:count] = names.astype(BF16)
    load_w.wait()
    for i in range(tiles):
        loads[i].wait()
        q = nn(x_buf[i], w_buf[...]).astype(BF16)
        for n in range(rows // BLOCK):
            at = (i * rows // BLOCK + n) * 128
            for h in range(2):
                out_ref[at + h * BLOCK : at + (h + 1) * BLOCK, :] = q[
                    n * BLOCK : (n + 1) * BLOCK, h * 128 : (h + 1) * 128
                ]


def query_message(x, w, owners, entries, tiles=4):
    rows, depth = x.shape
    hbm = pl.BlockSpec(memory_space=pltpu.HBM)
    whole = pl.BlockSpec(memory_space=VMEM)
    return pl.pallas_call(
        query_body,
        in_specs=[hbm, hbm, whole, whole],
        out_specs=whole,
        out_shape=jax.ShapeDtypeStruct((rows * 2 + 8, 128), BF16),
        scratch_shapes=[
            VMEM((tiles, rows // tiles, depth), BF16),
            VMEM(w.shape, BF16),
            pltpu.SemaphoreType.DMA((tiles + 1,)),
        ],
        compiler_params=params(62),
        cost_estimate=cost(2 * rows * depth * 256, 2 * (rows * depth + depth * 256)),
        name="query",
    )(x, w, owners, entries)


def mixed_body(
    x_hbm, wq_hbm, wk_hbm, wv_hbm, ga_ref, gb_ref, gc_ref, after_ref, q_ref, k_ref, v_ref, lg_ref, x_buf, w_buf, sems
):
    load_x = pltpu.make_async_copy(x_hbm, x_buf, sems.at[3])
    loads = [
        pltpu.make_async_copy(w, w_buf.at[i], sems.at[i])
        for i, w in enumerate((wq_hbm, wk_hbm, wv_hbm))
    ]
    load_x.start()
    for load in loads:
        load.start()
    depth = x_buf.shape[1]
    none = jnp.zeros((2, depth), BF16)
    gates = jnp.concatenate([ga_ref[...], gb_ref[...], gc_ref[...], none], axis=0)
    load_x.wait()
    lg_ref[...] = nt(x_buf[...], gates)
    for i, out_ref in enumerate((q_ref, k_ref, v_ref)):
        loads[i].wait()

        def tile(t, _):
            rows = nn(x_buf[pl.ds(t * 128, 128), :], w_buf[i]).astype(BF16)
            for n in range(2):
                for h in range(2):
                    out_ref[2 * t + n, h * BLOCK : (h + 1) * BLOCK, :] = rows[
                        n * BLOCK : (n + 1) * BLOCK, h * 128 : (h + 1) * 128
                    ]
            return 0

        lax.fori_loop(0, x_buf.shape[0] // 128, tile, 0)


def mixer_inputs(x, wq, wk, wv, ga, gb, gc, after):
    rows, depth = x.shape
    hbm = pl.BlockSpec(memory_space=pltpu.HBM)
    whole = pl.BlockSpec(memory_space=VMEM)
    stacked = jax.ShapeDtypeStruct((rows // BLOCK, 128, 128), BF16)
    return pl.pallas_call(
        mixed_body,
        in_specs=[hbm] * 4 + [whole] * 3 + [pl.BlockSpec(memory_space=pl.ANY)],
        out_specs=[whole] * 4,
        out_shape=[stacked] * 3 + [jax.ShapeDtypeStruct((rows, 8), F32)],
        scratch_shapes=[
            VMEM(x.shape, BF16),
            VMEM((3,) + wq.shape, BF16),
            pltpu.SemaphoreType.DMA((4,)),
        ],
        compiler_params=params(60),
        cost_estimate=cost(2 * rows * depth * 768, 2 * (rows * depth + depth * 768)),
        name="mixer_inputs",
    )(x, wq, wk, wv, ga, gb, gc, after)


def passages_body(store_ref, wk_ref, wv_ref, after_ref, out_ref):
    count, rows, depth = store_ref.shape
    flat = store_ref[...].reshape(count * rows, depth)
    keys = nn(flat, wk_ref[...]).astype(BF16)
    values = nn(flat, wv_ref[...]).astype(BF16).astype(F32)
    for p in range(count):
        span = slice(p * rows, (p + 1) * rows)
        for h in range(2):
            out_ref[p, h * rows : (h + 1) * rows, :] = keys[span, h * 128 : (h + 1) * 128]
        stacked = jnp.concatenate([values[span, :128], values[span, 128:]], axis=0)
        out_ref[p, 128:256, :] = stacked.T.astype(BF16)


def project_passages(store, wk, wv, after, per_step=2):
    number, rows, depth = store.shape
    return pl.pallas_call(
        passages_body,
        grid=(number // per_step,),
        in_specs=[
            pl.BlockSpec((per_step, rows, depth), lambda i: (i, 0, 0)),
            pl.BlockSpec(wk.shape, lambda i: (0, 0)),
            pl.BlockSpec(wv.shape, lambda i: (0, 0)),
            pl.BlockSpec(memory_space=pl.ANY),
        ],
        out_specs=pl.BlockSpec((per_step, 256, 128), lambda i: (i, 0, 0)),
        out_shape=jax.ShapeDtypeStruct((number, 256, 128), BF16),
        compiler_params=params(60),
        cost_estimate=cost(2 * number * rows * depth * 512, 2 * number * rows * depth),
        name="passages",
    )(store, wk, wv, after)


def mixer_body(
    first, q_ref, k_ref, v_ref, lg_ref, ex_ref, rate_ref, gain_ref, s_ref, after_ref, out_ref, s_out_ref
):
    ri = lax.broadcasted_iota(jnp.int32, (128, 128), 0)
    ci = lax.broadcasted_iota(jnp.int32, (128, 128), 1)
    same = (ri >= BLOCK) == (ci >= BLOCK)
    lower = same & (ri >= ci)
    strict = same & (ri > ci)
    upper = same & (ri <= ci)
    diag = ri == ci
    top = lax.broadcasted_iota(jnp.int32, (128, 1), 0) < BLOCK
    rate = jnp.where(top, rate_ref[0], rate_ref[1])
    pieces = []
    for n in range(q_ref.shape[0]):
        lg = lg_ref[n * BLOCK : (n + 1) * BLOCK, :]
        at = (first + n) * BLOCK
        ex = jnp.concatenate([ex_ref[0:1, at : at + BLOCK], ex_ref[1:2, at : at + BLOCK]], axis=1)
        beta = jax.nn.sigmoid(jnp.concatenate([lg[:, 0:1], lg[:, 1:2]], axis=0))
        pre = jnp.concatenate([lg[:, 2:3], lg[:, 3:4]], axis=0)
        extra = jnp.sum(jnp.where(diag, ex, 0.0), axis=1, keepdims=True)
        soft = jnp.maximum(pre, 0.0) + jnp.log1p(jnp.exp(-jnp.abs(pre)))
        g = extra - rate * soft
        g_row = jnp.sum(jnp.where(diag, g, 0.0), axis=0, keepdims=True)
        c = jnp.sum(jnp.where(lower, g_row, 0.0), axis=1, keepdims=True)
        total = jnp.sum(jnp.where(same, g_row, 0.0), axis=1, keepdims=True)
        c_row = jnp.sum(jnp.where(upper, g, 0.0), axis=0, keepdims=True)
        damping = jnp.where(lower, jnp.exp(jnp.where(lower, c - c_row, 0.0)), 0.0)
        q = q_ref[n].astype(F32)
        k = k_ref[n].astype(F32)
        v = v_ref[n].astype(F32)
        q = q * (lax.rsqrt(jnp.sum(q * q, axis=1, keepdims=True) + EPS) * 128**-0.5)
        k = k * lax.rsqrt(jnp.sum(k * k, axis=1, keepdims=True) + EPS)
        kb = k * beta
        decay = jnp.exp(c)
        k16 = k.astype(BF16)
        power = jnp.where(strict, nt(kb.astype(BF16), k16) * damping, 0.0)
        within = (nt(q.astype(BF16), k16) * damping).astype(BF16)
        inverse = jnp.where(diag, 1.0, 0.0) - power
        p16 = power.astype(BF16)
        for _ in range(5):
            p16 = nn(p16, p16).astype(BF16)
            inverse = inverse + nn(inverse.astype(BF16), p16)
        inv16 = inverse.astype(BF16)
        mix = nn(inv16, (kb * decay).astype(BF16)).astype(BF16)
        base = nn(inv16, (v * beta).astype(BF16))
        q_dec = (q * decay).astype(BF16)
        k_tail = (k * jnp.exp(total - c)).astype(BF16)
        pieces.append((mix, base, within, q_dec, k_tail, jnp.exp(total)))
    state = [s_ref[0], s_ref[1]]
    for n, (mix, base, within, q_dec, k_tail, keep) in enumerate(pieces):
        fresh, far = [], []
        for h in range(2):
            rows = slice(h * BLOCK, (h + 1) * BLOCK)
            both = nn(jnp.concatenate([mix[rows], q_dec[rows]], axis=0), state[h].astype(BF16))
            fresh.append(base[rows] - both[:BLOCK])
            far.append(both[BLOCK:])
        f16 = jnp.concatenate(fresh, axis=0).astype(BF16)
        recur = jnp.concatenate(far, axis=0) + nn(within, f16)
        for h in range(2):
            rows = slice(h * BLOCK, (h + 1) * BLOCK)
            state[h] = state[h] * keep[h * BLOCK : h * BLOCK + 1] + tn(k_tail[rows], f16[rows])
        scale = lax.rsqrt(jnp.mean(recur * recur, axis=1, keepdims=True) + EPS)
        out_ref[n] = recur * scale * gain_ref[...]
    s_out_ref[0] = state[0]
    s_out_ref[1] = state[1]


def mixer(q, k, v, logits, extra, rate, gain, state, after, first, number):
    at = first // number
    return pl.pallas_call(
        functools.partial(mixer_body, first),
        grid=(1,),
        in_specs=[
            pl.BlockSpec((number, 128, 128), lambda i: (at, 0, 0)),
            pl.BlockSpec((number, 128, 128), lambda i: (at, 0, 0)),
            pl.BlockSpec((number, 128, 128), lambda i: (at, 0, 0)),
            pl.BlockSpec((number * BLOCK, logits.shape[1]), lambda i: (at, 0)),
            pl.BlockSpec(extra.shape, lambda i: (0, 0)),
            pl.BlockSpec(memory_space=pltpu.SMEM),
            pl.BlockSpec((1, 128), lambda i: (0, 0)),
            pl.BlockSpec((2, 128, 128), lambda i: (0, 0, 0)),
            pl.BlockSpec(memory_space=pl.ANY),
        ],
        out_specs=[
            pl.BlockSpec((number, 128, 128), lambda i: (0, 0, 0)),
            pl.BlockSpec((2, 128, 128), lambda i: (0, 0, 0)),
        ],
        out_shape=[
            jax.ShapeDtypeStruct((number, 128, 128), F32),
            jax.ShapeDtypeStruct((2, 128, 128), F32),
        ],
        compiler_params=params(16),
        cost_estimate=cost(number * 1000 * MIB // 2, number * 300 * 1024),
        name="mixer",
    )(q, k, v, logits, extra, rate, gain, state, after)


def parts_body(count, own_ref, *refs):
    messages, refs = refs[:count], refs[count:]
    (kv_ref, mate_ref, _, sums_ref, stats_ref, codes_ref) = refs
    chip, core = own_ref[0], own_ref[1]
    rows = messages[0].shape[0]
    row = lax.broadcasted_iota(jnp.int32, (8, 128), 0)
    lane = lax.broadcasted_iota(jnp.int32, (8, 128), 1)
    before = (
        lax.broadcasted_iota(jnp.int32, (128, 128), 0) < lax.broadcasted_iota(jnp.int32, (128, 128), 1)
    )
    before = jnp.where(before, 1.0, 0.0).astype(BF16)
    blocks = (rows - 8) // 128
    left = lax.broadcasted_iota(jnp.int32, (BLOCK, 128), 1) < BLOCK
    spots = []
    for n in range(count):
        table = messages[n][rows - 8 :, :].astype(F32)
        entry = jnp.concatenate([table[4:8], table[4:8]], axis=0)
        name = table.astype(jnp.int32)
        hit = ((name >> 1) == chip) & (row < 4) & (lane < blocks)
        ones = jnp.where(hit, 1.0, 0.0)
        rank = nn(ones.astype(BF16), before)
        sums = jnp.sum(ones, axis=1, keepdims=True)
        first, second, third = sums[0:1], sums[1:2], sums[2:3]
        rank = rank + jnp.where(row > 0, first, 0.0)
        rank = rank + jnp.where(row > 1, second, 0.0)
        rank = rank + jnp.where(row > 2, third, 0.0)
        far = jnp.where((name & 1) == core, 0.0, 16.0)
        code = lane.astype(F32) * 32.0 + far + entry + 1.0
        for r in range(SLOTS):
            value = jnp.where(hit & (rank == float(r)), code, 0.0)
            spots.append(jnp.sum(value).astype(jnp.int32))
    for n in range(count):
        for r in range(SLOTS):
            i = n * SLOTS + r
            codes_ref[i] = spots[i]
            spot = jnp.maximum(spots[i] - 1, 0)
            at = pl.multiple_of((spot >> 5) * 128, 128)
            q = messages[n][pl.ds(at, 128), :]
            apart = (spot & 16) != 0
            kv = jnp.where(apart, mate_ref[spot & 15], kv_ref[spot & 15])
            both = nt(kv[0:128], q)
            scores = jnp.where(left, both[:BLOCK], both[BLOCK:]) * 128**-0.5
            peak = jnp.max(scores, axis=0, keepdims=True)
            expo = jnp.exp(scores - peak)
            denom = jnp.sum(expo, axis=0, keepdims=True)
            split = jnp.concatenate(
                [jnp.where(left, expo, 0.0), jnp.where(left, 0.0, expo)], axis=0
            ).astype(BF16)
            sums_ref[i] = nn(kv[128:256], split)
            stats_ref[i] = jnp.where(row == 0, peak, denom)


def parts(own, messages, kv, kv_mate, after):
    count = len(messages)
    total = count * SLOTS
    whole = pl.BlockSpec(memory_space=VMEM)
    scalars = pl.BlockSpec(memory_space=pltpu.SMEM)
    return pl.pallas_call(
        functools.partial(parts_body, count),
        in_specs=[scalars] + [whole] * (count + 2) + [pl.BlockSpec(memory_space=pl.ANY)],
        out_specs=[whole, whole, scalars],
        out_shape=[
            jax.ShapeDtypeStruct((total, 128, 128), F32),
            jax.ShapeDtypeStruct((total, 8, 128), F32),
            jax.ShapeDtypeStruct((total,), jnp.int32),
        ],
        compiler_params=params(12),
        cost_estimate=cost(count * 400 * MIB, count * 500 * 1024),
        name="parts",
    )(own, *messages, kv, kv_mate, after)


def split3(x):
    high = x.astype(BF16)
    rest = x - high.astype(F32)
    mid = rest.astype(BF16)
    low = (rest - mid.astype(F32)).astype(BF16)
    return high.astype(F32), mid.astype(F32), low.astype(F32)


def merge_body(first, empty, codes_ref, sums_ref, stats_ref, after_ref, *refs):
    if empty:
        (out_ref,) = refs
        pad = lax.broadcasted_iota(jnp.int32, (8, 128), 0)
        start = jnp.where(pad == 0, NONE, 0.0).astype(BF16)
        for b in range(out_ref.shape[0]):
            out_ref[b, 0:128, :] = jnp.zeros((128, 128), BF16)
            out_ref[b, 128:136, :] = start
    else:
        msg_ref, out_ref = refs
        out_ref[...] = msg_ref[...]
    for r in range(SLOTS):
        code = codes_ref[first + r]

        @pl.when(code > 0)
        def _():
            b = (code - 1) >> 5
            peak, denom = stats_ref[r, 0:1, :], stats_ref[r, 1:2, :]
            stats = out_ref[b, 128:136, :].astype(F32)
            m_old = stats[0:1] + stats[1:2] + stats[2:3]
            l_old = stats[3:4] + stats[4:5] + stats[5:6]
            m_new = jnp.maximum(m_old, peak)
            keep = jnp.exp(m_old - m_new)
            gain = jnp.exp(peak - m_new)
            l_new = l_old * keep + denom * gain
            zero = jnp.zeros((2, 128), F32)
            fresh = jnp.concatenate(split3(m_new) + split3(l_new) + (zero,), axis=0)
            out_ref[b, 128:136, :] = fresh.astype(BF16)
            mixed = out_ref[b, 0:128, :].astype(F32) * keep + sums_ref[r] * gain
            out_ref[b, 0:128, :] = mixed.astype(BF16)


def merge(part, blocks, after, msg=None):
    (sums, stats, codes), n = part
    whole = pl.BlockSpec(memory_space=VMEM)
    scalars = pl.BlockSpec(memory_space=pltpu.SMEM)
    more = () if msg is None else (msg,)
    return pl.pallas_call(
        functools.partial(merge_body, n * SLOTS, msg is None),
        grid=(1,),
        in_specs=[
            scalars,
            pl.BlockSpec((SLOTS, 128, 128), lambda i: (n, 0, 0)),
            pl.BlockSpec((SLOTS, 8, 128), lambda i: (n, 0, 0)),
            pl.BlockSpec(memory_space=pl.ANY),
        ]
        + [pl.BlockSpec((blocks, 136, 128), lambda i: (0, 0, 0))] * len(more),
        out_specs=pl.BlockSpec((blocks, 136, 128), lambda i: (0, 0, 0)),
        out_shape=jax.ShapeDtypeStruct((blocks, 136, 128), BF16),
        compiler_params=params(8),
        cost_estimate=cost(100 * MIB, 900 * 1024),
        name="merge",
    )(codes, sums, stats, after, *more)


def finish_body(a_ref, b_ref, lg_ref, *refs):
    normed, out_ref = refs[:-1], refs[-1]
    per = normed[0].shape[0]
    for b in range(a_ref.shape[0]):
        sa = a_ref[b, 128:136, :].astype(F32)
        sb = b_ref[b, 128:136, :].astype(F32)
        ma, mb = (s[0:1] + s[1:2] + s[2:3] for s in (sa, sb))
        la, lb = (s[3:4] + s[4:5] + s[5:6] for s in (sa, sb))
        peak = jnp.maximum(ma, mb)
        ga, gb = jnp.exp(ma - peak), jnp.exp(mb - peak)
        denom = la * ga + lb * gb
        sums = a_ref[b, 0:128, :].astype(F32) * ga + b_ref[b, 0:128, :].astype(F32) * gb
        retrieved = (sums / denom).T
        lg = lg_ref[b * BLOCK : (b + 1) * BLOCK, :]
        gate = jax.nn.sigmoid(jnp.concatenate([lg[:, 4:5], lg[:, 5:6]], axis=0))
        mixed = (normed[b // per][b % per] + gate * retrieved).astype(BF16)
        for h in range(2):
            out_ref[b * BLOCK : (b + 1) * BLOCK, h * 128 : (h + 1) * 128] = mixed[
                h * BLOCK : (h + 1) * BLOCK
            ]


def finish(a, b, logits, normed):
    rows = logits.shape[0]
    return pl.pallas_call(
        finish_body,
        out_shape=jax.ShapeDtypeStruct((rows, 256), BF16),
        compiler_params=params(16),
        cost_estimate=cost(100 * MIB, 2 * MIB),
        name="finish",
    )(a, b, logits, *normed)


def per_device(
    tokens,
    owners,
    entries,
    store,
    mixer_query_weight,
    mixer_key_weight,
    mixer_value_weight,
    strength_weight,
    decay_weight,
    head_decay_rate,
    extra_forgetting_exponent,
    output_norm_gain,
    retrieval_query_weight,
    passage_key_weight,
    passage_value_weight,
    retrieval_gate_weight,
):
    devices = lax.axis_size("st")
    me = lax.axis_index("st")
    core = lax.rem(me, 2)
    reach = devices // 4
    blocks = owners.shape[0]

    out_pairs = [(i, (i + (2 if i % 2 == 0 else -2)) % devices) for i in range(devices)]
    back_pairs = [(j, i) for i, j in out_pairs]
    mate_pairs = [(i, i ^ 1) for i in range(devices)]

    def out(x):
        return lax.ppermute(x, "st", out_pairs)

    def back(x):
        return lax.ppermute(x, "st", back_pairs)

    def mate(x):
        return lax.ppermute(x, "st", mate_pairs)

    query = query_message(tokens, retrieval_query_weight, owners.T, entries.T)
    own = {0: query}
    other = {}
    gain = output_norm_gain.reshape(1, 128)
    extra = extra_forgetting_exponent.T
    where_own = jnp.stack([me >> 1, me & 1])
    part = {}

    def compute_parts(names, after):
        messages = [(own if lane == "own" else other)[h] for lane, h in names]
        result = parts(where_own, messages, kv_own, kv_mate, after)
        for n, name in enumerate(names):
            part[name] = (result, n)
        return result[1]

    own[1] = out(query)
    other[0] = mate(query)
    kv_own = project_passages(store, passage_key_weight, passage_value_weight, query)
    kv_mate = mate(kv_own)
    for h in range(1, reach + 1):
        if h > 1:
            own[h] = out(own[h - 1])
        if h < reach:
            other[h] = out(other[h - 1])
    q, k, v, logits = mixer_inputs(
        tokens,
        mixer_query_weight,
        mixer_key_weight,
        mixer_value_weight,
        strength_weight.T,
        decay_weight.T,
        retrieval_gate_weight.T,
        other[1],
    )
    last = compute_parts([("own", 0)], logits)
    for h in range(1, reach):
        last = compute_parts([("own", h), ("other", h)], last)

    normed = []
    number = 2
    state = jnp.zeros((2, 128, 128), F32)

    def mixer_step(after):
        nonlocal state
        n = len(normed)
        if n * number >= blocks:
            return after
        result, state = mixer(
            q, k, v, logits, extra, head_decay_rate, gain, state, after, n * number, number
        )
        normed.append(result)
        return state

    last = merge(part[("other", reach - 1)], blocks, last)
    msg_other = back(last)
    last = compute_parts([("own", reach)], last)
    last = merge(part[("own", reach)], blocks, last)
    msg_own = back(last)
    last = mixer_step(last)
    for h in range(reach - 2, 0, -1):
        last = merge(part[("other", h)], blocks, last, msg_other)
        msg_other = back(last)
        last = merge(part[("own", h + 1)], blocks, last, msg_own)
        msg_own = back(last)
        last = mixer_step(last)
    msg_other = mate(msg_other)
    last = merge(part[("own", 1)], blocks, last, msg_own)
    msg_own = back(last)
    msg_own = merge(part[("own", 0)], blocks, last, msg_own)
    return finish(msg_own, msg_other, logits, normed)


def solution(mesh):
    return jax.shard_map(
        per_device,
        mesh=mesh,
        in_specs=(
            P(("grp", "st"), None),
            P(("grp", "st"), None),
            P(("grp", "st"), None),
            P(("grp", "st"), None, None),
            P(None, "tp"),
            P(None, "tp"),
            P(None, "tp"),
            P(None, "tp"),
            P(None, "tp"),
            P("tp"),
            P(("grp", "st"), "tp"),
            P(),
            P(None, "tp"),
            P(None, "tp"),
            P(None, "tp"),
            P(None, "tp"),
        ),
        out_specs=P(("grp", "st"), "tp"),
        check_vma=False,
    )
```

```python
import functools

import jax
import jax.numpy as jnp
from jax import lax
from jax.experimental import pallas as pl
from jax.experimental.pallas import tpu as pltpu
from jax.sharding import PartitionSpec as P


BLOCK = 64
SLOTS = 4
EPS = 1e-06
NONE = -1e30
MIB = 1024 * 1024
BIG = 52
F32 = jnp.float32
BF16 = jnp.bfloat16
VMEM = pltpu.VMEM


def nt(left, right):
    return lax.dot_general(left, right, (((1,), (1,)), ((), ())), preferred_element_type=F32)


def nn(left, right):
    return jnp.dot(left, right, preferred_element_type=F32)


def tn(left, right):
    return lax.dot_general(left, right, (((0,), (0,)), ((), ())), preferred_element_type=F32)


def params(limit, **more):
    return pltpu.CompilerParams(vmem_limit_bytes=limit * MIB, **more)


def cost(flops, size, trans=0):
    return pl.CostEstimate(flops=flops, bytes_accessed=size, transcendentals=trans)


def query_body(x_hbm, w_hbm, owners_ref, entries_ref, out_ref, x_buf, w_buf, sems):
    tiles, rows, _ = x_buf.shape
    load_w = pltpu.make_async_copy(w_hbm, w_buf, sems.at[tiles])
    loads = [
        pltpu.make_async_copy(x_hbm.at[pl.ds(i * rows, rows)], x_buf.at[i], sems.at[i])
        for i in range(tiles)
    ]
    load_w.start()
    for load in loads:
        load.start()
    per, count = owners_ref.shape
    blocks = tiles * rows // BLOCK
    names = jnp.concatenate([owners_ref[...], entries_ref[...]], axis=0).astype(F32)
    out_ref[blocks * 128 :, :] = jnp.zeros((2 * per, 128), BF16)
    out_ref[blocks * 128 :, 0:count] = names.astype(BF16)
    load_w.wait()
    for i in range(tiles):
        loads[i].wait()
        q = nn(x_buf[i], w_buf[...]).astype(BF16)
        for n in range(rows // BLOCK):
            at = (i * rows // BLOCK + n) * 128
            for h in range(2):
                out_ref[at + h * BLOCK : at + (h + 1) * BLOCK, :] = q[
                    n * BLOCK : (n + 1) * BLOCK, h * 128 : (h + 1) * 128
                ]


def query_message(x, w, owners, entries, tiles=2):
    rows, depth = x.shape
    hbm = pl.BlockSpec(memory_space=pltpu.HBM)
    whole = pl.BlockSpec(memory_space=VMEM)
    return pl.pallas_call(
        query_body,
        in_specs=[hbm, hbm, whole, whole],
        out_specs=whole,
        out_shape=jax.ShapeDtypeStruct((rows * 2 + 8, 128), BF16),
        scratch_shapes=[
            VMEM((tiles, rows // tiles, depth), BF16),
            VMEM(w.shape, BF16),
            pltpu.SemaphoreType.DMA((tiles + 1,)),
        ],
        compiler_params=params(60),
        cost_estimate=cost(2 * rows * depth * 256, 2 * (rows * depth + depth * 256)),
        name="query",
    )(x, w, owners, entries)


def mixed_body(
    x_hbm, wq_hbm, wk_hbm, wv_hbm, ga_ref, gb_ref, gc_ref, after_ref, out_ref, lg_ref, x_buf, w_buf, sems
):
    tiles, tall, depth = x_buf.shape

    def load(t):
        return pltpu.make_async_copy(x_hbm.at[pl.ds(t * tall, tall)], x_buf.at[t], sems.at[t])

    loads = [
        pltpu.make_async_copy(w, w_buf.at[i], sems.at[tiles + i])
        for i, w in enumerate((wq_hbm, wk_hbm, wv_hbm))
    ]
    loads[0].start()
    for t in range(tiles):
        load(t).start()
    loads[1].start()
    loads[2].start()
    none = jnp.zeros((2, depth), BF16)
    gates = jnp.concatenate([ga_ref[...], gb_ref[...], gc_ref[...], none], axis=0)
    for t in range(tiles):
        load(t).wait()
        lg_ref[t * tall : (t + 1) * tall, :] = nt(x_buf[t], gates)
    loads[0].wait()

    def piece(step, _):
        i, t = step // tiles, step % tiles
        rows = nn(x_buf[t], w_buf[i]).astype(BF16)
        for n in range(tall // BLOCK):
            for h in range(2):
                out_ref[i, t * (tall // BLOCK) + n, h * BLOCK : (h + 1) * BLOCK, :] = rows[
                    n * BLOCK : (n + 1) * BLOCK, h * 128 : (h + 1) * 128
                ]
        return 0

    lax.fori_loop(0, tiles, piece, 0)
    loads[1].wait()
    loads[2].wait()
    lax.fori_loop(tiles, 3 * tiles, piece, 0)


def mixer_inputs(x, wq, wk, wv, ga, gb, gc, after, tiles=2):
    rows, depth = x.shape
    hbm = pl.BlockSpec(memory_space=pltpu.HBM)
    whole = pl.BlockSpec(memory_space=VMEM)
    return pl.pallas_call(
        mixed_body,
        in_specs=[hbm] * 4 + [whole] * 3 + [pl.BlockSpec(memory_space=pl.ANY)],
        out_specs=[whole] * 2,
        out_shape=[
            jax.ShapeDtypeStruct((3, rows // BLOCK, 128, 128), BF16),
            jax.ShapeDtypeStruct((rows, 8), F32),
        ],
        scratch_shapes=[
            VMEM((tiles, rows // tiles, depth), BF16),
            VMEM((3,) + wq.shape, BF16),
            pltpu.SemaphoreType.DMA((tiles + 3,)),
        ],
        compiler_params=params(BIG),
        cost_estimate=cost(2 * rows * depth * 768, 2 * (rows * depth + depth * 768)),
        name="mixer_inputs",
    )(x, wq, wk, wv, ga, gb, gc, after)


def passages_body(store_hbm, wk_hbm, wv_hbm, after_ref, out_ref, x_buf, w_buf, sems):
    chunks, tall, _ = x_buf.shape
    rows = out_ref.shape[1] // 4
    count = tall // rows

    def load(i):
        return pltpu.make_async_copy(store_hbm.at[pl.ds(i * tall, tall)], x_buf.at[i], sems.at[i])

    load_k = pltpu.make_async_copy(wk_hbm, w_buf.at[0], sems.at[chunks])
    load_v = pltpu.make_async_copy(wv_hbm, w_buf.at[1], sems.at[chunks + 1])
    load_k.start()
    load(0).start()
    load_v.start()
    for i in range(1, chunks):
        load(i).start()
    load_k.wait()
    load_v.wait()

    def chunk(i, _):
        load(i).wait()
        keys = nn(x_buf[i], w_buf[0]).astype(BF16)
        values = nn(x_buf[i], w_buf[1]).astype(BF16).astype(F32)
        for p in range(count):
            span = slice(p * rows, (p + 1) * rows)
            at = i * count + p
            for h in range(2):
                out_ref[at, h * rows : (h + 1) * rows, :] = keys[span, h * 128 : (h + 1) * 128]
            stacked = jnp.concatenate([values[span, :128], values[span, 128:]], axis=0)
            out_ref[at, 128:256, :] = stacked.T.astype(BF16)
        return 0

    lax.fori_loop(0, chunks, chunk, 0)


def project_passages(store, wk, wv, after, chunks=4):
    number, rows, depth = store.shape
    hbm = pl.BlockSpec(memory_space=pltpu.HBM)
    return pl.pallas_call(
        passages_body,
        in_specs=[hbm, hbm, hbm, pl.BlockSpec(memory_space=pl.ANY)],
        out_specs=pl.BlockSpec(memory_space=VMEM),
        out_shape=jax.ShapeDtypeStruct((number, 256, 128), BF16),
        scratch_shapes=[
            VMEM((chunks, number * rows // chunks, depth), BF16),
            VMEM((2,) + wk.shape, BF16),
            pltpu.SemaphoreType.DMA((chunks + 2,)),
        ],
        compiler_params=params(BIG),
        cost_estimate=cost(2 * number * rows * depth * 512, 2 * number * rows * depth),
        name="passages",
    )(store.reshape(number * rows, depth), wk, wv, after)


def mixer_body(
    first, qkv_ref, lg_ref, ex_ref, rate_ref, gain_ref, s_ref, after_ref, out_ref, s_out_ref
):
    ri = lax.broadcasted_iota(jnp.int32, (128, 128), 0)
    ci = lax.broadcasted_iota(jnp.int32, (128, 128), 1)
    same = (ri >= BLOCK) == (ci >= BLOCK)
    lower = same & (ri >= ci)
    strict = same & (ri > ci)
    upper = same & (ri <= ci)
    diag = ri == ci
    top = lax.broadcasted_iota(jnp.int32, (128, 1), 0) < BLOCK
    rate = jnp.where(top, rate_ref[0], rate_ref[1])
    pieces = []
    for n in range(qkv_ref.shape[1]):
        lg = lg_ref[n * BLOCK : (n + 1) * BLOCK, :]
        at = (first + n) * BLOCK
        ex = jnp.concatenate([ex_ref[0:1, at : at + BLOCK], ex_ref[1:2, at : at + BLOCK]], axis=1)
        beta = jax.nn.sigmoid(jnp.concatenate([lg[:, 0:1], lg[:, 1:2]], axis=0))
        pre = jnp.concatenate([lg[:, 2:3], lg[:, 3:4]], axis=0)
        extra = jnp.sum(jnp.where(diag, ex, 0.0), axis=1, keepdims=True)
        soft = jnp.maximum(pre, 0.0) + jnp.log1p(jnp.exp(-jnp.abs(pre)))
        g = extra - rate * soft
        g_row = jnp.sum(jnp.where(diag, g, 0.0), axis=0, keepdims=True)
        c = jnp.sum(jnp.where(lower, g_row, 0.0), axis=1, keepdims=True)
        total = jnp.sum(jnp.where(same, g_row, 0.0), axis=1, keepdims=True)
        c_row = jnp.sum(jnp.where(upper, g, 0.0), axis=0, keepdims=True)
        damping = jnp.where(lower, jnp.exp(jnp.where(lower, c - c_row, 0.0)), 0.0)
        q = qkv_ref[0, n].astype(F32)
        k = qkv_ref[1, n].astype(F32)
        v = qkv_ref[2, n].astype(F32)
        q = q * (lax.rsqrt(jnp.sum(q * q, axis=1, keepdims=True) + EPS) * 128**-0.5)
        k = k * lax.rsqrt(jnp.sum(k * k, axis=1, keepdims=True) + EPS)
        kb = k * beta
        decay = jnp.exp(c)
        k16 = k.astype(BF16)
        power = jnp.where(strict, nt(kb.astype(BF16), k16) * damping, 0.0)
        within = (nt(q.astype(BF16), k16) * damping).astype(BF16)
        inverse = jnp.where(diag, 1.0, 0.0) - power
        p16 = power.astype(BF16)
        for _ in range(5):
            p16 = nn(p16, p16).astype(BF16)
            inverse = inverse + nn(inverse.astype(BF16), p16)
        inv16 = inverse.astype(BF16)
        mix = nn(inv16, (kb * decay).astype(BF16)).astype(BF16)
        base = nn(inv16, (v * beta).astype(BF16))
        q_dec = (q * decay).astype(BF16)
        k_tail = (k * jnp.exp(total - c)).astype(BF16)
        pieces.append((mix, base, within, q_dec, k_tail, jnp.exp(total)))
    state = [s_ref[0], s_ref[1]]
    for n, (mix, base, within, q_dec, k_tail, keep) in enumerate(pieces):
        fresh, far = [], []
        for h in range(2):
            rows = slice(h * BLOCK, (h + 1) * BLOCK)
            both = nn(jnp.concatenate([mix[rows], q_dec[rows]], axis=0), state[h].astype(BF16))
            fresh.append(base[rows] - both[:BLOCK])
            far.append(both[BLOCK:])
        f16 = jnp.concatenate(fresh, axis=0).astype(BF16)
        recur = jnp.concatenate(far, axis=0) + nn(within, f16)
        for h in range(2):
            rows = slice(h * BLOCK, (h + 1) * BLOCK)
            state[h] = state[h] * keep[h * BLOCK : h * BLOCK + 1] + tn(k_tail[rows], f16[rows])
        scale = lax.rsqrt(jnp.mean(recur * recur, axis=1, keepdims=True) + EPS)
        out_ref[n] = recur * scale * gain_ref[...]
    s_out_ref[0] = state[0]
    s_out_ref[1] = state[1]


def mixer(qkv, logits, extra, rate, gain, state, after, first, number):
    at = first // number
    return pl.pallas_call(
        functools.partial(mixer_body, first),
        grid=(1,),
        in_specs=[
            pl.BlockSpec((3, number, 128, 128), lambda i: (0, at, 0, 0)),
            pl.BlockSpec((number * BLOCK, logits.shape[1]), lambda i: (at, 0)),
            pl.BlockSpec(extra.shape, lambda i: (0, 0)),
            pl.BlockSpec(memory_space=pltpu.SMEM),
            pl.BlockSpec((1, 128), lambda i: (0, 0)),
            pl.BlockSpec((2, 128, 128), lambda i: (0, 0, 0)),
            pl.BlockSpec(memory_space=pl.ANY),
        ],
        out_specs=[
            pl.BlockSpec((number, 128, 128), lambda i: (0, 0, 0)),
            pl.BlockSpec((2, 128, 128), lambda i: (0, 0, 0)),
        ],
        out_shape=[
            jax.ShapeDtypeStruct((number, 128, 128), F32),
            jax.ShapeDtypeStruct((2, 128, 128), F32),
        ],
        compiler_params=params(16),
        cost_estimate=cost(number * 1000 * MIB // 2, number * 300 * 1024),
        name="mixer",
    )(qkv, logits, extra, rate, gain, state, after)


def parts_body(count, own_ref, *refs):
    messages, refs = refs[:count], refs[count:]
    (kv_ref, mate_ref, _, sums_ref, stats_ref, codes_ref) = refs
    chip, core = own_ref[0], own_ref[1]
    rows = messages[0].shape[0]
    row = lax.broadcasted_iota(jnp.int32, (8, 128), 0)
    lane = lax.broadcasted_iota(jnp.int32, (8, 128), 1)
    before = (
        lax.broadcasted_iota(jnp.int32, (128, 128), 0) < lax.broadcasted_iota(jnp.int32, (128, 128), 1)
    )
    before = jnp.where(before, 1.0, 0.0).astype(BF16)
    blocks = (rows - 8) // 128
    left = lax.broadcasted_iota(jnp.int32, (BLOCK, 128), 1) < BLOCK
    spots = []
    for n in range(count):
        table = messages[n][rows - 8 :, :].astype(F32)
        entry = jnp.concatenate([table[4:8], table[4:8]], axis=0)
        name = table.astype(jnp.int32)
        hit = ((name >> 1) == chip) & (row < 4) & (lane < blocks)
        ones = jnp.where(hit, 1.0, 0.0)
        rank = nn(ones.astype(BF16), before)
        sums = jnp.sum(ones, axis=1, keepdims=True)
        first, second, third = sums[0:1], sums[1:2], sums[2:3]
        rank = rank + jnp.where(row > 0, first, 0.0)
        rank = rank + jnp.where(row > 1, second, 0.0)
        rank = rank + jnp.where(row > 2, third, 0.0)
        far = jnp.where((name & 1) == core, 0.0, 16.0)
        code = lane.astype(F32) * 32.0 + far + entry + 1.0
        for r in range(SLOTS):
            value = jnp.where(hit & (rank == float(r)), code, 0.0)
            spots.append(jnp.sum(value).astype(jnp.int32))
    for n in range(count):
        found = []
        for r in range(SLOTS):
            spot = jnp.maximum(spots[n * SLOTS + r] - 1, 0)
            at = pl.multiple_of((spot >> 5) * 128, 128)
            q = messages[n][pl.ds(at, 128), :]
            kv = jnp.where((spot & 16) != 0, mate_ref[spot & 15], kv_ref[spot & 15])
            both = nt(kv[0:128], q)
            scores = jnp.where(left, both[:BLOCK], both[BLOCK:]) * 128**-0.5
            found.append((scores, kv[128:256]))
        weighed = []
        for scores, values in found:
            peak = jnp.max(scores, axis=0, keepdims=True)
            expo = jnp.exp(scores - peak)
            denom = jnp.sum(expo, axis=0, keepdims=True)
            split = jnp.concatenate(
                [jnp.where(left, expo, 0.0), jnp.where(left, 0.0, expo)], axis=0
            ).astype(BF16)
            weighed.append((nn(values, split), jnp.where(row == 0, peak, denom)))
        for r in range(SLOTS):
            i = n * SLOTS + r
            codes_ref[i] = spots[i]
            sums_ref[i], stats_ref[i] = weighed[r]


def parts(own, messages, kv, kv_mate, after):
    count = len(messages)
    total = count * SLOTS
    whole = pl.BlockSpec(memory_space=VMEM)
    scalars = pl.BlockSpec(memory_space=pltpu.SMEM)
    return pl.pallas_call(
        functools.partial(parts_body, count),
        in_specs=[scalars] + [whole] * (count + 2) + [pl.BlockSpec(memory_space=pl.ANY)],
        out_specs=[whole, whole, scalars],
        out_shape=[
            jax.ShapeDtypeStruct((total, 128, 128), F32),
            jax.ShapeDtypeStruct((total, 8, 128), F32),
            jax.ShapeDtypeStruct((total,), jnp.int32),
        ],
        compiler_params=params(12),
        cost_estimate=cost(count * 400 * MIB, count * 500 * 1024),
        name="parts",
    )(own, *messages, kv, kv_mate, after)


def split3(x):
    high = x.astype(BF16)
    rest = x - high.astype(F32)
    mid = rest.astype(BF16)
    low = (rest - mid.astype(F32)).astype(BF16)
    return high.astype(F32), mid.astype(F32), low.astype(F32)


def merge_body(first, empty, codes_ref, sums_ref, stats_ref, after_ref, *refs):
    if empty:
        (out_ref,) = refs
        pad = lax.broadcasted_iota(jnp.int32, (8, 128), 0)
        start = jnp.where(pad == 0, NONE, 0.0).astype(BF16)
        for b in range(out_ref.shape[0]):
            out_ref[b, 0:128, :] = jnp.zeros((128, 128), BF16)
            out_ref[b, 128:136, :] = start
    else:
        msg_ref, out_ref = refs
        out_ref[...] = msg_ref[...]
    for r in range(SLOTS):
        code = codes_ref[first + r]

        @pl.when(code > 0)
        def _():
            b = (code - 1) >> 5
            peak, denom = stats_ref[r, 0:1, :], stats_ref[r, 1:2, :]
            stats = out_ref[b, 128:136, :].astype(F32)
            m_old = stats[0:1] + stats[1:2] + stats[2:3]
            l_old = stats[3:4] + stats[4:5] + stats[5:6]
            m_new = jnp.maximum(m_old, peak)
            keep = jnp.exp(m_old - m_new)
            gain = jnp.exp(peak - m_new)
            l_new = l_old * keep + denom * gain
            zero = jnp.zeros((2, 128), F32)
            fresh = jnp.concatenate(split3(m_new) + split3(l_new) + (zero,), axis=0)
            out_ref[b, 128:136, :] = fresh.astype(BF16)
            mixed = out_ref[b, 0:128, :].astype(F32) * keep + sums_ref[r] * gain
            out_ref[b, 0:128, :] = mixed.astype(BF16)


def merge(part, blocks, after, msg=None):
    (sums, stats, codes), n = part
    whole = pl.BlockSpec(memory_space=VMEM)
    scalars = pl.BlockSpec(memory_space=pltpu.SMEM)
    more = () if msg is None else (msg,)
    return pl.pallas_call(
        functools.partial(merge_body, n * SLOTS, msg is None),
        grid=(1,),
        in_specs=[
            scalars,
            pl.BlockSpec((SLOTS, 128, 128), lambda i: (n, 0, 0)),
            pl.BlockSpec((SLOTS, 8, 128), lambda i: (n, 0, 0)),
            pl.BlockSpec(memory_space=pl.ANY),
        ]
        + [pl.BlockSpec((blocks, 136, 128), lambda i: (0, 0, 0))] * len(more),
        out_specs=pl.BlockSpec((blocks, 136, 128), lambda i: (0, 0, 0)),
        out_shape=jax.ShapeDtypeStruct((blocks, 136, 128), BF16),
        compiler_params=params(8),
        cost_estimate=cost(100 * MIB, 900 * 1024),
        name="merge",
    )(codes, sums, stats, after, *more)


def finish_body(a_ref, b_ref, lg_ref, *refs):
    normed, out_ref = refs[:-1], refs[-1]
    per = normed[0].shape[0]
    for b in range(a_ref.shape[0]):
        sa = a_ref[b, 128:136, :].astype(F32)
        sb = b_ref[b, 128:136, :].astype(F32)
        ma, mb = (s[0:1] + s[1:2] + s[2:3] for s in (sa, sb))
        la, lb = (s[3:4] + s[4:5] + s[5:6] for s in (sa, sb))
        peak = jnp.maximum(ma, mb)
        ga, gb = jnp.exp(ma - peak), jnp.exp(mb - peak)
        denom = la * ga + lb * gb
        sums = a_ref[b, 0:128, :].astype(F32) * ga + b_ref[b, 0:128, :].astype(F32) * gb
        retrieved = (sums / denom).T
        lg = lg_ref[b * BLOCK : (b + 1) * BLOCK, :]
        gate = jax.nn.sigmoid(jnp.concatenate([lg[:, 4:5], lg[:, 5:6]], axis=0))
        mixed = (normed[b // per][b % per] + gate * retrieved).astype(BF16)
        for h in range(2):
            out_ref[b * BLOCK : (b + 1) * BLOCK, h * 128 : (h + 1) * 128] = mixed[
                h * BLOCK : (h + 1) * BLOCK
            ]


def finish(a, b, logits, normed):
    rows = logits.shape[0]
    return pl.pallas_call(
        finish_body,
        out_shape=jax.ShapeDtypeStruct((rows, 256), BF16),
        compiler_params=params(16),
        cost_estimate=cost(100 * MIB, 2 * MIB),
        name="finish",
    )(a, b, logits, *normed)


def per_device(
    tokens,
    owners,
    entries,
    store,
    mixer_query_weight,
    mixer_key_weight,
    mixer_value_weight,
    strength_weight,
    decay_weight,
    head_decay_rate,
    extra_forgetting_exponent,
    output_norm_gain,
    retrieval_query_weight,
    passage_key_weight,
    passage_value_weight,
    retrieval_gate_weight,
):
    devices = lax.axis_size("st")
    me = lax.axis_index("st")
    core = lax.rem(me, 2)
    reach = devices // 4
    blocks = owners.shape[0]

    out_pairs = [(i, (i + (2 if i % 2 == 0 else -2)) % devices) for i in range(devices)]
    back_pairs = [(j, i) for i, j in out_pairs]
    mate_pairs = [(i, i ^ 1) for i in range(devices)]

    def out(x):
        return lax.ppermute(x, "st", out_pairs)

    def back(x):
        return lax.ppermute(x, "st", back_pairs)

    def mate(x):
        return lax.ppermute(x, "st", mate_pairs)

    query = query_message(tokens, retrieval_query_weight, owners.T, entries.T)
    own = {0: query}
    other = {}
    gain = output_norm_gain.reshape(1, 128)
    extra = extra_forgetting_exponent.T
    where_own = jnp.stack([me >> 1, me & 1])
    part = {}

    def compute_parts(names, after):
        messages = [(own if lane == "own" else other)[h] for lane, h in names]
        result = parts(where_own, messages, kv_own, kv_mate, after)
        for n, name in enumerate(names):
            part[name] = (result, n)
        return result[1]

    own[1] = out(query)
    other[0] = mate(query)
    kv_own = project_passages(store, passage_key_weight, passage_value_weight, query)
    kv_mate = mate(kv_own)
    for h in range(1, reach + 1):
        if h > 1:
            own[h] = out(own[h - 1])
        if h < reach:
            other[h] = out(other[h - 1])
    qkv, logits = mixer_inputs(
        tokens,
        mixer_query_weight,
        mixer_key_weight,
        mixer_value_weight,
        strength_weight.T,
        decay_weight.T,
        retrieval_gate_weight.T,
        other[1],
    )
    last = compute_parts([("own", 0)], logits)
    for h in range(1, reach):
        last = compute_parts([("own", h), ("other", h)], last)

    normed = []
    number = 1
    state = jnp.zeros((2, 128, 128), F32)

    def mixer_step(after):
        nonlocal state
        n = len(normed)
        if n * number >= blocks:
            return after
        result, state = mixer(
            qkv, logits, extra, head_decay_rate, gain, state, after, n * number, number
        )
        normed.append(result)
        return state

    last = merge(part[("other", reach - 1)], blocks, last)
    msg_other = back(last)
    last = compute_parts([("own", reach)], last)
    last = merge(part[("own", reach)], blocks, last)
    msg_own = back(last)
    last = mixer_step(last)
    for h in range(reach - 2, 0, -1):
        last = merge(part[("other", h)], blocks, last, msg_other)
        msg_other = back(last)
        last = merge(part[("own", h + 1)], blocks, last, msg_own)
        msg_own = back(last)
        last = mixer_step(last)
    msg_other = mate(msg_other)
    last = merge(part[("own", 1)], blocks, last, msg_own)
    msg_own = back(last)
    last = mixer_step(last)
    msg_own = merge(part[("own", 0)], blocks, last, msg_own)
    return finish(msg_own, msg_other, logits, normed)


def solution(mesh):
    return jax.shard_map(
        per_device,
        mesh=mesh,
        in_specs=(
            P(("grp", "st"), None),
            P(("grp", "st"), None),
            P(("grp", "st"), None),
            P(("grp", "st"), None, None),
            P(None, "tp"),
            P(None, "tp"),
            P(None, "tp"),
            P(None, "tp"),
            P(None, "tp"),
            P("tp"),
            P(("grp", "st"), "tp"),
            P(),
            P(None, "tp"),
            P(None, "tp"),
            P(None, "tp"),
            P(None, "tp"),
        ),
        out_specs=P(("grp", "st"), "tp"),
        check_vma=False,
    )
```

```python
import functools

import jax
import jax.numpy as jnp
from jax import lax
from jax.experimental import pallas as pl
from jax.experimental.pallas import tpu as pltpu
from jax.sharding import PartitionSpec as P


BLOCK = 64
SLOTS = 4
EPS = 1e-06
NONE = -1e30
MIB = 1024 * 1024
BIG = 52
F32 = jnp.float32
BF16 = jnp.bfloat16
VMEM = pltpu.VMEM


def nt(left, right):
    return lax.dot_general(left, right, (((1,), (1,)), ((), ())), preferred_element_type=F32)


def nn(left, right):
    return jnp.dot(left, right, preferred_element_type=F32)


def tn(left, right):
    return lax.dot_general(left, right, (((0,), (0,)), ((), ())), preferred_element_type=F32)


def params(limit, **more):
    return pltpu.CompilerParams(vmem_limit_bytes=limit * MIB, **more)


def cost(flops, size, trans=0):
    return pl.CostEstimate(flops=flops, bytes_accessed=size, transcendentals=trans)


def query_body(x_hbm, w_hbm, owners_hbm, entries_hbm, out_ref, x_buf, w_buf, owners_ref, entries_ref, sems):
    tiles, rows, _ = x_buf.shape
    load_w = pltpu.make_async_copy(w_hbm, w_buf, sems.at[tiles])
    loads = [
        pltpu.make_async_copy(x_hbm.at[pl.ds(i * rows, rows)], x_buf.at[i], sems.at[i])
        for i in range(tiles)
    ]
    tables = [
        pltpu.make_async_copy(owners_hbm, owners_ref, sems.at[tiles + 1]),
        pltpu.make_async_copy(entries_hbm, entries_ref, sems.at[tiles + 2]),
    ]
    load_w.start()
    for load in loads + tables:
        load.start()
    per, count = owners_ref.shape
    blocks = tiles * rows // BLOCK
    for table in tables:
        table.wait()
    names = jnp.concatenate([owners_ref[...] + 1, entries_ref[...]], axis=0).astype(F32)
    out_ref[blocks * 128 :, :] = jnp.zeros((2 * per, 128), BF16)
    out_ref[blocks * 128 :, 0:count] = names.astype(BF16)
    load_w.wait()
    for i in range(tiles):
        loads[i].wait()
        q = nn(x_buf[i], w_buf[...]).astype(BF16)
        for n in range(rows // BLOCK):
            at = (i * rows // BLOCK + n) * 128
            for h in range(2):
                out_ref[at + h * BLOCK : at + (h + 1) * BLOCK, :] = q[
                    n * BLOCK : (n + 1) * BLOCK, h * 128 : (h + 1) * 128
                ]


def query_message(x, w, owners, entries, tiles=2):
    rows, depth = x.shape
    hbm = pl.BlockSpec(memory_space=pltpu.HBM)
    whole = pl.BlockSpec(memory_space=VMEM)
    return pl.pallas_call(
        query_body,
        in_specs=[hbm] * 4,
        out_specs=whole,
        out_shape=jax.ShapeDtypeStruct((rows * 2 + 8, 128), BF16),
        scratch_shapes=[
            VMEM((tiles, rows // tiles, depth), BF16),
            VMEM(w.shape, BF16),
            VMEM(owners.shape, jnp.int32),
            VMEM(entries.shape, jnp.int32),
            pltpu.SemaphoreType.DMA((tiles + 3,)),
        ],
        compiler_params=params(BIG + 1),
        cost_estimate=cost(2 * rows * depth * 256, 2 * (rows * depth + depth * 256)),
        name="query",
    )(x, w, owners, entries)


def mixed_body(
    x_hbm, wq_hbm, wk_hbm, wv_hbm, ga_ref, gb_ref, gc_ref, after_ref, out_ref, lg_ref, x_buf, w_buf, sems
):
    tiles, tall, depth = x_buf.shape

    def load(t):
        return pltpu.make_async_copy(x_hbm.at[pl.ds(t * tall, tall)], x_buf.at[t], sems.at[t])

    loads = [
        pltpu.make_async_copy(w, w_buf.at[i], sems.at[tiles + i])
        for i, w in enumerate((wq_hbm, wk_hbm, wv_hbm))
    ]
    loads[0].start()
    for t in range(tiles):
        load(t).start()
    loads[1].start()
    loads[2].start()
    none = jnp.zeros((2, depth), BF16)
    gates = jnp.concatenate([ga_ref[...], gb_ref[...], gc_ref[...], none], axis=0)
    for t in range(tiles):
        load(t).wait()
        lg_ref[t * tall : (t + 1) * tall, :] = nt(x_buf[t], gates)
    loads[0].wait()

    def piece(step, _):
        i, t = step // tiles, step % tiles
        rows = nn(x_buf[t], w_buf[i]).astype(BF16)
        for n in range(tall // BLOCK):
            for h in range(2):
                out_ref[i, t * (tall // BLOCK) + n, h * BLOCK : (h + 1) * BLOCK, :] = rows[
                    n * BLOCK : (n + 1) * BLOCK, h * 128 : (h + 1) * 128
                ]
        return 0

    lax.fori_loop(0, tiles, piece, 0)
    loads[1].wait()
    loads[2].wait()
    lax.fori_loop(tiles, 3 * tiles, piece, 0)


def mixer_inputs(x, wq, wk, wv, ga, gb, gc, after, tiles=2):
    rows, depth = x.shape
    hbm = pl.BlockSpec(memory_space=pltpu.HBM)
    whole = pl.BlockSpec(memory_space=VMEM)
    return pl.pallas_call(
        mixed_body,
        in_specs=[hbm] * 4 + [whole] * 3 + [pl.BlockSpec(memory_space=pl.ANY)],
        out_specs=[whole] * 2,
        out_shape=[
            jax.ShapeDtypeStruct((3, rows // BLOCK, 128, 128), BF16),
            jax.ShapeDtypeStruct((rows, 8), F32),
        ],
        scratch_shapes=[
            VMEM((tiles, rows // tiles, depth), BF16),
            VMEM((3,) + wq.shape, BF16),
            pltpu.SemaphoreType.DMA((tiles + 3,)),
        ],
        compiler_params=params(BIG),
        cost_estimate=cost(2 * rows * depth * 768, 2 * (rows * depth + depth * 768)),
        name="mixer_inputs",
    )(x, wq, wk, wv, ga, gb, gc, after)


def passages_body(store_hbm, wk_hbm, wv_hbm, after_ref, out_ref, x_buf, w_buf, sems):
    chunks, tall, _ = x_buf.shape
    rows = out_ref.shape[1] // 4
    count = tall // rows

    def load(i):
        return pltpu.make_async_copy(store_hbm.at[pl.ds(i * tall, tall)], x_buf.at[i], sems.at[i])

    load_k = pltpu.make_async_copy(wk_hbm, w_buf.at[0], sems.at[chunks])
    load_v = pltpu.make_async_copy(wv_hbm, w_buf.at[1], sems.at[chunks + 1])
    load_k.start()
    load(0).start()
    load_v.start()
    for i in range(1, chunks):
        load(i).start()
    load_k.wait()
    load_v.wait()

    def chunk(i, _):
        load(i).wait()
        keys = nn(x_buf[i], w_buf[0]).astype(BF16)
        values = nn(x_buf[i], w_buf[1]).astype(BF16).astype(F32)
        for p in range(count):
            span = slice(p * rows, (p + 1) * rows)
            at = i * count + p
            for h in range(2):
                out_ref[at, h * rows : (h + 1) * rows, :] = keys[span, h * 128 : (h + 1) * 128]
            stacked = jnp.concatenate([values[span, :128], values[span, 128:]], axis=0)
            out_ref[at, 128:256, :] = stacked.T.astype(BF16)
        return 0

    lax.fori_loop(0, chunks, chunk, 0)


def project_passages(store, wk, wv, after, chunks=4):
    number, rows, depth = store.shape
    hbm = pl.BlockSpec(memory_space=pltpu.HBM)
    return pl.pallas_call(
        passages_body,
        in_specs=[hbm, hbm, hbm, pl.BlockSpec(memory_space=pl.ANY)],
        out_specs=pl.BlockSpec(memory_space=VMEM),
        out_shape=jax.ShapeDtypeStruct((number, 256, 128), BF16),
        scratch_shapes=[
            VMEM((chunks, number * rows // chunks, depth), BF16),
            VMEM((2,) + wk.shape, BF16),
            pltpu.SemaphoreType.DMA((chunks + 2,)),
        ],
        compiler_params=params(BIG),
        cost_estimate=cost(2 * number * rows * depth * 512, 2 * number * rows * depth),
        name="passages",
    )(store.reshape(number * rows, depth), wk, wv, after)


def mixer_body(
    first, qkv_ref, lg_ref, ex_ref, rate_ref, gain_ref, s_ref, after_ref, out_ref, s_out_ref
):
    ri = lax.broadcasted_iota(jnp.int32, (128, 128), 0)
    ci = lax.broadcasted_iota(jnp.int32, (128, 128), 1)
    same = (ri >= BLOCK) == (ci >= BLOCK)
    lower = same & (ri >= ci)
    strict = same & (ri > ci)
    upper = same & (ri <= ci)
    diag = ri == ci
    top = lax.broadcasted_iota(jnp.int32, (128, 1), 0) < BLOCK
    rate = jnp.where(top, rate_ref[0], rate_ref[1])
    pieces = []
    for n in range(qkv_ref.shape[1]):
        lg = lg_ref[n * BLOCK : (n + 1) * BLOCK, :]
        at = (first + n) * BLOCK
        ex = jnp.concatenate([ex_ref[0:1, at : at + BLOCK], ex_ref[1:2, at : at + BLOCK]], axis=1)
        beta = jax.nn.sigmoid(jnp.concatenate([lg[:, 0:1], lg[:, 1:2]], axis=0))
        pre = jnp.concatenate([lg[:, 2:3], lg[:, 3:4]], axis=0)
        extra = jnp.sum(jnp.where(diag, ex, 0.0), axis=1, keepdims=True)
        soft = jnp.maximum(pre, 0.0) + jnp.log1p(jnp.exp(-jnp.abs(pre)))
        g = extra - rate * soft
        g_row = jnp.sum(jnp.where(diag, g, 0.0), axis=0, keepdims=True)
        c = jnp.sum(jnp.where(lower, g_row, 0.0), axis=1, keepdims=True)
        total = jnp.sum(jnp.where(same, g_row, 0.0), axis=1, keepdims=True)
        c_row = jnp.sum(jnp.where(upper, g, 0.0), axis=0, keepdims=True)
        damping = jnp.where(lower, jnp.exp(jnp.where(lower, c - c_row, 0.0)), 0.0)
        q = qkv_ref[0, n].astype(F32)
        k = qkv_ref[1, n].astype(F32)
        v = qkv_ref[2, n].astype(F32)
        q = q * (lax.rsqrt(jnp.sum(q * q, axis=1, keepdims=True) + EPS) * 128**-0.5)
        k = k * lax.rsqrt(jnp.sum(k * k, axis=1, keepdims=True) + EPS)
        kb = k * beta
        decay = jnp.exp(c)
        k16 = k.astype(BF16)
        power = jnp.where(strict, nt(kb.astype(BF16), k16) * damping, 0.0)
        within = (nt(q.astype(BF16), k16) * damping).astype(BF16)
        inverse = jnp.where(diag, 1.0, 0.0) - power
        p16 = power.astype(BF16)
        for _ in range(5):
            p16 = nn(p16, p16).astype(BF16)
            inverse = inverse + nn(inverse.astype(BF16), p16)
        inv16 = inverse.astype(BF16)
        mix = nn(inv16, (kb * decay).astype(BF16)).astype(BF16)
        base = nn(inv16, (v * beta).astype(BF16))
        q_dec = (q * decay).astype(BF16)
        k_tail = (k * jnp.exp(total - c)).astype(BF16)
        pieces.append((mix, base, within, q_dec, k_tail, jnp.exp(total)))
    state = [s_ref[0], s_ref[1]]
    for n, (mix, base, within, q_dec, k_tail, keep) in enumerate(pieces):
        fresh, far = [], []
        for h in range(2):
            rows = slice(h * BLOCK, (h + 1) * BLOCK)
            both = nn(jnp.concatenate([mix[rows], q_dec[rows]], axis=0), state[h].astype(BF16))
            fresh.append(base[rows] - both[:BLOCK])
            far.append(both[BLOCK:])
        f16 = jnp.concatenate(fresh, axis=0).astype(BF16)
        recur = jnp.concatenate(far, axis=0) + nn(within, f16)
        for h in range(2):
            rows = slice(h * BLOCK, (h + 1) * BLOCK)
            state[h] = state[h] * keep[h * BLOCK : h * BLOCK + 1] + tn(k_tail[rows], f16[rows])
        scale = lax.rsqrt(jnp.mean(recur * recur, axis=1, keepdims=True) + EPS)
        out_ref[n] = recur * scale * gain_ref[...]
    s_out_ref[0] = state[0]
    s_out_ref[1] = state[1]


def mixer(qkv, logits, extra, rate, gain, state, after, first, number):
    at = first // number
    return pl.pallas_call(
        functools.partial(mixer_body, first),
        grid=(1,),
        in_specs=[
            pl.BlockSpec((3, number, 128, 128), lambda i: (0, at, 0, 0)),
            pl.BlockSpec((number * BLOCK, logits.shape[1]), lambda i: (at, 0)),
            pl.BlockSpec(extra.shape, lambda i: (0, 0)),
            pl.BlockSpec(memory_space=pltpu.SMEM),
            pl.BlockSpec((1, 128), lambda i: (0, 0)),
            pl.BlockSpec((2, 128, 128), lambda i: (0, 0, 0)),
            pl.BlockSpec(memory_space=pl.ANY),
        ],
        out_specs=[
            pl.BlockSpec((number, 128, 128), lambda i: (0, 0, 0)),
            pl.BlockSpec((2, 128, 128), lambda i: (0, 0, 0)),
        ],
        out_shape=[
            jax.ShapeDtypeStruct((number, 128, 128), F32),
            jax.ShapeDtypeStruct((2, 128, 128), F32),
        ],
        compiler_params=params(16),
        cost_estimate=cost(number * 1000 * MIB // 2, number * 300 * 1024),
        name="mixer",
    )(qkv, logits, extra, rate, gain, state, after)


def parts_body(count, own_ref, *refs):
    messages, refs = refs[:count], refs[count:]
    (kv_ref, mate_ref, _, sums_ref, stats_ref, codes_ref) = refs
    chip, core = own_ref[0], own_ref[1]
    rows = messages[0].shape[0]
    row = lax.broadcasted_iota(jnp.int32, (8, 128), 0)
    lane = lax.broadcasted_iota(jnp.int32, (8, 128), 1)
    before = (
        lax.broadcasted_iota(jnp.int32, (128, 128), 0) < lax.broadcasted_iota(jnp.int32, (128, 128), 1)
    )
    before = jnp.where(before, 1.0, 0.0).astype(BF16)
    blocks = (rows - 8) // 128
    left = lax.broadcasted_iota(jnp.int32, (BLOCK, 128), 1) < BLOCK
    spots = []
    for n in range(count):
        table = messages[n][rows - 8 :, :].astype(F32)
        entry = jnp.concatenate([table[4:8], table[4:8]], axis=0)
        name = table.astype(jnp.int32) - 1
        hit = ((name >> 1) == chip) & (row < 4) & (lane < blocks)
        ones = jnp.where(hit, 1.0, 0.0)
        rank = nn(ones.astype(BF16), before)
        sums = jnp.sum(ones, axis=1, keepdims=True)
        first, second, third = sums[0:1], sums[1:2], sums[2:3]
        rank = rank + jnp.where(row > 0, first, 0.0)
        rank = rank + jnp.where(row > 1, second, 0.0)
        rank = rank + jnp.where(row > 2, third, 0.0)
        far = jnp.where((name & 1) == core, 0.0, 16.0)
        code = lane.astype(F32) * 32.0 + far + entry + 1.0
        for r in range(SLOTS):
            value = jnp.where(hit & (rank == float(r)), code, 0.0)
            spots.append(jnp.sum(value).astype(jnp.int32))
    for n in range(count):
        found = []
        for r in range(SLOTS):
            spot = jnp.maximum(spots[n * SLOTS + r] - 1, 0)
            at = pl.multiple_of((spot >> 5) * 128, 128)
            q = messages[n][pl.ds(at, 128), :]
            kv = jnp.where((spot & 16) != 0, mate_ref[spot & 15], kv_ref[spot & 15])
            both = nt(kv[0:128], q)
            scores = jnp.where(left, both[:BLOCK], both[BLOCK:]) * 128**-0.5
            found.append((scores, kv[128:256]))
        weighed = []
        for scores, values in found:
            peak = jnp.max(scores, axis=0, keepdims=True)
            expo = jnp.exp(scores - peak)
            denom = jnp.sum(expo, axis=0, keepdims=True)
            split = jnp.concatenate(
                [jnp.where(left, expo, 0.0), jnp.where(left, 0.0, expo)], axis=0
            ).astype(BF16)
            weighed.append((nn(values, split), jnp.where(row == 0, peak, denom)))
        for r in range(SLOTS):
            i = n * SLOTS + r
            codes_ref[i] = spots[i]
            sums_ref[i], stats_ref[i] = weighed[r]


def parts(own, messages, kv, kv_mate, after):
    count = len(messages)
    total = count * SLOTS
    whole = pl.BlockSpec(memory_space=VMEM)
    scalars = pl.BlockSpec(memory_space=pltpu.SMEM)
    return pl.pallas_call(
        functools.partial(parts_body, count),
        in_specs=[scalars] + [whole] * (count + 2) + [pl.BlockSpec(memory_space=pl.ANY)],
        out_specs=[whole, whole, scalars],
        out_shape=[
            jax.ShapeDtypeStruct((total, 128, 128), F32),
            jax.ShapeDtypeStruct((total, 8, 128), F32),
            jax.ShapeDtypeStruct((total,), jnp.int32),
        ],
        compiler_params=params(12),
        cost_estimate=cost(count * 400 * MIB, count * 500 * 1024),
        name="parts",
    )(own, *messages, kv, kv_mate, after)


def split3(x):
    high = x.astype(BF16)
    rest = x - high.astype(F32)
    mid = rest.astype(BF16)
    low = (rest - mid.astype(F32)).astype(BF16)
    return high.astype(F32), mid.astype(F32), low.astype(F32)


def merge_body(first, start, own_ref, codes_ref, sums_ref, stats_ref, after_ref, *refs):
    out_ref = refs[-1]

    def begin():
        pad = lax.broadcasted_iota(jnp.int32, (8, 128), 0)
        none = jnp.where(pad == 0, NONE, 0.0).astype(BF16)
        for b in range(out_ref.shape[0]):
            out_ref[b, 0:128, :] = jnp.zeros((128, 128), BF16)
            out_ref[b, 128:136, :] = none

    def go_on():
        out_ref[...] = refs[0][...]

    if start == "all":
        begin()
    elif start == "core_0":
        pl.when(own_ref[1] == 0)(begin)
        pl.when(own_ref[1] != 0)(go_on)
    else:
        go_on()
    for r in range(SLOTS):
        code = codes_ref[first + r]

        @pl.when(code > 0)
        def _():
            b = (code - 1) >> 5
            peak, denom = stats_ref[r, 0:1, :], stats_ref[r, 1:2, :]
            stats = out_ref[b, 128:136, :].astype(F32)
            m_old = stats[0:1] + stats[1:2] + stats[2:3]
            l_old = stats[3:4] + stats[4:5] + stats[5:6]
            m_new = jnp.maximum(m_old, peak)
            keep = jnp.exp(m_old - m_new)
            gain = jnp.exp(peak - m_new)
            l_new = l_old * keep + denom * gain
            zero = jnp.zeros((2, 128), F32)
            fresh = jnp.concatenate(split3(m_new) + split3(l_new) + (zero,), axis=0)
            out_ref[b, 128:136, :] = fresh.astype(BF16)
            mixed = out_ref[b, 0:128, :].astype(F32) * keep + sums_ref[r] * gain
            out_ref[b, 0:128, :] = mixed.astype(BF16)


def merge(own, part, blocks, after, msg=None, start="none"):
    (sums, stats, codes), n = part
    whole = pl.BlockSpec(memory_space=VMEM)
    scalars = pl.BlockSpec(memory_space=pltpu.SMEM)
    more = () if msg is None else (msg,)
    return pl.pallas_call(
        functools.partial(merge_body, n * SLOTS, start),
        grid=(1,),
        in_specs=[
            scalars,
            scalars,
            pl.BlockSpec((SLOTS, 128, 128), lambda i: (n, 0, 0)),
            pl.BlockSpec((SLOTS, 8, 128), lambda i: (n, 0, 0)),
            pl.BlockSpec(memory_space=pl.ANY),
        ]
        + [pl.BlockSpec((blocks, 136, 128), lambda i: (0, 0, 0))] * len(more),
        out_specs=pl.BlockSpec((blocks, 136, 128), lambda i: (0, 0, 0)),
        out_shape=jax.ShapeDtypeStruct((blocks, 136, 128), BF16),
        compiler_params=params(8),
        cost_estimate=cost(100 * MIB, 900 * 1024),
        name="merge",
    )(own, codes, sums, stats, after, *more)


def finish_body(a_ref, b_ref, lg_ref, *refs):
    normed, out_ref = refs[:-1], refs[-1]
    per = normed[0].shape[0]
    for b in range(a_ref.shape[0]):
        sa = a_ref[b, 128:136, :].astype(F32)
        sb = b_ref[b, 128:136, :].astype(F32)
        ma, mb = (s[0:1] + s[1:2] + s[2:3] for s in (sa, sb))
        la, lb = (s[3:4] + s[4:5] + s[5:6] for s in (sa, sb))
        peak = jnp.maximum(ma, mb)
        ga, gb = jnp.exp(ma - peak), jnp.exp(mb - peak)
        denom = la * ga + lb * gb
        sums = a_ref[b, 0:128, :].astype(F32) * ga + b_ref[b, 0:128, :].astype(F32) * gb
        retrieved = (sums / denom).T
        lg = lg_ref[b * BLOCK : (b + 1) * BLOCK, :]
        gate = jax.nn.sigmoid(jnp.concatenate([lg[:, 4:5], lg[:, 5:6]], axis=0))
        mixed = (normed[b // per][b % per] + gate * retrieved).astype(BF16)
        for h in range(2):
            out_ref[b * BLOCK : (b + 1) * BLOCK, h * 128 : (h + 1) * 128] = mixed[
                h * BLOCK : (h + 1) * BLOCK
            ]


def finish(a, b, logits, normed):
    rows = logits.shape[0]
    return pl.pallas_call(
        finish_body,
        out_shape=jax.ShapeDtypeStruct((rows, 256), BF16),
        compiler_params=params(16),
        cost_estimate=cost(100 * MIB, 2 * MIB),
        name="finish",
    )(a, b, logits, *normed)


def per_device(
    tokens,
    owners,
    entries,
    store,
    mixer_query_weight,
    mixer_key_weight,
    mixer_value_weight,
    strength_weight,
    decay_weight,
    head_decay_rate,
    extra_forgetting_exponent,
    output_norm_gain,
    retrieval_query_weight,
    passage_key_weight,
    passage_value_weight,
    retrieval_gate_weight,
):
    devices = lax.axis_size("st")
    me = lax.axis_index("st")
    core = lax.rem(me, 2)
    reach = devices // 4
    blocks = owners.shape[0]

    step = [2 if i % 2 == 0 else -2 for i in range(devices)]
    ahead = [(i, (i + step[i]) % devices) for i in range(devices)]
    across = [(i ^ 1, j) for i, j in ahead]
    mates = [(i, i ^ 1) for i in range(devices)]

    def send(x, pairs):
        return lax.ppermute(x, "st", pairs)

    def out(x, h, first):
        pairs = first if h == 1 else ahead
        if h == reach:
            pairs = [(i, j) for i, j in pairs if i % 2 == 1]
        return send(x, pairs)

    def back(x, h, first):
        pairs = first if h == 1 else ahead
        if h == reach:
            pairs = [(i, j) for i, j in pairs if i % 2 == 1]
        return send(x, [(j, i) for i, j in pairs])

    query = query_message(tokens, retrieval_query_weight, owners.T, entries.T)
    own = {0: query}
    other = {}
    gain = output_norm_gain.reshape(1, 128)
    extra = extra_forgetting_exponent.T
    where_own = jnp.stack([me >> 1, me & 1])
    part = {}

    def compute_parts(names, after):
        messages = [(own if lane == "own" else other)[h] for lane, h in names]
        result = parts(where_own, messages, kv_own, kv_mate, after)
        for n, name in enumerate(names):
            part[name] = (result, n)
        return result[1]

    own[1] = out(query, 1, ahead)
    other[1] = out(query, 1, across)
    kv_own = project_passages(store, passage_key_weight, passage_value_weight, query)
    kv_mate = send(kv_own, mates)
    for h in range(2, reach + 1):
        own[h] = out(own[h - 1], h, ahead)
        other[h] = out(other[h - 1], h, across)
    qkv, logits = mixer_inputs(
        tokens,
        mixer_query_weight,
        mixer_key_weight,
        mixer_value_weight,
        strength_weight.T,
        decay_weight.T,
        retrieval_gate_weight.T,
        other[1],
    )
    last = compute_parts([("own", 0)], logits)
    for h in range(1, reach):
        last = compute_parts([("own", h), ("other", h)], last)

    normed = []
    number = 1
    state = jnp.zeros((2, 128, 128), F32)

    def mixer_step(after):
        nonlocal state
        n = len(normed)
        if n * number >= blocks:
            return after
        result, state = mixer(
            qkv, logits, extra, head_decay_rate, gain, state, after, n * number, number
        )
        normed.append(result)
        return state

    msg_own = msg_other = None
    for h in range(reach, 0, -1):
        start = {reach: "all", reach - 1: "core_0"}.get(h, "none")
        if h == reach:
            last = compute_parts([("own", h)], last)
        last = merge(where_own, part[("own", h)], blocks, last, msg_own, start)
        msg_own = back(last, h, ahead)
        if h == reach:
            last = compute_parts([("other", h)], last)
        last = merge(where_own, part[("other", h)], blocks, last, msg_other, start)
        msg_other = back(last, h, across)
        last = mixer_step(last)
    while len(normed) * number < blocks:
        last = mixer_step(last)
    msg_own = merge(where_own, part[("own", 0)], blocks, last, msg_own)
    return finish(msg_own, msg_other, logits, normed)


def solution(mesh):
    return jax.shard_map(
        per_device,
        mesh=mesh,
        in_specs=(
            P(("grp", "st"), None),
            P(("grp", "st"), None),
            P(("grp", "st"), None),
            P(("grp", "st"), None, None),
            P(None, "tp"),
            P(None, "tp"),
            P(None, "tp"),
            P(None, "tp"),
            P(None, "tp"),
            P("tp"),
            P(("grp", "st"), "tp"),
            P(),
            P(None, "tp"),
            P(None, "tp"),
            P(None, "tp"),
            P(None, "tp"),
        ),
        out_specs=P(("grp", "st"), "tp"),
        check_vma=False,
    )
```

```python
import functools

import jax
import jax.numpy as jnp
from jax import lax
from jax.experimental import pallas as pl
from jax.experimental.pallas import tpu as pltpu
from jax.sharding import PartitionSpec as P


BLOCK = 64
SLOTS = 4
EPS = 1e-06
NONE = -1e30
MIB = 1024 * 1024
BIG = 52
F32 = jnp.float32
BF16 = jnp.bfloat16
VMEM = pltpu.VMEM


def nt(left, right):
    return lax.dot_general(left, right, (((1,), (1,)), ((), ())), preferred_element_type=F32)


def nn(left, right):
    return jnp.dot(left, right, preferred_element_type=F32)


def tn(left, right):
    return lax.dot_general(left, right, (((0,), (0,)), ((), ())), preferred_element_type=F32)


def params(limit, **more):
    return pltpu.CompilerParams(vmem_limit_bytes=limit * MIB, **more)


def cost(flops, size, trans=0):
    return pl.CostEstimate(flops=flops, bytes_accessed=size, transcendentals=trans)


def query_body(x_hbm, w_hbm, owners_hbm, entries_hbm, out_ref, x_buf, w_buf, owners_ref, entries_ref, sems):
    tiles, rows, _ = x_buf.shape
    load_w = pltpu.make_async_copy(w_hbm, w_buf, sems.at[tiles])
    loads = [
        pltpu.make_async_copy(x_hbm.at[pl.ds(i * rows, rows)], x_buf.at[i], sems.at[i])
        for i in range(tiles)
    ]
    tables = [
        pltpu.make_async_copy(owners_hbm, owners_ref, sems.at[tiles + 1]),
        pltpu.make_async_copy(entries_hbm, entries_ref, sems.at[tiles + 2]),
    ]
    load_w.start()
    for load in loads + tables:
        load.start()
    per, count = owners_ref.shape
    blocks = tiles * rows // BLOCK
    for table in tables:
        table.wait()
    names = jnp.concatenate([owners_ref[...] + 1, entries_ref[...]], axis=0).astype(F32)
    out_ref[blocks * 128 :, :] = jnp.zeros((2 * per, 128), BF16)
    out_ref[blocks * 128 :, 0:count] = names.astype(BF16)
    load_w.wait()
    for i in range(tiles):
        loads[i].wait()
        q = nn(x_buf[i], w_buf[...]).astype(BF16)
        for n in range(rows // BLOCK):
            at = (i * rows // BLOCK + n) * 128
            for h in range(2):
                out_ref[at + h * BLOCK : at + (h + 1) * BLOCK, :] = q[
                    n * BLOCK : (n + 1) * BLOCK, h * 128 : (h + 1) * 128
                ]


def query_message(x, w, owners, entries, tiles=2):
    rows, depth = x.shape
    hbm = pl.BlockSpec(memory_space=pltpu.HBM)
    whole = pl.BlockSpec(memory_space=VMEM)
    return pl.pallas_call(
        query_body,
        in_specs=[hbm] * 4,
        out_specs=whole,
        out_shape=jax.ShapeDtypeStruct((rows * 2 + 8, 128), BF16),
        scratch_shapes=[
            VMEM((tiles, rows // tiles, depth), BF16),
            VMEM(w.shape, BF16),
            VMEM(owners.shape, jnp.int32),
            VMEM(entries.shape, jnp.int32),
            pltpu.SemaphoreType.DMA((tiles + 3,)),
        ],
        compiler_params=params(BIG + 1),
        cost_estimate=cost(2 * rows * depth * 256, 2 * (rows * depth + depth * 256)),
        name="query",
    )(x, w, owners, entries)


def mixed_body(
    x_hbm, wq_hbm, wk_hbm, wv_hbm, ga_ref, gb_ref, gc_ref, after_ref, out_ref, lg_ref, x_buf, w_buf, sems
):
    tiles, tall, depth = x_buf.shape

    def load(t):
        return pltpu.make_async_copy(x_hbm.at[pl.ds(t * tall, tall)], x_buf.at[t], sems.at[t])

    loads = [
        pltpu.make_async_copy(w, w_buf.at[i], sems.at[tiles + i])
        for i, w in enumerate((wq_hbm, wk_hbm, wv_hbm))
    ]
    loads[0].start()
    for t in range(tiles):
        load(t).start()
    loads[1].start()
    loads[2].start()
    none = jnp.zeros((2, depth), BF16)
    gates = jnp.concatenate([ga_ref[...], gb_ref[...], gc_ref[...], none], axis=0)
    for t in range(tiles):
        load(t).wait()
        lg_ref[t * tall : (t + 1) * tall, :] = nt(x_buf[t], gates)
    loads[0].wait()

    def piece(step, _):
        i, t = step // tiles, step % tiles
        rows = nn(x_buf[t], w_buf[i]).astype(BF16)
        for n in range(tall // BLOCK):
            for h in range(2):
                out_ref[i, t * (tall // BLOCK) + n, h * BLOCK : (h + 1) * BLOCK, :] = rows[
                    n * BLOCK : (n + 1) * BLOCK, h * 128 : (h + 1) * 128
                ]
        return 0

    lax.fori_loop(0, tiles, piece, 0)
    loads[1].wait()
    loads[2].wait()
    lax.fori_loop(tiles, 3 * tiles, piece, 0)


def mixer_inputs(x, wq, wk, wv, ga, gb, gc, after, tiles=2):
    rows, depth = x.shape
    hbm = pl.BlockSpec(memory_space=pltpu.HBM)
    whole = pl.BlockSpec(memory_space=VMEM)
    return pl.pallas_call(
        mixed_body,
        in_specs=[hbm] * 4 + [whole] * 3 + [pl.BlockSpec(memory_space=pl.ANY)],
        out_specs=[whole] * 2,
        out_shape=[
            jax.ShapeDtypeStruct((3, rows // BLOCK, 128, 128), BF16),
            jax.ShapeDtypeStruct((rows, 8), F32),
        ],
        scratch_shapes=[
            VMEM((tiles, rows // tiles, depth), BF16),
            VMEM((3,) + wq.shape, BF16),
            pltpu.SemaphoreType.DMA((tiles + 3,)),
        ],
        compiler_params=params(BIG),
        cost_estimate=cost(2 * rows * depth * 768, 2 * (rows * depth + depth * 768)),
        name="mixer_inputs",
    )(x, wq, wk, wv, ga, gb, gc, after)


def passages_body(store_hbm, wk_hbm, wv_hbm, after_ref, out_ref, x_buf, w_buf, sems):
    chunks, tall, _ = x_buf.shape
    rows = out_ref.shape[1] // 4
    count = tall // rows

    def load(i):
        return pltpu.make_async_copy(store_hbm.at[pl.ds(i * tall, tall)], x_buf.at[i], sems.at[i])

    load_k = pltpu.make_async_copy(wk_hbm, w_buf.at[0], sems.at[chunks])
    load_v = pltpu.make_async_copy(wv_hbm, w_buf.at[1], sems.at[chunks + 1])
    load_k.start()
    load(0).start()
    load_v.start()
    for i in range(1, chunks):
        load(i).start()
    load_k.wait()
    load_v.wait()

    def chunk(i, _):
        load(i).wait()
        keys = nn(x_buf[i], w_buf[0]).astype(BF16)
        values = nn(x_buf[i], w_buf[1]).astype(BF16).astype(F32)
        for p in range(count):
            span = slice(p * rows, (p + 1) * rows)
            at = i * count + p
            for h in range(2):
                out_ref[at, h * rows : (h + 1) * rows, :] = keys[span, h * 128 : (h + 1) * 128]
            stacked = jnp.concatenate([values[span, :128], values[span, 128:]], axis=0)
            out_ref[at, 128:256, :] = stacked.T.astype(BF16)
        return 0

    lax.fori_loop(0, chunks, chunk, 0)


def project_passages(store, wk, wv, after, chunks=4):
    number, rows, depth = store.shape
    hbm = pl.BlockSpec(memory_space=pltpu.HBM)
    return pl.pallas_call(
        passages_body,
        in_specs=[hbm, hbm, hbm, pl.BlockSpec(memory_space=pl.ANY)],
        out_specs=pl.BlockSpec(memory_space=VMEM),
        out_shape=jax.ShapeDtypeStruct((number, 256, 128), BF16),
        scratch_shapes=[
            VMEM((chunks, number * rows // chunks, depth), BF16),
            VMEM((2,) + wk.shape, BF16),
            pltpu.SemaphoreType.DMA((chunks + 2,)),
        ],
        compiler_params=params(BIG),
        cost_estimate=cost(2 * number * rows * depth * 512, 2 * number * rows * depth),
        name="passages",
    )(store.reshape(number * rows, depth), wk, wv, after)


def prepare_body(first, qkv_ref, lg_ref, ex_ref, rate_ref, after_ref, mats_ref, base_ref, keep_ref):
    ri = lax.broadcasted_iota(jnp.int32, (128, 128), 0)
    ci = lax.broadcasted_iota(jnp.int32, (128, 128), 1)
    same = (ri >= BLOCK) == (ci >= BLOCK)
    lower = same & (ri >= ci)
    strict = same & (ri > ci)
    upper = same & (ri <= ci)
    diag = ri == ci
    top = lax.broadcasted_iota(jnp.int32, (128, 1), 0) < BLOCK
    rate = jnp.where(top, rate_ref[0], rate_ref[1])
    pieces = []
    for n in range(qkv_ref.shape[1]):
        lg = lg_ref[n * BLOCK : (n + 1) * BLOCK, :]
        at = (first + n) * BLOCK
        ex = jnp.concatenate([ex_ref[0:1, at : at + BLOCK], ex_ref[1:2, at : at + BLOCK]], axis=1)
        beta = jax.nn.sigmoid(jnp.concatenate([lg[:, 0:1], lg[:, 1:2]], axis=0))
        pre = jnp.concatenate([lg[:, 2:3], lg[:, 3:4]], axis=0)
        extra = jnp.sum(jnp.where(diag, ex, 0.0), axis=1, keepdims=True)
        soft = jnp.maximum(pre, 0.0) + jnp.log1p(jnp.exp(-jnp.abs(pre)))
        g = extra - rate * soft
        g_row = jnp.sum(jnp.where(diag, g, 0.0), axis=0, keepdims=True)
        c = jnp.sum(jnp.where(lower, g_row, 0.0), axis=1, keepdims=True)
        total = jnp.sum(jnp.where(same, g_row, 0.0), axis=1, keepdims=True)
        c_row = jnp.sum(jnp.where(upper, g, 0.0), axis=0, keepdims=True)
        damping = jnp.where(lower, jnp.exp(jnp.where(lower, c - c_row, 0.0)), 0.0)
        q = qkv_ref[0, n].astype(F32)
        k = qkv_ref[1, n].astype(F32)
        v = qkv_ref[2, n].astype(F32)
        q = q * (lax.rsqrt(jnp.sum(q * q, axis=1, keepdims=True) + EPS) * 128**-0.5)
        k = k * lax.rsqrt(jnp.sum(k * k, axis=1, keepdims=True) + EPS)
        kb = k * beta
        decay = jnp.exp(c)
        k16 = k.astype(BF16)
        power = jnp.where(strict, nt(kb.astype(BF16), k16) * damping, 0.0)
        within = (nt(q.astype(BF16), k16) * damping).astype(BF16)
        inverse = jnp.where(diag, 1.0, 0.0) - power
        p16 = power.astype(BF16)
        for _ in range(5):
            p16 = nn(p16, p16).astype(BF16)
            inverse = inverse + nn(inverse.astype(BF16), p16)
        inv16 = inverse.astype(BF16)
        mix = nn(inv16, (kb * decay).astype(BF16)).astype(BF16)
        base = nn(inv16, (v * beta).astype(BF16))
        q_dec = (q * decay).astype(BF16)
        k_tail = (k * jnp.exp(total - c)).astype(BF16)
        sub = lax.broadcasted_iota(jnp.int32, (8, 128), 0)
        ends = jnp.exp(total)
        keep = jnp.where(sub == 0, ends[0:1], ends[BLOCK : BLOCK + 1])
        pieces.append((mix, q_dec, within, k_tail, base, keep))
    for n, (mix, q_dec, within, k_tail, base, keep) in enumerate(pieces):
        for h in range(2):
            rows = slice(h * BLOCK, (h + 1) * BLOCK)
            mats_ref[n, h, :BLOCK, :] = mix[rows]
            mats_ref[n, h, BLOCK:, :] = q_dec[rows]
        mats_ref[n, 2] = within
        mats_ref[n, 3] = k_tail
        base_ref[n] = base
        keep_ref[n] = keep


def prepare(qkv, logits, extra, rate, after, first, number):
    at = first // number
    return pl.pallas_call(
        functools.partial(prepare_body, first),
        grid=(1,),
        in_specs=[
            pl.BlockSpec((3, number, 128, 128), lambda i: (0, at, 0, 0)),
            pl.BlockSpec((number * BLOCK, logits.shape[1]), lambda i: (at, 0)),
            pl.BlockSpec(extra.shape, lambda i: (0, 0)),
            pl.BlockSpec(memory_space=pltpu.SMEM),
            pl.BlockSpec(memory_space=pl.ANY),
        ],
        out_specs=[
            pl.BlockSpec((number, 4, 128, 128), lambda i: (0, 0, 0, 0)),
            pl.BlockSpec((number, 128, 128), lambda i: (0, 0, 0)),
            pl.BlockSpec((number, 8, 128), lambda i: (0, 0, 0)),
        ],
        out_shape=[
            jax.ShapeDtypeStruct((number, 4, 128, 128), BF16),
            jax.ShapeDtypeStruct((number, 128, 128), F32),
            jax.ShapeDtypeStruct((number, 8, 128), F32),
        ],
        compiler_params=params(16),
        cost_estimate=cost(number * 400 * MIB, number * 300 * 1024),
        name="prepare",
    )(qkv, logits, extra, rate, after)


def advance_body(n, mats_ref, base_ref, keep_ref, gain_ref, s_ref, after_ref, out_ref, s_out_ref):
    base = base_ref[n]
    state = [s_ref[0], s_ref[1]]
    fresh, far = [], []
    for h in range(2):
        both = nn(mats_ref[n, h], state[h].astype(BF16))
        fresh.append(base[h * BLOCK : (h + 1) * BLOCK] - both[:BLOCK])
        far.append(both[BLOCK:])
    f16 = jnp.concatenate(fresh, axis=0).astype(BF16)
    recur = jnp.concatenate(far, axis=0) + nn(mats_ref[n, 2], f16)
    tail = mats_ref[n, 3]
    for h in range(2):
        rows = slice(h * BLOCK, (h + 1) * BLOCK)
        state[h] = state[h] * keep_ref[n, h : h + 1, :] + tn(tail[rows], f16[rows])
    scale = lax.rsqrt(jnp.mean(recur * recur, axis=1, keepdims=True) + EPS)
    out_ref[0] = recur * scale * gain_ref[...]
    s_out_ref[0] = state[0]
    s_out_ref[1] = state[1]


def advance(prepared, n, gain, state, after):
    whole = pl.BlockSpec(memory_space=VMEM)
    return pl.pallas_call(
        functools.partial(advance_body, n),
        in_specs=[whole] * 5 + [pl.BlockSpec(memory_space=pl.ANY)],
        out_specs=[whole] * 2,
        out_shape=[
            jax.ShapeDtypeStruct((1, 128, 128), F32),
            jax.ShapeDtypeStruct((2, 128, 128), F32),
        ],
        compiler_params=params(8),
        cost_estimate=cost(200 * MIB, 300 * 1024),
        name="advance",
    )(*prepared, gain, state, after)


def parts_body(count, far, own_ref, *refs):
    codes_ref = refs[-1]

    def run():
        find_parts(count, own_ref, *refs)

    def skip():
        for i in range(count * SLOTS):
            codes_ref[i] = 0

    if far:
        pl.when(own_ref[1] != 0)(run)
        pl.when(own_ref[1] == 0)(skip)
    else:
        run()


def find_parts(count, own_ref, *refs):
    messages, refs = refs[:count], refs[count:]
    (kv_ref, mate_ref, _, sums_ref, stats_ref, codes_ref) = refs
    chip, core = own_ref[0], own_ref[1]
    rows = messages[0].shape[0]
    row = lax.broadcasted_iota(jnp.int32, (8, 128), 0)
    lane = lax.broadcasted_iota(jnp.int32, (8, 128), 1)
    before = (
        lax.broadcasted_iota(jnp.int32, (128, 128), 0) < lax.broadcasted_iota(jnp.int32, (128, 128), 1)
    )
    before = jnp.where(before, 1.0, 0.0).astype(BF16)
    blocks = (rows - 8) // 128
    left = lax.broadcasted_iota(jnp.int32, (BLOCK, 128), 1) < BLOCK
    spots = []
    for n in range(count):
        table = messages[n][rows - 8 :, :].astype(F32)
        entry = jnp.concatenate([table[4:8], table[4:8]], axis=0)
        name = table.astype(jnp.int32) - 1
        hit = ((name >> 1) == chip) & (row < 4) & (lane < blocks)
        ones = jnp.where(hit, 1.0, 0.0)
        rank = nn(ones.astype(BF16), before)
        sums = jnp.sum(ones, axis=1, keepdims=True)
        first, second, third = sums[0:1], sums[1:2], sums[2:3]
        rank = rank + jnp.where(row > 0, first, 0.0)
        rank = rank + jnp.where(row > 1, second, 0.0)
        rank = rank + jnp.where(row > 2, third, 0.0)
        far = jnp.where((name & 1) == core, 0.0, 16.0)
        code = lane.astype(F32) * 32.0 + far + entry + 1.0
        for r in range(SLOTS):
            value = jnp.where(hit & (rank == float(r)), code, 0.0)
            spots.append(jnp.sum(value).astype(jnp.int32))
    for n in range(count):
        found = []
        for r in range(SLOTS):
            spot = jnp.maximum(spots[n * SLOTS + r] - 1, 0)
            at = pl.multiple_of((spot >> 5) * 128, 128)
            q = messages[n][pl.ds(at, 128), :]
            kv = jnp.where((spot & 16) != 0, mate_ref[spot & 15], kv_ref[spot & 15])
            both = nt(kv[0:128], q)
            scores = jnp.where(left, both[:BLOCK], both[BLOCK:]) * 128**-0.5
            found.append((scores, kv[128:256]))
        weighed = []
        for scores, values in found:
            peak = jnp.max(scores, axis=0, keepdims=True)
            expo = jnp.exp(scores - peak)
            denom = jnp.sum(expo, axis=0, keepdims=True)
            split = jnp.concatenate(
                [jnp.where(left, expo, 0.0), jnp.where(left, 0.0, expo)], axis=0
            ).astype(BF16)
            weighed.append((nn(values, split), jnp.where(row == 0, peak, denom)))
        for r in range(SLOTS):
            i = n * SLOTS + r
            codes_ref[i] = spots[i]
            sums_ref[i], stats_ref[i] = weighed[r]


def parts(own, messages, kv, kv_mate, after, far):
    count = len(messages)
    total = count * SLOTS
    whole = pl.BlockSpec(memory_space=VMEM)
    scalars = pl.BlockSpec(memory_space=pltpu.SMEM)
    return pl.pallas_call(
        functools.partial(parts_body, count, far),
        in_specs=[scalars] + [whole] * (count + 2) + [pl.BlockSpec(memory_space=pl.ANY)],
        out_specs=[whole, whole, scalars],
        out_shape=[
            jax.ShapeDtypeStruct((total, 128, 128), F32),
            jax.ShapeDtypeStruct((total, 8, 128), F32),
            jax.ShapeDtypeStruct((total,), jnp.int32),
        ],
        compiler_params=params(12),
        cost_estimate=cost(count * 400 * MIB, count * 500 * 1024),
        name="parts",
    )(own, *messages, kv, kv_mate, after)


def split3(x):
    high = x.astype(BF16)
    rest = x - high.astype(F32)
    mid = rest.astype(BF16)
    low = (rest - mid.astype(F32)).astype(BF16)
    return high.astype(F32), mid.astype(F32), low.astype(F32)


def merge_body(first, start, own_ref, codes_ref, sums_ref, stats_ref, after_ref, *refs):
    out_ref = refs[-1]

    def begin():
        pad = lax.broadcasted_iota(jnp.int32, (8, 128), 0)
        none = jnp.where(pad == 0, NONE, 0.0).astype(BF16)
        for b in range(out_ref.shape[0]):
            out_ref[b, 0:128, :] = jnp.zeros((128, 128), BF16)
            out_ref[b, 128:136, :] = none

    if start == "core_1":
        pl.when(own_ref[1] != 0)(begin)
    elif start == "core_0":
        pl.when(own_ref[1] == 0)(begin)
    for r in range(SLOTS):
        code = codes_ref[first + r]

        @pl.when(code > 0)
        def _():
            b = (code - 1) >> 5
            peak, denom = stats_ref[first + r, 0:1, :], stats_ref[first + r, 1:2, :]
            stats = out_ref[b, 128:136, :].astype(F32)
            m_old = stats[0:1] + stats[1:2] + stats[2:3]
            l_old = stats[3:4] + stats[4:5] + stats[5:6]
            m_new = jnp.maximum(m_old, peak)
            keep = jnp.exp(m_old - m_new)
            gain = jnp.exp(peak - m_new)
            l_new = l_old * keep + denom * gain
            zero = jnp.zeros((2, 128), F32)
            fresh = jnp.concatenate(split3(m_new) + split3(l_new) + (zero,), axis=0)
            out_ref[b, 128:136, :] = fresh.astype(BF16)
            mixed = out_ref[b, 0:128, :].astype(F32) * keep + sums_ref[first + r] * gain
            out_ref[b, 0:128, :] = mixed.astype(BF16)


def merge(own, part, blocks, after, msg=None, start="none"):
    (sums, stats, codes), n = part
    whole = pl.BlockSpec(memory_space=VMEM)
    scalars = pl.BlockSpec(memory_space=pltpu.SMEM)
    more = () if msg is None else (msg,)
    return pl.pallas_call(
        functools.partial(merge_body, n * SLOTS, start),
        in_specs=[scalars, scalars, whole, whole, pl.BlockSpec(memory_space=pl.ANY)]
        + [whole] * len(more),
        out_specs=whole,
        out_shape=jax.ShapeDtypeStruct((blocks, 136, 128), BF16),
        input_output_aliases={5: 0} if more else {},
        compiler_params=params(8),
        cost_estimate=cost(100 * MIB, 900 * 1024),
        name="merge",
    )(own, codes, sums, stats, after, *more)


def finish_body(a_ref, b_ref, lg_ref, *refs):
    normed, out_ref = refs[:-1], refs[-1]
    per = normed[0].shape[0]
    for b in range(a_ref.shape[0]):
        sa = a_ref[b, 128:136, :].astype(F32)
        sb = b_ref[b, 128:136, :].astype(F32)
        ma, mb = (s[0:1] + s[1:2] + s[2:3] for s in (sa, sb))
        la, lb = (s[3:4] + s[4:5] + s[5:6] for s in (sa, sb))
        peak = jnp.maximum(ma, mb)
        ga, gb = jnp.exp(ma - peak), jnp.exp(mb - peak)
        denom = la * ga + lb * gb
        sums = a_ref[b, 0:128, :].astype(F32) * ga + b_ref[b, 0:128, :].astype(F32) * gb
        retrieved = (sums / denom).T
        lg = lg_ref[b * BLOCK : (b + 1) * BLOCK, :]
        gate = jax.nn.sigmoid(jnp.concatenate([lg[:, 4:5], lg[:, 5:6]], axis=0))
        mixed = (normed[b // per][b % per] + gate * retrieved).astype(BF16)
        for h in range(2):
            out_ref[b * BLOCK : (b + 1) * BLOCK, h * 128 : (h + 1) * 128] = mixed[
                h * BLOCK : (h + 1) * BLOCK
            ]


def finish(a, b, logits, normed):
    rows = logits.shape[0]
    return pl.pallas_call(
        finish_body,
        out_shape=jax.ShapeDtypeStruct((rows, 256), BF16),
        compiler_params=params(16),
        cost_estimate=cost(100 * MIB, 2 * MIB),
        name="finish",
    )(a, b, logits, *normed)


def per_device(
    tokens,
    owners,
    entries,
    store,
    mixer_query_weight,
    mixer_key_weight,
    mixer_value_weight,
    strength_weight,
    decay_weight,
    head_decay_rate,
    extra_forgetting_exponent,
    output_norm_gain,
    retrieval_query_weight,
    passage_key_weight,
    passage_value_weight,
    retrieval_gate_weight,
):
    devices = lax.axis_size("st")
    me = lax.axis_index("st")
    core = lax.rem(me, 2)
    reach = devices // 4
    blocks = owners.shape[0]

    step = [2 if i % 2 == 0 else -2 for i in range(devices)]
    ahead = [(i, (i + step[i]) % devices) for i in range(devices)]
    across = [(i ^ 1, j) for i, j in ahead]
    mates = [(i, i ^ 1) for i in range(devices)]

    def send(x, pairs):
        return lax.ppermute(x, "st", pairs)

    def out(x, h, first):
        pairs = first if h == 1 else ahead
        if h == reach:
            pairs = [(i, j) for i, j in pairs if i % 2 == 1]
        return send(x, pairs)

    def back(x, h, first):
        pairs = first if h == 1 else ahead
        if h == reach:
            pairs = [(i, j) for i, j in pairs if i % 2 == 1]
        return send(x, [(j, i) for i, j in pairs])

    query = query_message(tokens, retrieval_query_weight, owners.T, entries.T)
    own = {0: query}
    other = {}
    gain = output_norm_gain.reshape(1, 128)
    extra = extra_forgetting_exponent.T
    where_own = jnp.stack([me >> 1, me & 1])
    part = {}

    def compute_parts(names, after):
        messages = [(own if lane == "own" else other)[h] for lane, h in names]
        result = parts(where_own, messages, kv_own, kv_mate, after, names[0][1] == reach)
        for n, name in enumerate(names):
            part[name] = (result, n)
        return result[1]

    own[1] = out(query, 1, ahead)
    other[1] = out(query, 1, across)
    kv_own = project_passages(store, passage_key_weight, passage_value_weight, query)
    kv_mate = send(kv_own, mates)
    for h in range(2, reach + 1):
        own[h] = out(own[h - 1], h, ahead)
        other[h] = out(other[h - 1], h, across)
    qkv, logits = mixer_inputs(
        tokens,
        mixer_query_weight,
        mixer_key_weight,
        mixer_value_weight,
        strength_weight.T,
        decay_weight.T,
        retrieval_gate_weight.T,
        other[1],
    )
    together = blocks // 2
    prepared = []
    for n in range(2):
        prepared.append(
            prepare(qkv, logits, extra, head_decay_rate, own[3], n * together, together)
        )
    last = compute_parts([("own", 0)], logits)
    for h in range(1, reach):
        last = compute_parts([("own", h), ("other", h)], last)

    normed = []
    state = jnp.zeros((2, 128, 128), F32)

    def mixer_step(after):
        nonlocal state
        n = len(normed)
        result, state = advance(prepared[n // together], n % together, gain, state, after)
        normed.append(result)
        return state

    msg_own = msg_other = None
    for h in range(reach, 0, -1):
        start = {reach: "core_1", reach - 1: "core_0"}.get(h, "none")
        if h == reach:
            last = compute_parts([("own", h)], last)
        last = merge(where_own, part[("own", h)], blocks, last, msg_own, start)
        msg_own = back(last, h, ahead)
        if h == reach:
            last = compute_parts([("other", h)], last)
        last = merge(where_own, part[("other", h)], blocks, last, msg_other, start)
        msg_other = back(last, h, across)
        last = mixer_step(last)
    while len(normed) < blocks:
        last = mixer_step(last)
    msg_own = merge(where_own, part[("own", 0)], blocks, last, msg_own)
    return finish(msg_own, msg_other, logits, normed)


def solution(mesh):
    return jax.shard_map(
        per_device,
        mesh=mesh,
        in_specs=(
            P(("grp", "st"), None),
            P(("grp", "st"), None),
            P(("grp", "st"), None),
            P(("grp", "st"), None, None),
            P(None, "tp"),
            P(None, "tp"),
            P(None, "tp"),
            P(None, "tp"),
            P(None, "tp"),
            P("tp"),
            P(("grp", "st"), "tp"),
            P(),
            P(None, "tp"),
            P(None, "tp"),
            P(None, "tp"),
            P(None, "tp"),
        ),
        out_specs=P(("grp", "st"), "tp"),
        check_vma=False,
    )
```

```python
import functools

import jax
import jax.numpy as jnp
from jax import lax
from jax.experimental import pallas as pl
from jax.experimental.pallas import tpu as pltpu
from jax.sharding import PartitionSpec as P


BLOCK = 64
SLOTS = 4
EPS = 1e-06
NONE = -1e30
MIB = 1024 * 1024
BIG = 52
F32 = jnp.float32
BF16 = jnp.bfloat16
VMEM = pltpu.VMEM


def nt(left, right):
    return lax.dot_general(left, right, (((1,), (1,)), ((), ())), preferred_element_type=F32)


def nn(left, right):
    return jnp.dot(left, right, preferred_element_type=F32)


def tn(left, right):
    return lax.dot_general(left, right, (((0,), (0,)), ((), ())), preferred_element_type=F32)


def params(limit, **more):
    return pltpu.CompilerParams(vmem_limit_bytes=limit * MIB, **more)


def cost(flops, size, trans=0):
    return pl.CostEstimate(flops=flops, bytes_accessed=size, transcendentals=trans)


def pieces(src, dst, sems, first, count):
    rows = dst.shape[0] // count
    return [
        pltpu.make_async_copy(
            src.at[pl.ds(i * rows, rows)], dst.at[pl.ds(i * rows, rows)], sems.at[first + i]
        )
        for i in range(count)
    ]


def query_body(x_hbm, w_hbm, owners_hbm, entries_hbm, out_ref, x_buf, w_buf, owners_ref, entries_ref, sems):
    tiles, rows, _ = x_buf.shape
    loads = pieces(w_hbm, w_buf, sems, 0, 4)
    x_loads = [
        pieces(x_hbm.at[pl.ds(i * rows, rows)], x_buf.at[i], sems, 4 + i * 4, 4)
        for i in range(tiles)
    ]
    tables = [
        pltpu.make_async_copy(owners_hbm, owners_ref, sems.at[tiles * 4 + 4]),
        pltpu.make_async_copy(entries_hbm, entries_ref, sems.at[tiles * 4 + 5]),
    ]
    for copies in [loads] + x_loads + [tables]:
        for copy in copies:
            copy.start()
    per, count = owners_ref.shape
    blocks = tiles * rows // BLOCK
    for table in tables:
        table.wait()
    names = jnp.concatenate([owners_ref[...] + 1, entries_ref[...]], axis=0).astype(F32)
    out_ref[blocks * 128 :, :] = jnp.zeros((2 * per, 128), BF16)
    out_ref[blocks * 128 :, 0:count] = names.astype(BF16)
    for copy in loads:
        copy.wait()
    for i in range(tiles):
        for copy in x_loads[i]:
            copy.wait()
        q = nn(x_buf[i], w_buf[...]).astype(BF16)
        for n in range(rows // BLOCK):
            at = (i * rows // BLOCK + n) * 128
            for h in range(2):
                out_ref[at + h * BLOCK : at + (h + 1) * BLOCK, :] = q[
                    n * BLOCK : (n + 1) * BLOCK, h * 128 : (h + 1) * 128
                ]


def query_message(x, w, owners, entries, tiles=2):
    rows, depth = x.shape
    hbm = pl.BlockSpec(memory_space=pltpu.HBM)
    whole = pl.BlockSpec(memory_space=VMEM)
    return pl.pallas_call(
        query_body,
        in_specs=[hbm] * 4,
        out_specs=whole,
        out_shape=jax.ShapeDtypeStruct((rows * 2 + 8, 128), BF16),
        scratch_shapes=[
            VMEM((tiles, rows // tiles, depth), BF16),
            VMEM(w.shape, BF16),
            VMEM(owners.shape, jnp.int32),
            VMEM(entries.shape, jnp.int32),
            pltpu.SemaphoreType.DMA((tiles * 4 + 6,)),
        ],
        compiler_params=params(BIG + 1),
        cost_estimate=cost(2 * rows * depth * 256, 2 * (rows * depth + depth * 256)),
        name="query",
    )(x, w, owners, entries)


def mixed_body(
    x_hbm, wq_hbm, wk_hbm, wv_hbm, ga_ref, gb_ref, gc_ref, after_ref, out_ref, lg_ref, x_buf, w_buf, sems
):
    tiles, tall, depth = x_buf.shape

    x_loads = [
        pieces(x_hbm.at[pl.ds(t * tall, tall)], x_buf.at[t], sems, t * 4, 4) for t in range(tiles)
    ]
    w_loads = [
        pieces(w, w_buf.at[i], sems, (tiles + i) * 4, 4)
        for i, w in enumerate((wq_hbm, wk_hbm, wv_hbm))
    ]
    for copies in x_loads + w_loads:
        for copy in copies:
            copy.start()
    none = jnp.zeros((2, depth), BF16)
    gates = jnp.concatenate([ga_ref[...], gb_ref[...], gc_ref[...], none], axis=0)
    for t in range(tiles):
        for copy in x_loads[t]:
            copy.wait()
        lg_ref[t * tall : (t + 1) * tall, :] = nt(x_buf[t], gates)
    for copy in w_loads[0]:
        copy.wait()

    def piece(step, _):
        i, t = step // tiles, step % tiles
        rows = nn(x_buf[t], w_buf[i]).astype(BF16)
        for n in range(tall // BLOCK):
            for h in range(2):
                out_ref[i, t * (tall // BLOCK) + n, h * BLOCK : (h + 1) * BLOCK, :] = rows[
                    n * BLOCK : (n + 1) * BLOCK, h * 128 : (h + 1) * 128
                ]
        return 0

    lax.fori_loop(0, tiles, piece, 0)
    for copy in w_loads[1] + w_loads[2]:
        copy.wait()
    lax.fori_loop(tiles, 3 * tiles, piece, 0)


def mixer_inputs(x, wq, wk, wv, ga, gb, gc, after, tiles=2):
    rows, depth = x.shape
    hbm = pl.BlockSpec(memory_space=pltpu.HBM)
    whole = pl.BlockSpec(memory_space=VMEM)
    return pl.pallas_call(
        mixed_body,
        in_specs=[hbm] * 4 + [whole] * 3 + [pl.BlockSpec(memory_space=pl.ANY)],
        out_specs=[whole] * 2,
        out_shape=[
            jax.ShapeDtypeStruct((3, rows // BLOCK, 128, 128), BF16),
            jax.ShapeDtypeStruct((rows, 8), F32),
        ],
        scratch_shapes=[
            VMEM((tiles, rows // tiles, depth), BF16),
            VMEM((3,) + wq.shape, BF16),
            pltpu.SemaphoreType.DMA((tiles * 4 + 12,)),
        ],
        compiler_params=params(BIG),
        cost_estimate=cost(2 * rows * depth * 768, 2 * (rows * depth + depth * 768)),
        name="mixer_inputs",
    )(x, wq, wk, wv, ga, gb, gc, after)


def passages_body(store_hbm, wk_hbm, wv_hbm, after_ref, out_ref, x_buf, w_buf, sems):
    chunks, tall, _ = x_buf.shape
    rows = out_ref.shape[1] // 4
    count = tall // rows

    def load(i):
        return pieces(store_hbm.at[pl.ds(i * tall, tall)], x_buf.at[i], sems, i * 4, 4)

    weights = pieces(wk_hbm, w_buf.at[0], sems, chunks * 4, 4)
    weights += pieces(wv_hbm, w_buf.at[1], sems, chunks * 4 + 4, 4)
    for copy in load(0) + weights:
        copy.start()
    for i in range(1, chunks):
        for copy in load(i):
            copy.start()
    for copy in weights:
        copy.wait()

    def chunk(i, _):
        for copy in load(i):
            copy.wait()
        keys = nn(x_buf[i], w_buf[0]).astype(BF16)
        values = nn(x_buf[i], w_buf[1]).astype(BF16).astype(F32)
        for p in range(count):
            span = slice(p * rows, (p + 1) * rows)
            at = i * count + p
            for h in range(2):
                out_ref[at, h * rows : (h + 1) * rows, :] = keys[span, h * 128 : (h + 1) * 128]
            stacked = jnp.concatenate([values[span, :128], values[span, 128:]], axis=0)
            out_ref[at, 128:256, :] = stacked.T.astype(BF16)
        return 0

    lax.fori_loop(0, chunks, chunk, 0)


def project_passages(store, wk, wv, after, chunks=4):
    number, rows, depth = store.shape
    hbm = pl.BlockSpec(memory_space=pltpu.HBM)
    return pl.pallas_call(
        passages_body,
        in_specs=[hbm, hbm, hbm, pl.BlockSpec(memory_space=pl.ANY)],
        out_specs=pl.BlockSpec(memory_space=VMEM),
        out_shape=jax.ShapeDtypeStruct((number, 256, 128), BF16),
        scratch_shapes=[
            VMEM((chunks, number * rows // chunks, depth), BF16),
            VMEM((2,) + wk.shape, BF16),
            pltpu.SemaphoreType.DMA((chunks * 4 + 8,)),
        ],
        compiler_params=params(BIG),
        cost_estimate=cost(2 * number * rows * depth * 512, 2 * number * rows * depth),
        name="passages",
    )(store.reshape(number * rows, depth), wk, wv, after)


def mixer_body(
    first, qkv_ref, lg_ref, ex_ref, rate_ref, gain_ref, s_ref, after_ref, out_ref, s_out_ref
):
    ri = lax.broadcasted_iota(jnp.int32, (128, 128), 0)
    ci = lax.broadcasted_iota(jnp.int32, (128, 128), 1)
    same = (ri >= BLOCK) == (ci >= BLOCK)
    lower = same & (ri >= ci)
    strict = same & (ri > ci)
    upper = same & (ri <= ci)
    diag = ri == ci
    top = lax.broadcasted_iota(jnp.int32, (128, 1), 0) < BLOCK
    rate = jnp.where(top, rate_ref[0], rate_ref[1])
    pieces = []
    for n in range(qkv_ref.shape[1]):
        lg = lg_ref[n * BLOCK : (n + 1) * BLOCK, :]
        at = (first + n) * BLOCK
        ex = jnp.concatenate([ex_ref[0:1, at : at + BLOCK], ex_ref[1:2, at : at + BLOCK]], axis=1)
        beta = jax.nn.sigmoid(jnp.concatenate([lg[:, 0:1], lg[:, 1:2]], axis=0))
        pre = jnp.concatenate([lg[:, 2:3], lg[:, 3:4]], axis=0)
        extra = jnp.sum(jnp.where(diag, ex, 0.0), axis=1, keepdims=True)
        soft = jnp.maximum(pre, 0.0) + jnp.log1p(jnp.exp(-jnp.abs(pre)))
        g = extra - rate * soft
        g_row = jnp.sum(jnp.where(diag, g, 0.0), axis=0, keepdims=True)
        c = jnp.sum(jnp.where(lower, g_row, 0.0), axis=1, keepdims=True)
        total = jnp.sum(jnp.where(same, g_row, 0.0), axis=1, keepdims=True)
        c_row = jnp.sum(jnp.where(upper, g, 0.0), axis=0, keepdims=True)
        damping = jnp.where(lower, jnp.exp(jnp.where(lower, c - c_row, 0.0)), 0.0)
        q = qkv_ref[0, n].astype(F32)
        k = qkv_ref[1, n].astype(F32)
        v = qkv_ref[2, n].astype(F32)
        q = q * (lax.rsqrt(jnp.sum(q * q, axis=1, keepdims=True) + EPS) * 128**-0.5)
        k = k * lax.rsqrt(jnp.sum(k * k, axis=1, keepdims=True) + EPS)
        kb = k * beta
        decay = jnp.exp(c)
        k16 = k.astype(BF16)
        power = jnp.where(strict, nt(kb.astype(BF16), k16) * damping, 0.0)
        within = (nt(q.astype(BF16), k16) * damping).astype(BF16)
        inverse = jnp.where(diag, 1.0, 0.0) - power
        p16 = power.astype(BF16)
        for _ in range(5):
            p16 = nn(p16, p16).astype(BF16)
            inverse = inverse + nn(inverse.astype(BF16), p16)
        inv16 = inverse.astype(BF16)
        mix = nn(inv16, (kb * decay).astype(BF16)).astype(BF16)
        base = nn(inv16, (v * beta).astype(BF16))
        q_dec = (q * decay).astype(BF16)
        k_tail = (k * jnp.exp(total - c)).astype(BF16)
        pieces.append((mix, base, within, q_dec, k_tail, jnp.exp(total)))
    state = [s_ref[0], s_ref[1]]
    for n, (mix, base, within, q_dec, k_tail, keep) in enumerate(pieces):
        fresh, far = [], []
        for h in range(2):
            rows = slice(h * BLOCK, (h + 1) * BLOCK)
            both = nn(jnp.concatenate([mix[rows], q_dec[rows]], axis=0), state[h].astype(BF16))
            fresh.append(base[rows] - both[:BLOCK])
            far.append(both[BLOCK:])
        f16 = jnp.concatenate(fresh, axis=0).astype(BF16)
        recur = jnp.concatenate(far, axis=0) + nn(within, f16)
        for h in range(2):
            rows = slice(h * BLOCK, (h + 1) * BLOCK)
            state[h] = state[h] * keep[h * BLOCK : h * BLOCK + 1] + tn(k_tail[rows], f16[rows])
        scale = lax.rsqrt(jnp.mean(recur * recur, axis=1, keepdims=True) + EPS)
        out_ref[n] = recur * scale * gain_ref[...]
    s_out_ref[0] = state[0]
    s_out_ref[1] = state[1]


def mixer(qkv, logits, extra, rate, gain, state, after, first, number):
    at = first // number
    return pl.pallas_call(
        functools.partial(mixer_body, first),
        grid=(1,),
        in_specs=[
            pl.BlockSpec((3, number, 128, 128), lambda i: (0, at, 0, 0)),
            pl.BlockSpec((number * BLOCK, logits.shape[1]), lambda i: (at, 0)),
            pl.BlockSpec(extra.shape, lambda i: (0, 0)),
            pl.BlockSpec(memory_space=pltpu.SMEM),
            pl.BlockSpec((1, 128), lambda i: (0, 0)),
            pl.BlockSpec((2, 128, 128), lambda i: (0, 0, 0)),
            pl.BlockSpec(memory_space=pl.ANY),
        ],
        out_specs=[
            pl.BlockSpec((number, 128, 128), lambda i: (0, 0, 0)),
            pl.BlockSpec((2, 128, 128), lambda i: (0, 0, 0)),
        ],
        out_shape=[
            jax.ShapeDtypeStruct((number, 128, 128), F32),
            jax.ShapeDtypeStruct((2, 128, 128), F32),
        ],
        compiler_params=params(16),
        cost_estimate=cost(number * 1000 * MIB // 2, number * 300 * 1024),
        name="mixer",
    )(qkv, logits, extra, rate, gain, state, after)


def find_parts(count, own_ref, *refs):
    messages, refs = refs[:count], refs[count:]
    (kv_ref, mate_ref, _, sums_ref, stats_ref, codes_ref) = refs
    chip, core = own_ref[0], own_ref[1]
    rows = messages[0].shape[0]
    row = lax.broadcasted_iota(jnp.int32, (8, 128), 0)
    lane = lax.broadcasted_iota(jnp.int32, (8, 128), 1)
    before = (
        lax.broadcasted_iota(jnp.int32, (128, 128), 0) < lax.broadcasted_iota(jnp.int32, (128, 128), 1)
    )
    before = jnp.where(before, 1.0, 0.0).astype(BF16)
    blocks = (rows - 8) // 128
    left = lax.broadcasted_iota(jnp.int32, (BLOCK, 128), 1) < BLOCK
    spots = []
    for n in range(count):
        table = messages[n][rows - 8 :, :].astype(F32)
        entry = jnp.concatenate([table[4:8], table[4:8]], axis=0)
        name = table.astype(jnp.int32) - 1
        hit = ((name >> 1) == chip) & (row < 4) & (lane < blocks)
        ones = jnp.where(hit, 1.0, 0.0)
        rank = nn(ones.astype(BF16), before)
        sums = jnp.sum(ones, axis=1, keepdims=True)
        first, second, third = sums[0:1], sums[1:2], sums[2:3]
        rank = rank + jnp.where(row > 0, first, 0.0)
        rank = rank + jnp.where(row > 1, second, 0.0)
        rank = rank + jnp.where(row > 2, third, 0.0)
        far = jnp.where((name & 1) == core, 0.0, 16.0)
        code = lane.astype(F32) * 32.0 + far + entry + 1.0
        for r in range(SLOTS):
            value = jnp.where(hit & (rank == float(r)), code, 0.0)
            spots.append(jnp.sum(value).astype(jnp.int32))
    for n in range(count):
        found = []
        for r in range(SLOTS):
            spot = jnp.maximum(spots[n * SLOTS + r] - 1, 0)
            at = pl.multiple_of((spot >> 5) * 128, 128)
            q = messages[n][pl.ds(at, 128), :]
            kv = jnp.where((spot & 16) != 0, mate_ref[spot & 15], kv_ref[spot & 15])
            both = nt(kv[0:128], q)
            scores = jnp.where(left, both[:BLOCK], both[BLOCK:]) * 128**-0.5
            found.append((scores, kv[128:256]))
        weighed = []
        for scores, values in found:
            peak = jnp.max(scores, axis=0, keepdims=True)
            expo = jnp.exp(scores - peak)
            denom = jnp.sum(expo, axis=0, keepdims=True)
            split = jnp.concatenate(
                [jnp.where(left, expo, 0.0), jnp.where(left, 0.0, expo)], axis=0
            ).astype(BF16)
            weighed.append((nn(values, split), jnp.where(row == 0, peak, denom)))
        for r in range(SLOTS):
            i = n * SLOTS + r
            codes_ref[i] = spots[i]
            sums_ref[i], stats_ref[i] = weighed[r]


def parts(own, messages, kv, kv_mate, after):
    count = len(messages)
    total = count * SLOTS
    whole = pl.BlockSpec(memory_space=VMEM)
    scalars = pl.BlockSpec(memory_space=pltpu.SMEM)
    return pl.pallas_call(
        functools.partial(find_parts, count),
        in_specs=[scalars] + [whole] * (count + 2) + [pl.BlockSpec(memory_space=pl.ANY)],
        out_specs=[whole, whole, scalars],
        out_shape=[
            jax.ShapeDtypeStruct((total, 128, 128), F32),
            jax.ShapeDtypeStruct((total, 8, 128), F32),
            jax.ShapeDtypeStruct((total,), jnp.int32),
        ],
        compiler_params=params(12),
        cost_estimate=cost(count * 400 * MIB, count * 500 * 1024),
        name="parts",
    )(own, *messages, kv, kv_mate, after)


def split3(x):
    high = x.astype(BF16)
    rest = x - high.astype(F32)
    mid = rest.astype(BF16)
    low = (rest - mid.astype(F32)).astype(BF16)
    return high.astype(F32), mid.astype(F32), low.astype(F32)


def begin(out_ref):
    pad = lax.broadcasted_iota(jnp.int32, (8, 128), 0)
    none = jnp.where(pad == 0, NONE, 0.0).astype(BF16)
    for b in range(out_ref.shape[0]):
        out_ref[b, 0:128, :] = jnp.zeros((128, 128), BF16)
        out_ref[b, 128:136, :] = none


def merge_into(first, codes_ref, sums_ref, stats_ref, out_ref):
    for r in range(SLOTS):
        code = codes_ref[first + r]

        @pl.when(code > 0)
        def _():
            b = (code - 1) >> 5
            peak, denom = stats_ref[first + r, 0:1, :], stats_ref[first + r, 1:2, :]
            stats = out_ref[b, 128:136, :].astype(F32)
            m_old = stats[0:1] + stats[1:2] + stats[2:3]
            l_old = stats[3:4] + stats[4:5] + stats[5:6]
            m_new = jnp.maximum(m_old, peak)
            keep = jnp.exp(m_old - m_new)
            gain = jnp.exp(peak - m_new)
            l_new = l_old * keep + denom * gain
            zero = jnp.zeros((2, 128), F32)
            fresh = jnp.concatenate(split3(m_new) + split3(l_new) + (zero,), axis=0)
            out_ref[b, 128:136, :] = fresh.astype(BF16)
            mixed = out_ref[b, 0:128, :].astype(F32) * keep + sums_ref[first + r] * gain
            out_ref[b, 0:128, :] = mixed.astype(BF16)


def merge_body(first, start, own_ref, codes_ref, sums_ref, stats_ref, after_ref, *refs):
    out_ref = refs[-1]
    if start == "all":
        begin(out_ref)
    elif start == "core_0":
        pl.when(own_ref[1] == 0)(lambda: begin(out_ref))
    merge_into(first, codes_ref, sums_ref, stats_ref, out_ref)


def far_body(own_ref, q_ref, kv_ref, mate_ref, after_ref, out_ref, sums_ref, stats_ref, codes_ref):
    @pl.when(own_ref[1] != 0)
    def _():
        find_parts(1, own_ref, q_ref, kv_ref, mate_ref, after_ref, sums_ref, stats_ref, codes_ref)
        begin(out_ref)
        merge_into(0, codes_ref, sums_ref, stats_ref, out_ref)


def far_message(own, q, kv, kv_mate, blocks, after):
    whole = pl.BlockSpec(memory_space=VMEM)
    return pl.pallas_call(
        far_body,
        in_specs=[pl.BlockSpec(memory_space=pltpu.SMEM), whole, whole, whole]
        + [pl.BlockSpec(memory_space=pl.ANY)],
        out_specs=whole,
        out_shape=jax.ShapeDtypeStruct((blocks, 136, 128), BF16),
        scratch_shapes=[
            VMEM((SLOTS, 128, 128), F32),
            VMEM((SLOTS, 8, 128), F32),
            pltpu.SMEM((SLOTS,), jnp.int32),
        ],
        compiler_params=params(10),
        cost_estimate=cost(500 * MIB, 500 * 1024),
        name="far",
    )(own, q, kv, kv_mate, after)


def merge(own, part, blocks, after, msg=None, start="none"):
    (sums, stats, codes), n = part
    whole = pl.BlockSpec(memory_space=VMEM)
    scalars = pl.BlockSpec(memory_space=pltpu.SMEM)
    more = () if msg is None else (msg,)
    return pl.pallas_call(
        functools.partial(merge_body, n * SLOTS, start),
        in_specs=[scalars, scalars, whole, whole, pl.BlockSpec(memory_space=pl.ANY)]
        + [whole] * len(more),
        out_specs=whole,
        out_shape=jax.ShapeDtypeStruct((blocks, 136, 128), BF16),
        input_output_aliases={5: 0} if more else {},
        compiler_params=params(8),
        cost_estimate=cost(100 * MIB, 900 * 1024),
        name="merge",
    )(own, codes, sums, stats, after, *more)


def finish_body(count, lg_ref, *refs):
    messages, normed, out_ref = refs[:count], refs[count:-1], refs[-1]
    for b in range(messages[0].shape[0]):
        peaks, denoms = [], []
        for message in messages:
            s = message[b, 128:136, :].astype(F32)
            peaks.append(s[0:1] + s[1:2] + s[2:3])
            denoms.append(s[3:4] + s[4:5] + s[5:6])
        peak = functools.reduce(jnp.maximum, peaks)
        gains = [jnp.exp(p - peak) for p in peaks]
        denom = sum(d * g for d, g in zip(denoms, gains))
        sums = sum(m[b, 0:128, :].astype(F32) * g for m, g in zip(messages, gains))
        retrieved = (sums / denom).T
        lg = lg_ref[b * BLOCK : (b + 1) * BLOCK, :]
        gate = jax.nn.sigmoid(jnp.concatenate([lg[:, 4:5], lg[:, 5:6]], axis=0))
        mixed = (normed[b][0] + gate * retrieved).astype(BF16)
        for h in range(2):
            out_ref[b * BLOCK : (b + 1) * BLOCK, h * 128 : (h + 1) * 128] = mixed[
                h * BLOCK : (h + 1) * BLOCK
            ]


def finish(messages, logits, normed):
    rows = logits.shape[0]
    return pl.pallas_call(
        functools.partial(finish_body, len(messages)),
        out_shape=jax.ShapeDtypeStruct((rows, 256), BF16),
        compiler_params=params(16),
        cost_estimate=cost(100 * MIB, 2 * MIB),
        name="finish",
    )(logits, *messages, *normed)


def per_device(
    tokens,
    owners,
    entries,
    store,
    mixer_query_weight,
    mixer_key_weight,
    mixer_value_weight,
    strength_weight,
    decay_weight,
    head_decay_rate,
    extra_forgetting_exponent,
    output_norm_gain,
    retrieval_query_weight,
    passage_key_weight,
    passage_value_weight,
    retrieval_gate_weight,
):
    devices = lax.axis_size("st")
    me = lax.axis_index("st")
    core = lax.rem(me, 2)
    reach = devices // 4
    blocks = owners.shape[0]

    step = [2 if i % 2 == 0 else -2 for i in range(devices)]

    def hops(lane, chips=1, ends=False):
        pairs = [(i, (i + chips * step[i]) % devices) for i in range(devices)]
        if lane == "other" and ends:
            pairs = [(i ^ 1, j) for i, j in pairs]
        return pairs

    def send(x, pairs):
        return lax.ppermute(x, "st", pairs)

    def second(pairs):
        return [(i, j) for i, j in pairs if i % 2 == 1]

    def reverse(pairs):
        return [(j, i) for i, j in pairs]

    query = query_message(tokens, retrieval_query_weight, owners.T, entries.T)
    own = {0: query}
    other = {}
    gain = output_norm_gain.reshape(1, 128)
    extra = extra_forgetting_exponent.T
    where_own = jnp.stack([me >> 1, me & 1])
    part = {}

    def compute_parts(names, after):
        messages = [(own if lane == "own" else other)[h] for lane, h in names]
        result = parts(where_own, messages, kv_own, kv_mate, after)
        for n, name in enumerate(names):
            part[name] = (result, n)
        return result[1]

    lanes = {"own": own, "other": other}
    for name, lane in lanes.items():
        lane[2] = send(query, hops(name, 2, True))
    kv_own = project_passages(store, passage_key_weight, passage_value_weight, query)
    kv_mate = send(kv_own, [(i, i ^ 1) for i in range(devices)])
    for name, lane in lanes.items():
        lane[1] = send(query, hops(name, 1, True))
    for h in range(3, reach + 1):
        for name, lane in lanes.items():
            pairs = hops(name)
            lane[h] = send(lane[h - 1], second(pairs) if h == reach else pairs)
    qkv, logits = mixer_inputs(
        tokens,
        mixer_query_weight,
        mixer_key_weight,
        mixer_value_weight,
        strength_weight.T,
        decay_weight.T,
        retrieval_gate_weight.T,
        own[2],
    )
    last = compute_parts([("own", 0)], logits)
    for h in ORDER:
        last = compute_parts([("own", h), ("other", h)], last)

    normed = []
    state = jnp.zeros((2, 128, 128), F32)

    def mixer_step(after):
        nonlocal state
        result, state = mixer(
            qkv, logits, extra, head_decay_rate, gain, state, after, len(normed), 1
        )
        normed.append(result)
        return state

    came = {}
    near = {}
    for h in range(reach, 1, -1):
        for name, lane in lanes.items():
            if h == reach:
                last = far_message(where_own, lane[h], kv_own, kv_mate, blocks, last)
            else:
                start = "core_0" if h == reach - 1 else "none"
                last = merge(where_own, part[(name, h)], blocks, last, came[name], start)
            pairs = hops(name, 2, True) if h == 2 else hops(name)
            pairs = second(pairs) if h == reach else pairs
            came[name] = send(last, reverse(pairs))
        last = mixer_step(last)
        if h in NEAR:
            name = NEAR[h]
            last = merge(where_own, part[(name, 1)], blocks, last, None, "all")
            near[name] = send(last, reverse(hops(name, 1, True)))
    while len(normed) < blocks:
        last = mixer_step(last)
    came["own"] = merge(where_own, part[("own", 0)], blocks, last, came["own"])
    messages = (came["own"], came["other"], near["own"], near["other"])
    return finish(messages, logits, normed)


ORDER = (2, 3, 1, 4, 5, 6, 7)
NEAR = {5: "own", 4: "other"}


def solution(mesh):
    return jax.shard_map(
        per_device,
        mesh=mesh,
        in_specs=(
            P(("grp", "st"), None),
            P(("grp", "st"), None),
            P(("grp", "st"), None),
            P(("grp", "st"), None, None),
            P(None, "tp"),
            P(None, "tp"),
            P(None, "tp"),
            P(None, "tp"),
            P(None, "tp"),
            P("tp"),
            P(("grp", "st"), "tp"),
            P(),
            P(None, "tp"),
            P(None, "tp"),
            P(None, "tp"),
            P(None, "tp"),
        ),
        out_specs=P(("grp", "st"), "tp"),
        check_vma=False,
    )
```

```python
import functools

import jax
import jax.numpy as jnp
from jax import lax
from jax.experimental import pallas as pl
from jax.experimental.pallas import tpu as pltpu
from jax.sharding import PartitionSpec as P


BLOCK = 64
SLOTS = 4
EPS = 1e-06
NONE = -1e30
MIB = 1024 * 1024
BIG = 52
F32 = jnp.float32
BF16 = jnp.bfloat16
VMEM = pltpu.VMEM


def nt(left, right):
    return lax.dot_general(left, right, (((1,), (1,)), ((), ())), preferred_element_type=F32)


def nn(left, right):
    return jnp.dot(left, right, preferred_element_type=F32)


def tn(left, right):
    return lax.dot_general(left, right, (((0,), (0,)), ((), ())), preferred_element_type=F32)


def params(limit, **more):
    return pltpu.CompilerParams(vmem_limit_bytes=limit * MIB, **more)


def cost(flops, size, trans=0):
    return pl.CostEstimate(flops=flops, bytes_accessed=size, transcendentals=trans)


def pieces(src, dst, sems, first, count):
    rows = dst.shape[0] // count
    return [
        pltpu.make_async_copy(
            src.at[pl.ds(i * rows, rows)], dst.at[pl.ds(i * rows, rows)], sems.at[first + i]
        )
        for i in range(count)
    ]


def query_body(x_hbm, w_hbm, owners_hbm, entries_hbm, out_ref, x_buf, w_buf, owners_ref, entries_ref, sems):
    tiles, rows, _ = x_buf.shape
    loads = pieces(w_hbm, w_buf, sems, 0, 4)
    x_loads = [
        pieces(x_hbm.at[pl.ds(i * rows, rows)], x_buf.at[i], sems, 4 + i * 4, 4)
        for i in range(tiles)
    ]
    tables = [
        pltpu.make_async_copy(owners_hbm, owners_ref, sems.at[tiles * 4 + 4]),
        pltpu.make_async_copy(entries_hbm, entries_ref, sems.at[tiles * 4 + 5]),
    ]
    for copies in [loads] + x_loads + [tables]:
        for copy in copies:
            copy.start()
    per, count = owners_ref.shape
    blocks = tiles * rows // BLOCK
    for table in tables:
        table.wait()
    names = jnp.concatenate([owners_ref[...] + 1, entries_ref[...]], axis=0).astype(F32)
    out_ref[blocks * 128 :, :] = jnp.zeros((2 * per, 128), BF16)
    out_ref[blocks * 128 :, 0:count] = names.astype(BF16)
    for copy in loads:
        copy.wait()
    for i in range(tiles):
        for copy in x_loads[i]:
            copy.wait()
        q = nn(x_buf[i], w_buf[...]).astype(BF16)
        for n in range(rows // BLOCK):
            at = (i * rows // BLOCK + n) * 128
            for h in range(2):
                out_ref[at + h * BLOCK : at + (h + 1) * BLOCK, :] = q[
                    n * BLOCK : (n + 1) * BLOCK, h * 128 : (h + 1) * 128
                ]


def query_message(x, w, owners, entries, tiles=2):
    rows, depth = x.shape
    hbm = pl.BlockSpec(memory_space=pltpu.HBM)
    whole = pl.BlockSpec(memory_space=VMEM)
    return pl.pallas_call(
        query_body,
        in_specs=[hbm] * 4,
        out_specs=whole,
        out_shape=jax.ShapeDtypeStruct((rows * 2 + 8, 128), BF16),
        scratch_shapes=[
            VMEM((tiles, rows // tiles, depth), BF16),
            VMEM(w.shape, BF16),
            VMEM(owners.shape, jnp.int32),
            VMEM(entries.shape, jnp.int32),
            pltpu.SemaphoreType.DMA((tiles * 4 + 6,)),
        ],
        compiler_params=params(BIG + 1),
        cost_estimate=cost(2 * rows * depth * 256, 2 * (rows * depth + depth * 256)),
        name="query",
    )(x, w, owners, entries)


def mixed_body(
    x_hbm, wq_hbm, wk_hbm, wv_hbm, ga_ref, gb_ref, gc_ref, after_ref, out_ref, lg_ref, x_buf, w_buf, sems
):
    tiles, tall, depth = x_buf.shape

    x_loads = [
        pieces(x_hbm.at[pl.ds(t * tall, tall)], x_buf.at[t], sems, t * 4, 4) for t in range(tiles)
    ]
    w_loads = [
        pieces(w, w_buf.at[i], sems, (tiles + i) * 4, 4)
        for i, w in enumerate((wq_hbm, wk_hbm, wv_hbm))
    ]
    for copies in x_loads + w_loads:
        for copy in copies:
            copy.start()
    none = jnp.zeros((2, depth), BF16)
    gates = jnp.concatenate([ga_ref[...], gb_ref[...], gc_ref[...], none], axis=0)
    for t in range(tiles):
        for copy in x_loads[t]:
            copy.wait()
        lg_ref[t * tall : (t + 1) * tall, :] = nt(x_buf[t], gates)
    for copy in w_loads[0]:
        copy.wait()

    def piece(step, _):
        i, t = step // tiles, step % tiles
        rows = nn(x_buf[t], w_buf[i]).astype(BF16)
        for n in range(tall // BLOCK):
            for h in range(2):
                out_ref[i, t * (tall // BLOCK) + n, h * BLOCK : (h + 1) * BLOCK, :] = rows[
                    n * BLOCK : (n + 1) * BLOCK, h * 128 : (h + 1) * 128
                ]
        return 0

    lax.fori_loop(0, tiles, piece, 0)
    for copy in w_loads[1] + w_loads[2]:
        copy.wait()
    lax.fori_loop(tiles, 3 * tiles, piece, 0)


def mixer_inputs(x, wq, wk, wv, ga, gb, gc, after, tiles=2):
    rows, depth = x.shape
    hbm = pl.BlockSpec(memory_space=pltpu.HBM)
    whole = pl.BlockSpec(memory_space=VMEM)
    return pl.pallas_call(
        mixed_body,
        in_specs=[hbm] * 4 + [whole] * 3 + [pl.BlockSpec(memory_space=pl.ANY)],
        out_specs=[whole] * 2,
        out_shape=[
            jax.ShapeDtypeStruct((3, rows // BLOCK, 128, 128), BF16),
            jax.ShapeDtypeStruct((rows, 8), F32),
        ],
        scratch_shapes=[
            VMEM((tiles, rows // tiles, depth), BF16),
            VMEM((3,) + wq.shape, BF16),
            pltpu.SemaphoreType.DMA((tiles * 4 + 12,)),
        ],
        compiler_params=params(BIG),
        cost_estimate=cost(2 * rows * depth * 768, 2 * (rows * depth + depth * 768)),
        name="mixer_inputs",
    )(x, wq, wk, wv, ga, gb, gc, after)


def passages_body(store_hbm, wk_hbm, wv_hbm, after_ref, out_ref, x_buf, w_buf, sems):
    chunks, tall, _ = x_buf.shape
    rows = out_ref.shape[1] // 4
    count = tall // rows

    def load(i):
        return pieces(store_hbm.at[pl.ds(i * tall, tall)], x_buf.at[i], sems, i * 4, 4)

    weights = pieces(wk_hbm, w_buf.at[0], sems, chunks * 4, 4)
    weights += pieces(wv_hbm, w_buf.at[1], sems, chunks * 4 + 4, 4)
    for copy in load(0) + weights:
        copy.start()
    for i in range(1, chunks):
        for copy in load(i):
            copy.start()
    for copy in weights:
        copy.wait()

    def chunk(i, _):
        for copy in load(i):
            copy.wait()
        keys = nn(x_buf[i], w_buf[0]).astype(BF16)
        values = nn(x_buf[i], w_buf[1]).astype(BF16).astype(F32)
        for p in range(count):
            span = slice(p * rows, (p + 1) * rows)
            at = i * count + p
            for h in range(2):
                out_ref[at, h * rows : (h + 1) * rows, :] = keys[span, h * 128 : (h + 1) * 128]
            stacked = jnp.concatenate([values[span, :128], values[span, 128:]], axis=0)
            out_ref[at, 128:256, :] = stacked.T.astype(BF16)
        return 0

    lax.fori_loop(0, chunks, chunk, 0)


def project_passages(store, wk, wv, after, chunks=4):
    number, rows, depth = store.shape
    hbm = pl.BlockSpec(memory_space=pltpu.HBM)
    return pl.pallas_call(
        passages_body,
        in_specs=[hbm, hbm, hbm, pl.BlockSpec(memory_space=pl.ANY)],
        out_specs=pl.BlockSpec(memory_space=VMEM),
        out_shape=jax.ShapeDtypeStruct((number, 256, 128), BF16),
        scratch_shapes=[
            VMEM((chunks, number * rows // chunks, depth), BF16),
            VMEM((2,) + wk.shape, BF16),
            pltpu.SemaphoreType.DMA((chunks * 4 + 8,)),
        ],
        compiler_params=params(BIG),
        cost_estimate=cost(2 * number * rows * depth * 512, 2 * number * rows * depth),
        name="passages",
    )(store.reshape(number * rows, depth), wk, wv, after)


def mixer_body(
    first, qkv_ref, lg_ref, ex_ref, rate_ref, gain_ref, s_ref, after_ref, out_ref, s_out_ref
):
    ri = lax.broadcasted_iota(jnp.int32, (128, 128), 0)
    ci = lax.broadcasted_iota(jnp.int32, (128, 128), 1)
    same = (ri >= BLOCK) == (ci >= BLOCK)
    lower = same & (ri >= ci)
    strict = same & (ri > ci)
    upper = same & (ri <= ci)
    diag = ri == ci
    top = lax.broadcasted_iota(jnp.int32, (128, 1), 0) < BLOCK
    rate = jnp.where(top, rate_ref[0], rate_ref[1])
    pieces = []
    for n in range(qkv_ref.shape[1]):
        lg = lg_ref[n * BLOCK : (n + 1) * BLOCK, :]
        at = (first + n) * BLOCK
        ex = jnp.concatenate([ex_ref[0:1, at : at + BLOCK], ex_ref[1:2, at : at + BLOCK]], axis=1)
        beta = jax.nn.sigmoid(jnp.concatenate([lg[:, 0:1], lg[:, 1:2]], axis=0))
        pre = jnp.concatenate([lg[:, 2:3], lg[:, 3:4]], axis=0)
        extra = jnp.sum(jnp.where(diag, ex, 0.0), axis=1, keepdims=True)
        soft = jnp.maximum(pre, 0.0) + jnp.log1p(jnp.exp(-jnp.abs(pre)))
        g = extra - rate * soft
        g_row = jnp.sum(jnp.where(diag, g, 0.0), axis=0, keepdims=True)
        c = jnp.sum(jnp.where(lower, g_row, 0.0), axis=1, keepdims=True)
        total = jnp.sum(jnp.where(same, g_row, 0.0), axis=1, keepdims=True)
        c_row = jnp.sum(jnp.where(upper, g, 0.0), axis=0, keepdims=True)
        damping = jnp.where(lower, jnp.exp(jnp.where(lower, c - c_row, 0.0)), 0.0)
        q = qkv_ref[0, n].astype(F32)
        k = qkv_ref[1, n].astype(F32)
        v = qkv_ref[2, n].astype(F32)
        q = q * (lax.rsqrt(jnp.sum(q * q, axis=1, keepdims=True) + EPS) * 128**-0.5)
        k = k * lax.rsqrt(jnp.sum(k * k, axis=1, keepdims=True) + EPS)
        kb = k * beta
        decay = jnp.exp(c)
        k16 = k.astype(BF16)
        power = jnp.where(strict, nt(kb.astype(BF16), k16) * damping, 0.0)
        within = (nt(q.astype(BF16), k16) * damping).astype(BF16)
        inverse = jnp.where(diag, 1.0, 0.0) - power
        p16 = power.astype(BF16)
        for _ in range(5):
            p16 = nn(p16, p16).astype(BF16)
            inverse = inverse + nn(inverse.astype(BF16), p16)
        inv16 = inverse.astype(BF16)
        mix = nn(inv16, (kb * decay).astype(BF16)).astype(BF16)
        base = nn(inv16, (v * beta).astype(BF16))
        q_dec = (q * decay).astype(BF16)
        k_tail = (k * jnp.exp(total - c)).astype(BF16)
        pieces.append((mix, base, within, q_dec, k_tail, jnp.exp(total)))
    state = [s_ref[0], s_ref[1]]
    for n, (mix, base, within, q_dec, k_tail, keep) in enumerate(pieces):
        fresh, far = [], []
        for h in range(2):
            rows = slice(h * BLOCK, (h + 1) * BLOCK)
            both = nn(jnp.concatenate([mix[rows], q_dec[rows]], axis=0), state[h].astype(BF16))
            fresh.append(base[rows] - both[:BLOCK])
            far.append(both[BLOCK:])
        f16 = jnp.concatenate(fresh, axis=0).astype(BF16)
        recur = jnp.concatenate(far, axis=0) + nn(within, f16)
        for h in range(2):
            rows = slice(h * BLOCK, (h + 1) * BLOCK)
            state[h] = state[h] * keep[h * BLOCK : h * BLOCK + 1] + tn(k_tail[rows], f16[rows])
        scale = lax.rsqrt(jnp.mean(recur * recur, axis=1, keepdims=True) + EPS)
        out_ref[n] = recur * scale * gain_ref[...]
    s_out_ref[0] = state[0]
    s_out_ref[1] = state[1]


def mixer(qkv, logits, extra, rate, gain, state, after, first, number):
    at = first // number
    return pl.pallas_call(
        functools.partial(mixer_body, first),
        grid=(1,),
        in_specs=[
            pl.BlockSpec((3, number, 128, 128), lambda i: (0, at, 0, 0)),
            pl.BlockSpec((number * BLOCK, logits.shape[1]), lambda i: (at, 0)),
            pl.BlockSpec(extra.shape, lambda i: (0, 0)),
            pl.BlockSpec(memory_space=pltpu.SMEM),
            pl.BlockSpec((1, 128), lambda i: (0, 0)),
            pl.BlockSpec((2, 128, 128), lambda i: (0, 0, 0)),
            pl.BlockSpec(memory_space=pl.ANY),
        ],
        out_specs=[
            pl.BlockSpec((number, 128, 128), lambda i: (0, 0, 0)),
            pl.BlockSpec((2, 128, 128), lambda i: (0, 0, 0)),
        ],
        out_shape=[
            jax.ShapeDtypeStruct((number, 128, 128), F32),
            jax.ShapeDtypeStruct((2, 128, 128), F32),
        ],
        compiler_params=params(16),
        cost_estimate=cost(number * 1000 * MIB // 2, number * 300 * 1024),
        name="mixer",
    )(qkv, logits, extra, rate, gain, state, after)


def find_parts(count, own_ref, *refs):
    messages, refs = refs[:count], refs[count:]
    (kv_ref, mate_ref, _, sums_ref, stats_ref, codes_ref) = refs
    chip, core = own_ref[0], own_ref[1]
    rows = messages[0].shape[0]
    row = lax.broadcasted_iota(jnp.int32, (8, 128), 0)
    lane = lax.broadcasted_iota(jnp.int32, (8, 128), 1)
    before = (
        lax.broadcasted_iota(jnp.int32, (128, 128), 0) < lax.broadcasted_iota(jnp.int32, (128, 128), 1)
    )
    before = jnp.where(before, 1.0, 0.0).astype(BF16)
    blocks = (rows - 8) // 128
    left = lax.broadcasted_iota(jnp.int32, (BLOCK, 128), 1) < BLOCK
    spots = []
    for n in range(count):
        table = messages[n][rows - 8 :, :].astype(F32)
        entry = jnp.concatenate([table[4:8], table[4:8]], axis=0)
        name = table.astype(jnp.int32) - 1
        hit = ((name >> 1) == chip) & (row < 4) & (lane < blocks)
        ones = jnp.where(hit, 1.0, 0.0)
        rank = nn(ones.astype(BF16), before)
        sums = jnp.sum(ones, axis=1, keepdims=True)
        first, second, third = sums[0:1], sums[1:2], sums[2:3]
        rank = rank + jnp.where(row > 0, first, 0.0)
        rank = rank + jnp.where(row > 1, second, 0.0)
        rank = rank + jnp.where(row > 2, third, 0.0)
        far = jnp.where((name & 1) == core, 0.0, 16.0)
        code = lane.astype(F32) * 32.0 + far + entry + 1.0
        for r in range(SLOTS):
            value = jnp.where(hit & (rank == float(r)), code, 0.0)
            spots.append(jnp.sum(value).astype(jnp.int32))
    for i, spot in enumerate(spots):
        codes_ref[i] = spot

    def some(step, _):
        found = []
        for n in range(count):
            for r in range(2):
                i = n * SLOTS + step * 2 + r
                spot = jnp.maximum(codes_ref[i] - 1, 0)
                at = pl.multiple_of((spot >> 5) * 128, 128)
                q = messages[n][pl.ds(at, 128), :]
                kv = jnp.where((spot & 16) != 0, mate_ref[spot & 15], kv_ref[spot & 15])
                both = nt(kv[0:128], q)
                scores = jnp.where(left, both[:BLOCK], both[BLOCK:]) * 128**-0.5
                found.append((i, scores, kv[128:256]))
        weighed = []
        for i, scores, values in found:
            peak = jnp.max(scores, axis=0, keepdims=True)
            expo = jnp.exp(scores - peak)
            denom = jnp.sum(expo, axis=0, keepdims=True)
            split = jnp.concatenate(
                [jnp.where(left, expo, 0.0), jnp.where(left, 0.0, expo)], axis=0
            ).astype(BF16)
            weighed.append((i, nn(values, split), jnp.where(row == 0, peak, denom)))
        for i, sums, stats in weighed:
            sums_ref[i], stats_ref[i] = sums, stats
        return 0

    lax.fori_loop(0, SLOTS // 2, some, 0)


def parts(own, messages, kv, kv_mate, after):
    count = len(messages)
    total = count * SLOTS
    whole = pl.BlockSpec(memory_space=VMEM)
    scalars = pl.BlockSpec(memory_space=pltpu.SMEM)
    return pl.pallas_call(
        functools.partial(find_parts, count),
        in_specs=[scalars] + [whole] * (count + 2) + [pl.BlockSpec(memory_space=pl.ANY)],
        out_specs=[whole, whole, scalars],
        out_shape=[
            jax.ShapeDtypeStruct((total, 128, 128), F32),
            jax.ShapeDtypeStruct((total, 8, 128), F32),
            jax.ShapeDtypeStruct((total,), jnp.int32),
        ],
        compiler_params=params(12),
        cost_estimate=cost(count * 400 * MIB, count * 500 * 1024),
        name="parts",
    )(own, *messages, kv, kv_mate, after)


def split3(x):
    high = x.astype(BF16)
    rest = x - high.astype(F32)
    mid = rest.astype(BF16)
    low = (rest - mid.astype(F32)).astype(BF16)
    return high.astype(F32), mid.astype(F32), low.astype(F32)


def begin(out_ref):
    pad = lax.broadcasted_iota(jnp.int32, (8, 128), 0)
    none = jnp.where(pad == 0, NONE, 0.0).astype(BF16)
    for b in range(out_ref.shape[0]):
        out_ref[b, 0:128, :] = jnp.zeros((128, 128), BF16)
        out_ref[b, 128:136, :] = none


def merge_into(first, codes_ref, sums_ref, stats_ref, out_ref):
    for r in range(SLOTS):
        code = codes_ref[first + r]

        @pl.when(code > 0)
        def _():
            b = (code - 1) >> 5
            peak, denom = stats_ref[first + r, 0:1, :], stats_ref[first + r, 1:2, :]
            stats = out_ref[b, 128:136, :].astype(F32)
            m_old = stats[0:1] + stats[1:2] + stats[2:3]
            l_old = stats[3:4] + stats[4:5] + stats[5:6]
            m_new = jnp.maximum(m_old, peak)
            keep = jnp.exp(m_old - m_new)
            gain = jnp.exp(peak - m_new)
            l_new = l_old * keep + denom * gain
            zero = jnp.zeros((2, 128), F32)
            fresh = jnp.concatenate(split3(m_new) + split3(l_new) + (zero,), axis=0)
            out_ref[b, 128:136, :] = fresh.astype(BF16)
            mixed = out_ref[b, 0:128, :].astype(F32) * keep + sums_ref[first + r] * gain
            out_ref[b, 0:128, :] = mixed.astype(BF16)


def merge_body(first, start, own_ref, codes_ref, sums_ref, stats_ref, after_ref, *refs):
    out_ref = refs[-1]
    if start == "all":
        begin(out_ref)
    elif start == "core_0":
        pl.when(own_ref[1] == 0)(lambda: begin(out_ref))
    merge_into(first, codes_ref, sums_ref, stats_ref, out_ref)


def far_body(own_ref, q_ref, kv_ref, mate_ref, after_ref, out_ref, sums_ref, stats_ref, codes_ref):
    @pl.when(own_ref[1] != 0)
    def _():
        find_parts(1, own_ref, q_ref, kv_ref, mate_ref, after_ref, sums_ref, stats_ref, codes_ref)
        begin(out_ref)
        merge_into(0, codes_ref, sums_ref, stats_ref, out_ref)


def far_message(own, q, kv, kv_mate, blocks, after):
    whole = pl.BlockSpec(memory_space=VMEM)
    return pl.pallas_call(
        far_body,
        in_specs=[pl.BlockSpec(memory_space=pltpu.SMEM), whole, whole, whole]
        + [pl.BlockSpec(memory_space=pl.ANY)],
        out_specs=whole,
        out_shape=jax.ShapeDtypeStruct((blocks, 136, 128), BF16),
        scratch_shapes=[
            VMEM((SLOTS, 128, 128), F32),
            VMEM((SLOTS, 8, 128), F32),
            pltpu.SMEM((SLOTS,), jnp.int32),
        ],
        compiler_params=params(10),
        cost_estimate=cost(500 * MIB, 500 * 1024),
        name="far",
    )(own, q, kv, kv_mate, after)


def merge(own, part, blocks, after, msg=None, start="none"):
    (sums, stats, codes), n = part
    whole = pl.BlockSpec(memory_space=VMEM)
    scalars = pl.BlockSpec(memory_space=pltpu.SMEM)
    more = () if msg is None else (msg,)
    return pl.pallas_call(
        functools.partial(merge_body, n * SLOTS, start),
        in_specs=[scalars, scalars, whole, whole, pl.BlockSpec(memory_space=pl.ANY)]
        + [whole] * len(more),
        out_specs=whole,
        out_shape=jax.ShapeDtypeStruct((blocks, 136, 128), BF16),
        input_output_aliases={5: 0} if more else {},
        compiler_params=params(8),
        cost_estimate=cost(100 * MIB, 900 * 1024),
        name="merge",
    )(own, codes, sums, stats, after, *more)


def finish_body(count, lg_ref, *refs):
    messages, normed, out_ref = refs[:count], refs[count:-1], refs[-1]
    for b in range(messages[0].shape[0]):
        peaks, denoms = [], []
        for message in messages:
            s = message[b, 128:136, :].astype(F32)
            peaks.append(s[0:1] + s[1:2] + s[2:3])
            denoms.append(s[3:4] + s[4:5] + s[5:6])
        peak = functools.reduce(jnp.maximum, peaks)
        gains = [jnp.exp(p - peak) for p in peaks]
        denom = sum(d * g for d, g in zip(denoms, gains))
        sums = sum(m[b, 0:128, :].astype(F32) * g for m, g in zip(messages, gains))
        retrieved = (sums / denom).T
        lg = lg_ref[b * BLOCK : (b + 1) * BLOCK, :]
        gate = jax.nn.sigmoid(jnp.concatenate([lg[:, 4:5], lg[:, 5:6]], axis=0))
        mixed = (normed[b][0] + gate * retrieved).astype(BF16)
        for h in range(2):
            out_ref[b * BLOCK : (b + 1) * BLOCK, h * 128 : (h + 1) * 128] = mixed[
                h * BLOCK : (h + 1) * BLOCK
            ]


def finish(messages, logits, normed):
    rows = logits.shape[0]
    return pl.pallas_call(
        functools.partial(finish_body, len(messages)),
        out_shape=jax.ShapeDtypeStruct((rows, 256), BF16),
        compiler_params=params(16),
        cost_estimate=cost(100 * MIB, 2 * MIB),
        name="finish",
    )(logits, *messages, *normed)


def per_device(
    tokens,
    owners,
    entries,
    store,
    mixer_query_weight,
    mixer_key_weight,
    mixer_value_weight,
    strength_weight,
    decay_weight,
    head_decay_rate,
    extra_forgetting_exponent,
    output_norm_gain,
    retrieval_query_weight,
    passage_key_weight,
    passage_value_weight,
    retrieval_gate_weight,
):
    devices = lax.axis_size("st")
    me = lax.axis_index("st")
    core = lax.rem(me, 2)
    reach = devices // 4
    blocks = owners.shape[0]

    step = [2 if i % 2 == 0 else -2 for i in range(devices)]

    def hops(lane, chips=1, ends=False):
        pairs = [(i, (i + chips * step[i]) % devices) for i in range(devices)]
        if lane == "other" and ends:
            pairs = [(i ^ 1, j) for i, j in pairs]
        return pairs

    def send(x, pairs):
        return lax.ppermute(x, "st", pairs)

    def second(pairs):
        return [(i, j) for i, j in pairs if i % 2 == 1]

    def reverse(pairs):
        return [(j, i) for i, j in pairs]

    query = query_message(tokens, retrieval_query_weight, owners.T, entries.T)
    own = {0: query}
    other = {}
    gain = output_norm_gain.reshape(1, 128)
    extra = extra_forgetting_exponent.T
    where_own = jnp.stack([me >> 1, me & 1])
    part = {}

    def compute_parts(names, after):
        messages = [(own if lane == "own" else other)[h] for lane, h in names]
        result = parts(where_own, messages, kv_own, kv_mate, after)
        for n, name in enumerate(names):
            part[name] = (result, n)
        return result[1]

    lanes = {"own": own, "other": other}
    for name, lane in lanes.items():
        lane[2] = send(query, hops(name, 2, True))
    kv_own = project_passages(store, passage_key_weight, passage_value_weight, query)
    kv_mate = send(kv_own, [(i, i ^ 1) for i in range(devices)])
    for name, lane in lanes.items():
        lane[1] = send(query, hops(name, 1, True))
    for h in range(3, reach + 1):
        for name, lane in lanes.items():
            pairs = hops(name)
            lane[h] = send(lane[h - 1], second(pairs) if h == reach else pairs)
    qkv, logits = mixer_inputs(
        tokens,
        mixer_query_weight,
        mixer_key_weight,
        mixer_value_weight,
        strength_weight.T,
        decay_weight.T,
        retrieval_gate_weight.T,
        own[2],
    )
    last = compute_parts([("own", 0)], logits)
    for h in ORDER:
        last = compute_parts([("own", h), ("other", h)], last)

    normed = []
    state = jnp.zeros((2, 128, 128), F32)

    def mixer_step(after):
        nonlocal state
        result, state = mixer(
            qkv, logits, extra, head_decay_rate, gain, state, after, len(normed), 1
        )
        normed.append(result)
        return state

    came = {}
    near = {}
    for h in range(reach, 1, -1):
        for name, lane in lanes.items():
            if h == reach:
                last = far_message(where_own, lane[h], kv_own, kv_mate, blocks, last)
            else:
                start = "core_0" if h == reach - 1 else "none"
                last = merge(where_own, part[(name, h)], blocks, last, came[name], start)
            pairs = hops(name, 2, True) if h == 2 else hops(name)
            pairs = second(pairs) if h == reach else pairs
            came[name] = send(last, reverse(pairs))
        last = mixer_step(last)
        if h in NEAR:
            name = NEAR[h]
            last = merge(where_own, part[(name, 1)], blocks, last, None, "all")
            near[name] = send(last, reverse(hops(name, 1, True)))
    while len(normed) < blocks:
        last = mixer_step(last)
    came["own"] = merge(where_own, part[("own", 0)], blocks, last, came["own"])
    messages = (came["own"], came["other"], near["own"], near["other"])
    return finish(messages, logits, normed)


ORDER = (2, 3, 1, 4, 5, 6, 7)
NEAR = {5: "own", 4: "other"}


def solution(mesh):
    return jax.shard_map(
        per_device,
        mesh=mesh,
        in_specs=(
            P(("grp", "st"), None),
            P(("grp", "st"), None),
            P(("grp", "st"), None),
            P(("grp", "st"), None, None),
            P(None, "tp"),
            P(None, "tp"),
            P(None, "tp"),
            P(None, "tp"),
            P(None, "tp"),
            P("tp"),
            P(("grp", "st"), "tp"),
            P(),
            P(None, "tp"),
            P(None, "tp"),
            P(None, "tp"),
            P(None, "tp"),
        ),
        out_specs=P(("grp", "st"), "tp"),
        check_vma=False,
    )
```

```python
import functools

import jax
import jax.numpy as jnp
from jax import lax
from jax.experimental import pallas as pl
from jax.experimental.pallas import tpu as pltpu
from jax.sharding import PartitionSpec as P


BLOCK = 64
SLOTS = 4
EPS = 1e-06
NONE = -1e30
MIB = 1024 * 1024
BIG = 52
F32 = jnp.float32
BF16 = jnp.bfloat16
VMEM = pltpu.VMEM


def nt(left, right):
    return lax.dot_general(left, right, (((1,), (1,)), ((), ())), preferred_element_type=F32)


def nn(left, right):
    return jnp.dot(left, right, preferred_element_type=F32)


def tn(left, right):
    return lax.dot_general(left, right, (((0,), (0,)), ((), ())), preferred_element_type=F32)


def params(limit, **more):
    return pltpu.CompilerParams(vmem_limit_bytes=limit * MIB, **more)


def cost(flops, size, trans=0):
    return pl.CostEstimate(flops=flops, bytes_accessed=size, transcendentals=trans)


def pieces(src, dst, sems, first, count):
    rows = dst.shape[0] // count
    return [
        pltpu.make_async_copy(
            src.at[pl.ds(i * rows, rows)], dst.at[pl.ds(i * rows, rows)], sems.at[first + i]
        )
        for i in range(count)
    ]


def query_body(x_hbm, w_hbm, owners_hbm, entries_hbm, out_ref, x_buf, w_buf, owners_ref, entries_ref, sems):
    tiles, rows, _ = x_buf.shape
    loads = pieces(w_hbm, w_buf, sems, 0, 4)
    x_loads = [
        pieces(x_hbm.at[pl.ds(i * rows, rows)], x_buf.at[i], sems, 4 + i * 4, 4)
        for i in range(tiles)
    ]
    tables = [
        pltpu.make_async_copy(owners_hbm, owners_ref, sems.at[tiles * 4 + 4]),
        pltpu.make_async_copy(entries_hbm, entries_ref, sems.at[tiles * 4 + 5]),
    ]
    for copies in [loads] + x_loads + [tables]:
        for copy in copies:
            copy.start()
    per, count = owners_ref.shape
    blocks = tiles * rows // BLOCK
    for table in tables:
        table.wait()
    names = jnp.concatenate([owners_ref[...] + 1, entries_ref[...]], axis=0).astype(F32)
    out_ref[blocks * 128 :, :] = jnp.zeros((2 * per, 128), BF16)
    out_ref[blocks * 128 :, 0:count] = names.astype(BF16)
    for copy in loads:
        copy.wait()
    for i in range(tiles):
        for copy in x_loads[i]:
            copy.wait()
        q = nn(x_buf[i], w_buf[...]).astype(BF16)
        for n in range(rows // BLOCK):
            at = (i * rows // BLOCK + n) * 128
            for h in range(2):
                out_ref[at + h * BLOCK : at + (h + 1) * BLOCK, :] = q[
                    n * BLOCK : (n + 1) * BLOCK, h * 128 : (h + 1) * 128
                ]


def query_message(x, w, owners, entries, tiles=2):
    rows, depth = x.shape
    hbm = pl.BlockSpec(memory_space=pltpu.HBM)
    whole = pl.BlockSpec(memory_space=VMEM)
    return pl.pallas_call(
        query_body,
        in_specs=[hbm] * 4,
        out_specs=whole,
        out_shape=jax.ShapeDtypeStruct((rows * 2 + 8, 128), BF16),
        scratch_shapes=[
            VMEM((tiles, rows // tiles, depth), BF16),
            VMEM(w.shape, BF16),
            VMEM(owners.shape, jnp.int32),
            VMEM(entries.shape, jnp.int32),
            pltpu.SemaphoreType.DMA((tiles * 4 + 6,)),
        ],
        compiler_params=params(BIG + 1),
        cost_estimate=cost(2 * rows * depth * 256, 2 * (rows * depth + depth * 256)),
        name="query",
    )(x, w, owners, entries)


def mixed_body(
    x_hbm, wq_hbm, wk_hbm, wv_hbm, ga_ref, gb_ref, gc_ref, after_ref, out_ref, lg_ref, x_buf, w_buf, sems
):
    tiles, tall, depth = x_buf.shape

    x_loads = [
        pieces(x_hbm.at[pl.ds(t * tall, tall)], x_buf.at[t], sems, t * 4, 4) for t in range(tiles)
    ]
    w_loads = [
        pieces(w, w_buf.at[i], sems, (tiles + i) * 4, 4)
        for i, w in enumerate((wq_hbm, wk_hbm, wv_hbm))
    ]
    for copies in x_loads + w_loads:
        for copy in copies:
            copy.start()
    none = jnp.zeros((2, depth), BF16)
    gates = jnp.concatenate([ga_ref[...], gb_ref[...], gc_ref[...], none], axis=0)
    for t in range(tiles):
        for copy in x_loads[t]:
            copy.wait()
        lg_ref[t * tall : (t + 1) * tall, :] = nt(x_buf[t], gates)
    for copy in w_loads[0]:
        copy.wait()

    def piece(step, _):
        i, t = step // tiles, step % tiles
        rows = nn(x_buf[t], w_buf[i]).astype(BF16)
        for n in range(tall // BLOCK):
            for h in range(2):
                out_ref[i, t * (tall // BLOCK) + n, h * BLOCK : (h + 1) * BLOCK, :] = rows[
                    n * BLOCK : (n + 1) * BLOCK, h * 128 : (h + 1) * 128
                ]
        return 0

    lax.fori_loop(0, tiles, piece, 0)
    for copy in w_loads[1] + w_loads[2]:
        copy.wait()
    lax.fori_loop(tiles, 3 * tiles, piece, 0)


def mixer_inputs(x, wq, wk, wv, ga, gb, gc, after, tiles=2):
    rows, depth = x.shape
    hbm = pl.BlockSpec(memory_space=pltpu.HBM)
    whole = pl.BlockSpec(memory_space=VMEM)
    return pl.pallas_call(
        mixed_body,
        in_specs=[hbm] * 4 + [whole] * 3 + [pl.BlockSpec(memory_space=pl.ANY)],
        out_specs=[whole] * 2,
        out_shape=[
            jax.ShapeDtypeStruct((3, rows // BLOCK, 128, 128), BF16),
            jax.ShapeDtypeStruct((rows, 8), F32),
        ],
        scratch_shapes=[
            VMEM((tiles, rows // tiles, depth), BF16),
            VMEM((3,) + wq.shape, BF16),
            pltpu.SemaphoreType.DMA((tiles * 4 + 12,)),
        ],
        compiler_params=params(BIG),
        cost_estimate=cost(2 * rows * depth * 768, 2 * (rows * depth + depth * 768)),
        name="mixer_inputs",
    )(x, wq, wk, wv, ga, gb, gc, after)


def passages_body(store_hbm, wk_hbm, wv_hbm, after_ref, out_ref, x_buf, w_buf, sems):
    chunks, tall, _ = x_buf.shape
    rows = out_ref.shape[1] // 4
    count = tall // rows

    def load(i):
        return pieces(store_hbm.at[pl.ds(i * tall, tall)], x_buf.at[i], sems, i * 4, 4)

    weights = pieces(wk_hbm, w_buf.at[0], sems, chunks * 4, 4)
    weights += pieces(wv_hbm, w_buf.at[1], sems, chunks * 4 + 4, 4)
    for copy in load(0) + weights:
        copy.start()
    for i in range(1, chunks):
        for copy in load(i):
            copy.start()
    for copy in weights:
        copy.wait()

    def chunk(i, _):
        for copy in load(i):
            copy.wait()
        keys = nn(x_buf[i], w_buf[0]).astype(BF16)
        values = nn(x_buf[i], w_buf[1]).astype(BF16).astype(F32)
        for p in range(count):
            span = slice(p * rows, (p + 1) * rows)
            at = i * count + p
            for h in range(2):
                out_ref[at, h * rows : (h + 1) * rows, :] = keys[span, h * 128 : (h + 1) * 128]
            stacked = jnp.concatenate([values[span, :128], values[span, 128:]], axis=0)
            out_ref[at, 128:256, :] = stacked.T.astype(BF16)
        return 0

    lax.fori_loop(0, chunks, chunk, 0)


def project_passages(store, wk, wv, after, chunks=4):
    number, rows, depth = store.shape
    hbm = pl.BlockSpec(memory_space=pltpu.HBM)
    return pl.pallas_call(
        passages_body,
        in_specs=[hbm, hbm, hbm, pl.BlockSpec(memory_space=pl.ANY)],
        out_specs=pl.BlockSpec(memory_space=VMEM),
        out_shape=jax.ShapeDtypeStruct((number, 256, 128), BF16),
        scratch_shapes=[
            VMEM((chunks, number * rows // chunks, depth), BF16),
            VMEM((2,) + wk.shape, BF16),
            pltpu.SemaphoreType.DMA((chunks * 4 + 8,)),
        ],
        compiler_params=params(BIG),
        cost_estimate=cost(2 * number * rows * depth * 512, 2 * number * rows * depth),
        name="passages",
    )(store.reshape(number * rows, depth), wk, wv, after)


def mixer_body(
    first, qkv_ref, lg_ref, ex_ref, rate_ref, gain_ref, s_ref, after_ref, out_ref, s_out_ref
):
    ri = lax.broadcasted_iota(jnp.int32, (128, 128), 0)
    ci = lax.broadcasted_iota(jnp.int32, (128, 128), 1)
    same = (ri >= BLOCK) == (ci >= BLOCK)
    lower = same & (ri >= ci)
    strict = same & (ri > ci)
    upper = same & (ri <= ci)
    diag = ri == ci
    top = lax.broadcasted_iota(jnp.int32, (128, 1), 0) < BLOCK
    rate = jnp.where(top, rate_ref[0], rate_ref[1])
    pieces = []
    for n in range(qkv_ref.shape[1]):
        lg = lg_ref[n * BLOCK : (n + 1) * BLOCK, :]
        at = (first + n) * BLOCK
        ex = jnp.concatenate([ex_ref[0:1, at : at + BLOCK], ex_ref[1:2, at : at + BLOCK]], axis=1)
        beta = jax.nn.sigmoid(jnp.concatenate([lg[:, 0:1], lg[:, 1:2]], axis=0))
        pre = jnp.concatenate([lg[:, 2:3], lg[:, 3:4]], axis=0)
        extra = jnp.sum(jnp.where(diag, ex, 0.0), axis=1, keepdims=True)
        soft = jnp.maximum(pre, 0.0) + jnp.log1p(jnp.exp(-jnp.abs(pre)))
        g = extra - rate * soft
        g_row = jnp.sum(jnp.where(diag, g, 0.0), axis=0, keepdims=True)
        c = jnp.sum(jnp.where(lower, g_row, 0.0), axis=1, keepdims=True)
        total = jnp.sum(jnp.where(same, g_row, 0.0), axis=1, keepdims=True)
        c_row = jnp.sum(jnp.where(upper, g, 0.0), axis=0, keepdims=True)
        damping = jnp.where(lower, jnp.exp(jnp.where(lower, c - c_row, 0.0)), 0.0)
        q = qkv_ref[0, n].astype(F32)
        k = qkv_ref[1, n].astype(F32)
        v = qkv_ref[2, n].astype(F32)
        q = q * (lax.rsqrt(jnp.sum(q * q, axis=1, keepdims=True) + EPS) * 128**-0.5)
        k = k * lax.rsqrt(jnp.sum(k * k, axis=1, keepdims=True) + EPS)
        kb = k * beta
        decay = jnp.exp(c)
        k16 = k.astype(BF16)
        power = jnp.where(strict, nt(kb.astype(BF16), k16) * damping, 0.0)
        within = (nt(q.astype(BF16), k16) * damping).astype(BF16)
        inverse = jnp.where(diag, 1.0, 0.0) - power
        p16 = power.astype(BF16)
        for _ in range(5):
            p16 = nn(p16, p16).astype(BF16)
            inverse = inverse + nn(inverse.astype(BF16), p16)
        inv16 = inverse.astype(BF16)
        mix = nn(inv16, (kb * decay).astype(BF16)).astype(BF16)
        base = nn(inv16, (v * beta).astype(BF16))
        q_dec = (q * decay).astype(BF16)
        k_tail = (k * jnp.exp(total - c)).astype(BF16)
        pieces.append((mix, base, within, q_dec, k_tail, jnp.exp(total)))
    state = [s_ref[0], s_ref[1]]
    for n, (mix, base, within, q_dec, k_tail, keep) in enumerate(pieces):
        fresh, far = [], []
        for h in range(2):
            rows = slice(h * BLOCK, (h + 1) * BLOCK)
            both = nn(jnp.concatenate([mix[rows], q_dec[rows]], axis=0), state[h].astype(BF16))
            fresh.append(base[rows] - both[:BLOCK])
            far.append(both[BLOCK:])
        f16 = jnp.concatenate(fresh, axis=0).astype(BF16)
        recur = jnp.concatenate(far, axis=0) + nn(within, f16)
        for h in range(2):
            rows = slice(h * BLOCK, (h + 1) * BLOCK)
            state[h] = state[h] * keep[h * BLOCK : h * BLOCK + 1] + tn(k_tail[rows], f16[rows])
        scale = lax.rsqrt(jnp.mean(recur * recur, axis=1, keepdims=True) + EPS)
        out_ref[n] = recur * scale * gain_ref[...]
    s_out_ref[0] = state[0]
    s_out_ref[1] = state[1]


def mixer(qkv, logits, extra, rate, gain, state, after, first, number):
    at = first // number
    return pl.pallas_call(
        functools.partial(mixer_body, first),
        grid=(1,),
        in_specs=[
            pl.BlockSpec((3, number, 128, 128), lambda i: (0, at, 0, 0)),
            pl.BlockSpec((number * BLOCK, logits.shape[1]), lambda i: (at, 0)),
            pl.BlockSpec(extra.shape, lambda i: (0, 0)),
            pl.BlockSpec(memory_space=pltpu.SMEM),
            pl.BlockSpec((1, 128), lambda i: (0, 0)),
            pl.BlockSpec((2, 128, 128), lambda i: (0, 0, 0)),
            pl.BlockSpec(memory_space=pl.ANY),
        ],
        out_specs=[
            pl.BlockSpec((number, 128, 128), lambda i: (0, 0, 0)),
            pl.BlockSpec((2, 128, 128), lambda i: (0, 0, 0)),
        ],
        out_shape=[
            jax.ShapeDtypeStruct((number, 128, 128), F32),
            jax.ShapeDtypeStruct((2, 128, 128), F32),
        ],
        compiler_params=params(16),
        cost_estimate=cost(number * 1000 * MIB // 2, number * 300 * 1024),
        name="mixer",
    )(qkv, logits, extra, rate, gain, state, after)


def find_parts(count, own_ref, *refs):
    messages, refs = refs[:count], refs[count:]
    (kv_ref, mate_ref, _, sums_ref, stats_ref, codes_ref) = refs
    chip, core = own_ref[0], own_ref[1]
    rows = messages[0].shape[0]
    row = lax.broadcasted_iota(jnp.int32, (8, 128), 0)
    lane = lax.broadcasted_iota(jnp.int32, (8, 128), 1)
    before = (
        lax.broadcasted_iota(jnp.int32, (128, 128), 0) < lax.broadcasted_iota(jnp.int32, (128, 128), 1)
    )
    before = jnp.where(before, 1.0, 0.0).astype(BF16)
    blocks = (rows - 8) // 128
    left = lax.broadcasted_iota(jnp.int32, (BLOCK, 128), 1) < BLOCK
    spots = []
    for n in range(count):
        table = messages[n][rows - 8 :, :].astype(F32)
        entry = jnp.concatenate([table[4:8], table[4:8]], axis=0)
        name = table.astype(jnp.int32) - 1
        hit = ((name >> 1) == chip) & (row < 4) & (lane < blocks)
        ones = jnp.where(hit, 1.0, 0.0)
        rank = nn(ones.astype(BF16), before)
        sums = jnp.sum(ones, axis=1, keepdims=True)
        first, second, third = sums[0:1], sums[1:2], sums[2:3]
        rank = rank + jnp.where(row > 0, first, 0.0)
        rank = rank + jnp.where(row > 1, second, 0.0)
        rank = rank + jnp.where(row > 2, third, 0.0)
        far = jnp.where((name & 1) == core, 0.0, 16.0)
        code = lane.astype(F32) * 32.0 + far + entry + 1.0
        for r in range(SLOTS):
            value = jnp.where(hit & (rank == float(r)), code, 0.0)
            spots.append(jnp.sum(value).astype(jnp.int32))
    for i, spot in enumerate(spots):
        codes_ref[i] = spot

    def some(step, _):
        found = []
        for n in range(count):
            for r in range(2):
                i = n * SLOTS + step * 2 + r
                spot = jnp.maximum(codes_ref[i] - 1, 0)
                at = pl.multiple_of((spot >> 5) * 128, 128)
                q = messages[n][pl.ds(at, 128), :]
                kv = jnp.where((spot & 16) != 0, mate_ref[spot & 15], kv_ref[spot & 15])
                both = nt(kv[0:128], q)
                scores = jnp.where(left, both[:BLOCK], both[BLOCK:]) * 128**-0.5
                found.append((i, scores, kv[128:256]))
        weighed = []
        for i, scores, values in found:
            peak = jnp.max(scores, axis=0, keepdims=True)
            expo = jnp.exp(scores - peak)
            denom = jnp.sum(expo, axis=0, keepdims=True)
            split = jnp.concatenate(
                [jnp.where(left, expo, 0.0), jnp.where(left, 0.0, expo)], axis=0
            ).astype(BF16)
            weighed.append((i, nn(values, split), jnp.where(row == 0, peak, denom)))
        for i, sums, stats in weighed:
            sums_ref[i], stats_ref[i] = sums, stats
        return 0

    lax.fori_loop(0, SLOTS // 2, some, 0)


def parts(own, messages, kv, kv_mate, after):
    count = len(messages)
    total = count * SLOTS
    whole = pl.BlockSpec(memory_space=VMEM)
    scalars = pl.BlockSpec(memory_space=pltpu.SMEM)
    return pl.pallas_call(
        functools.partial(find_parts, count),
        in_specs=[scalars] + [whole] * (count + 2) + [pl.BlockSpec(memory_space=pl.ANY)],
        out_specs=[whole, whole, scalars],
        out_shape=[
            jax.ShapeDtypeStruct((total, 128, 128), F32),
            jax.ShapeDtypeStruct((total, 8, 128), F32),
            jax.ShapeDtypeStruct((total,), jnp.int32),
        ],
        compiler_params=params(12),
        cost_estimate=cost(count * 400 * MIB, count * 500 * 1024),
        name="parts",
    )(own, *messages, kv, kv_mate, after)


def split3(x):
    high = x.astype(BF16)
    rest = x - high.astype(F32)
    mid = rest.astype(BF16)
    low = (rest - mid.astype(F32)).astype(BF16)
    return high.astype(F32), mid.astype(F32), low.astype(F32)


def begin(out_ref):
    pad = lax.broadcasted_iota(jnp.int32, (8, 128), 0)
    none = jnp.where(pad == 0, NONE, 0.0).astype(BF16)
    for b in range(out_ref.shape[0]):
        out_ref[b, 0:128, :] = jnp.zeros((128, 128), BF16)
        out_ref[b, 128:136, :] = none


def merge_into(first, codes_ref, sums_ref, stats_ref, out_ref):
    for r in range(SLOTS):
        code = codes_ref[first + r]

        @pl.when(code > 0)
        def _():
            b = (code - 1) >> 5
            peak, denom = stats_ref[first + r, 0:1, :], stats_ref[first + r, 1:2, :]
            stats = out_ref[b, 128:136, :].astype(F32)
            m_old = stats[0:1] + stats[1:2] + stats[2:3]
            l_old = stats[3:4] + stats[4:5] + stats[5:6]
            m_new = jnp.maximum(m_old, peak)
            keep = jnp.exp(m_old - m_new)
            gain = jnp.exp(peak - m_new)
            l_new = l_old * keep + denom * gain
            zero = jnp.zeros((2, 128), F32)
            fresh = jnp.concatenate(split3(m_new) + split3(l_new) + (zero,), axis=0)
            out_ref[b, 128:136, :] = fresh.astype(BF16)
            mixed = out_ref[b, 0:128, :].astype(F32) * keep + sums_ref[first + r] * gain
            out_ref[b, 0:128, :] = mixed.astype(BF16)


def merge_body(first, start, own_ref, codes_ref, sums_ref, stats_ref, after_ref, *refs):
    out_ref = refs[-1]
    if start == "all":
        begin(out_ref)
    elif start == "core_0":
        pl.when(own_ref[1] == 0)(lambda: begin(out_ref))
    merge_into(first, codes_ref, sums_ref, stats_ref, out_ref)


def far_body(own_ref, q_ref, kv_ref, mate_ref, after_ref, out_ref, sums_ref, stats_ref, codes_ref):
    @pl.when(own_ref[1] != 0)
    def _():
        find_parts(1, own_ref, q_ref, kv_ref, mate_ref, after_ref, sums_ref, stats_ref, codes_ref)
        begin(out_ref)
        merge_into(0, codes_ref, sums_ref, stats_ref, out_ref)


def far_message(own, q, kv, kv_mate, blocks, after):
    whole = pl.BlockSpec(memory_space=VMEM)
    return pl.pallas_call(
        far_body,
        in_specs=[pl.BlockSpec(memory_space=pltpu.SMEM), whole, whole, whole]
        + [pl.BlockSpec(memory_space=pl.ANY)],
        out_specs=whole,
        out_shape=jax.ShapeDtypeStruct((blocks, 136, 128), BF16),
        scratch_shapes=[
            VMEM((SLOTS, 128, 128), F32),
            VMEM((SLOTS, 8, 128), F32),
            pltpu.SMEM((SLOTS,), jnp.int32),
        ],
        compiler_params=params(10),
        cost_estimate=cost(500 * MIB, 500 * 1024),
        name="far",
    )(own, q, kv, kv_mate, after)


def merge(own, part, blocks, after, msg=None, start="none"):
    (sums, stats, codes), n = part
    whole = pl.BlockSpec(memory_space=VMEM)
    scalars = pl.BlockSpec(memory_space=pltpu.SMEM)
    more = () if msg is None else (msg,)
    return pl.pallas_call(
        functools.partial(merge_body, n * SLOTS, start),
        in_specs=[scalars, scalars, whole, whole, pl.BlockSpec(memory_space=pl.ANY)]
        + [whole] * len(more),
        out_specs=whole,
        out_shape=jax.ShapeDtypeStruct((blocks, 136, 128), BF16),
        input_output_aliases={5: 0} if more else {},
        compiler_params=params(8),
        cost_estimate=cost(100 * MIB, 900 * 1024),
        name="merge",
    )(own, codes, sums, stats, after, *more)


def finish_body(count, lg_ref, *refs):
    messages, normed, out_ref = refs[:count], refs[count:-1], refs[-1]
    for b in range(messages[0].shape[0]):
        peaks, denoms = [], []
        for message in messages:
            s = message[b, 128:136, :].astype(F32)
            peaks.append(s[0:1] + s[1:2] + s[2:3])
            denoms.append(s[3:4] + s[4:5] + s[5:6])
        peak = functools.reduce(jnp.maximum, peaks)
        gains = [jnp.exp(p - peak) for p in peaks]
        denom = sum(d * g for d, g in zip(denoms, gains))
        sums = sum(m[b, 0:128, :].astype(F32) * g for m, g in zip(messages, gains))
        retrieved = (sums / denom).T
        lg = lg_ref[b * BLOCK : (b + 1) * BLOCK, :]
        gate = jax.nn.sigmoid(jnp.concatenate([lg[:, 4:5], lg[:, 5:6]], axis=0))
        mixed = (normed[b][0] + gate * retrieved).astype(BF16)
        for h in range(2):
            out_ref[b * BLOCK : (b + 1) * BLOCK, h * 128 : (h + 1) * 128] = mixed[
                h * BLOCK : (h + 1) * BLOCK
            ]


def finish(messages, logits, normed):
    rows = logits.shape[0]
    return pl.pallas_call(
        functools.partial(finish_body, len(messages)),
        out_shape=jax.ShapeDtypeStruct((rows, 256), BF16),
        compiler_params=params(16),
        cost_estimate=cost(100 * MIB, 2 * MIB),
        name="finish",
    )(logits, *messages, *normed)


def per_device(
    tokens,
    owners,
    entries,
    store,
    mixer_query_weight,
    mixer_key_weight,
    mixer_value_weight,
    strength_weight,
    decay_weight,
    head_decay_rate,
    extra_forgetting_exponent,
    output_norm_gain,
    retrieval_query_weight,
    passage_key_weight,
    passage_value_weight,
    retrieval_gate_weight,
):
    devices = lax.axis_size("st")
    me = lax.axis_index("st")
    core = lax.rem(me, 2)
    reach = devices // 4
    blocks = owners.shape[0]

    step = [2 if i % 2 == 0 else -2 for i in range(devices)]

    def hops(lane, end):
        ring = [(i, (i + step[i]) % devices) for i in range(devices)]
        return [(i ^ 1, j) for i, j in ring] if lane == "other" and end else ring

    def send(x, pairs):
        return lax.ppermute(x, "st", pairs)

    def second(pairs):
        return [(i, j) for i, j in pairs if i % 2 == 1]

    def reverse(pairs):
        return [(j, i) for i, j in pairs]

    query = query_message(tokens, retrieval_query_weight, owners.T, entries.T)
    own = {0: query}
    other = {}
    gain = output_norm_gain.reshape(1, 128)
    extra = extra_forgetting_exponent.T
    where_own = jnp.stack([me >> 1, me & 1])
    part = {}

    def compute_parts(names, after):
        messages = [(own if lane == "own" else other)[h] for lane, h in names]
        result = parts(where_own, messages, kv_own, kv_mate, after)
        for n, name in enumerate(names):
            part[name] = (result, n)
        return result[1]

    lanes = {"own": own, "other": other}

    def pairs(name, h):
        hop = hops(name, h == 1)
        return second(hop) if h == reach else hop

    for h in range(1, reach + 1):
        for name, lane in lanes.items():
            lane[h] = send(lane[h - 1] if h > 1 else query, pairs(name, h))
        if h == 1:
            kv_own = project_passages(store, passage_key_weight, passage_value_weight, query)
            kv_mate = send(kv_own, [(i, i ^ 1) for i in range(devices)])
    qkv, logits = mixer_inputs(
        tokens,
        mixer_query_weight,
        mixer_key_weight,
        mixer_value_weight,
        strength_weight.T,
        decay_weight.T,
        retrieval_gate_weight.T,
        other[1],
    )
    last = compute_parts([("own", 0)], logits)
    for h in range(1, reach):
        last = compute_parts([("own", h), ("other", h)], last)

    normed = []
    state = jnp.zeros((2, 128, 128), F32)

    def mixer_step(after):
        nonlocal state
        result, state = mixer(
            qkv, logits, extra, head_decay_rate, gain, state, after, len(normed), 1
        )
        normed.append(result)
        return state

    came = {}
    for h in range(reach, 0, -1):
        for name, lane in lanes.items():
            if h == reach:
                last = far_message(where_own, lane[h], kv_own, kv_mate, blocks, last)
            else:
                start = "core_0" if h == reach - 1 else "none"
                last = merge(where_own, part[(name, h)], blocks, last, came[name], start)
            came[name] = send(last, reverse(pairs(name, h)))
        if len(normed) < blocks:
            last = mixer_step(last)
    while len(normed) < blocks:
        last = mixer_step(last)
    came["own"] = merge(where_own, part[("own", 0)], blocks, last, came["own"])
    return finish((came["own"], came["other"]), logits, normed)


def solution(mesh):
    return jax.shard_map(
        per_device,
        mesh=mesh,
        in_specs=(
            P(("grp", "st"), None),
            P(("grp", "st"), None),
            P(("grp", "st"), None),
            P(("grp", "st"), None, None),
            P(None, "tp"),
            P(None, "tp"),
            P(None, "tp"),
            P(None, "tp"),
            P(None, "tp"),
            P("tp"),
            P(("grp", "st"), "tp"),
            P(),
            P(None, "tp"),
            P(None, "tp"),
            P(None, "tp"),
            P(None, "tp"),
        ),
        out_specs=P(("grp", "st"), "tp"),
        check_vma=False,
    )
```

```python
import functools

import jax
import jax.numpy as jnp
from jax import lax
from jax.experimental import pallas as pl
from jax.experimental.pallas import tpu as pltpu
from jax.sharding import PartitionSpec as P


BLOCK = 64
SLOTS = 4
EPS = 1e-06
NONE = -1e30
MIB = 1024 * 1024
BIG = 52
F32 = jnp.float32
BF16 = jnp.bfloat16
VMEM = pltpu.VMEM


def nt(left, right):
    return lax.dot_general(left, right, (((1,), (1,)), ((), ())), preferred_element_type=F32)


def nn(left, right):
    return jnp.dot(left, right, preferred_element_type=F32)


def tn(left, right):
    return lax.dot_general(left, right, (((0,), (0,)), ((), ())), preferred_element_type=F32)


def params(limit, **more):
    return pltpu.CompilerParams(vmem_limit_bytes=limit * MIB, **more)


def cost(flops, size, trans=0):
    return pl.CostEstimate(flops=flops, bytes_accessed=size, transcendentals=trans)


def pieces(src, dst, sems, first, count):
    rows = dst.shape[0] // count
    return [
        pltpu.make_async_copy(
            src.at[pl.ds(i * rows, rows)], dst.at[pl.ds(i * rows, rows)], sems.at[first + i]
        )
        for i in range(count)
    ]


def query_body(x_hbm, w_hbm, owners_hbm, entries_hbm, out_ref, x_buf, w_buf, owners_ref, entries_ref, sems):
    tiles, rows, _ = x_buf.shape
    loads = pieces(w_hbm, w_buf, sems, 0, 4)
    x_loads = [
        pieces(x_hbm.at[pl.ds(i * rows, rows)], x_buf.at[i], sems, 4 + i * 4, 4)
        for i in range(tiles)
    ]
    tables = [
        pltpu.make_async_copy(owners_hbm, owners_ref, sems.at[tiles * 4 + 4]),
        pltpu.make_async_copy(entries_hbm, entries_ref, sems.at[tiles * 4 + 5]),
    ]
    for copies in [loads] + x_loads + [tables]:
        for copy in copies:
            copy.start()
    per, count = owners_ref.shape
    blocks = tiles * rows // BLOCK
    for table in tables:
        table.wait()
    names = jnp.concatenate([owners_ref[...] + 1, entries_ref[...]], axis=0).astype(F32)
    out_ref[blocks * 128 :, :] = jnp.zeros((2 * per, 128), BF16)
    out_ref[blocks * 128 :, 0:count] = names.astype(BF16)
    for copy in loads:
        copy.wait()
    for i in range(tiles):
        for copy in x_loads[i]:
            copy.wait()
        q = nn(x_buf[i], w_buf[...]).astype(BF16)
        for n in range(rows // BLOCK):
            at = (i * rows // BLOCK + n) * 128
            for h in range(2):
                out_ref[at + h * BLOCK : at + (h + 1) * BLOCK, :] = q[
                    n * BLOCK : (n + 1) * BLOCK, h * 128 : (h + 1) * 128
                ]


def query_message(x, w, owners, entries, tiles=2):
    rows, depth = x.shape
    hbm = pl.BlockSpec(memory_space=pltpu.HBM)
    whole = pl.BlockSpec(memory_space=VMEM)
    return pl.pallas_call(
        query_body,
        in_specs=[hbm] * 4,
        out_specs=whole,
        out_shape=jax.ShapeDtypeStruct((rows * 2 + 8, 128), BF16),
        scratch_shapes=[
            VMEM((tiles, rows // tiles, depth), BF16),
            VMEM(w.shape, BF16),
            VMEM(owners.shape, jnp.int32),
            VMEM(entries.shape, jnp.int32),
            pltpu.SemaphoreType.DMA((tiles * 4 + 6,)),
        ],
        compiler_params=params(BIG + 1),
        cost_estimate=cost(2 * rows * depth * 256, 2 * (rows * depth + depth * 256)),
        name="query",
    )(x, w, owners, entries)


def mixed_body(
    x_hbm, wq_hbm, wk_hbm, wv_hbm, ga_ref, gb_ref, gc_ref, after_ref, out_ref, lg_ref, x_buf, w_buf, sems
):
    tiles, tall, depth = x_buf.shape

    x_loads = [
        pieces(x_hbm.at[pl.ds(t * tall, tall)], x_buf.at[t], sems, t * 4, 4) for t in range(tiles)
    ]
    w_loads = [
        pieces(w, w_buf.at[i], sems, (tiles + i) * 4, 4)
        for i, w in enumerate((wq_hbm, wk_hbm, wv_hbm))
    ]
    for copies in x_loads + w_loads:
        for copy in copies:
            copy.start()
    none = jnp.zeros((2, depth), BF16)
    gates = jnp.concatenate([ga_ref[...], gb_ref[...], gc_ref[...], none], axis=0)
    for t in range(tiles):
        for copy in x_loads[t]:
            copy.wait()
        lg_ref[t * tall : (t + 1) * tall, :] = nt(x_buf[t], gates)
    for copy in w_loads[0]:
        copy.wait()

    def piece(step, _):
        i, t = step // tiles, step % tiles
        rows = nn(x_buf[t], w_buf[i]).astype(BF16)
        for n in range(tall // BLOCK):
            for h in range(2):
                out_ref[i, t * (tall // BLOCK) + n, h * BLOCK : (h + 1) * BLOCK, :] = rows[
                    n * BLOCK : (n + 1) * BLOCK, h * 128 : (h + 1) * 128
                ]
        return 0

    lax.fori_loop(0, tiles, piece, 0)
    for copy in w_loads[1] + w_loads[2]:
        copy.wait()
    lax.fori_loop(tiles, 3 * tiles, piece, 0)


def mixer_inputs(x, wq, wk, wv, ga, gb, gc, after, tiles=2):
    rows, depth = x.shape
    hbm = pl.BlockSpec(memory_space=pltpu.HBM)
    whole = pl.BlockSpec(memory_space=VMEM)
    return pl.pallas_call(
        mixed_body,
        in_specs=[hbm] * 4 + [whole] * 3 + [pl.BlockSpec(memory_space=pl.ANY)],
        out_specs=[whole] * 2,
        out_shape=[
            jax.ShapeDtypeStruct((3, rows // BLOCK, 128, 128), BF16),
            jax.ShapeDtypeStruct((rows, 8), F32),
        ],
        scratch_shapes=[
            VMEM((tiles, rows // tiles, depth), BF16),
            VMEM((3,) + wq.shape, BF16),
            pltpu.SemaphoreType.DMA((tiles * 4 + 12,)),
        ],
        compiler_params=params(BIG),
        cost_estimate=cost(2 * rows * depth * 768, 2 * (rows * depth + depth * 768)),
        name="mixer_inputs",
    )(x, wq, wk, wv, ga, gb, gc, after)


def passages_body(store_hbm, wk_hbm, wv_hbm, after_ref, out_ref, x_buf, w_buf, sems):
    chunks, tall, _ = x_buf.shape
    rows = out_ref.shape[1] // 4
    count = tall // rows

    def load(i):
        return pieces(store_hbm.at[pl.ds(i * tall, tall)], x_buf.at[i], sems, i * 4, 4)

    weights = pieces(wk_hbm, w_buf.at[0], sems, chunks * 4, 4)
    weights += pieces(wv_hbm, w_buf.at[1], sems, chunks * 4 + 4, 4)
    for copy in load(0) + weights:
        copy.start()
    for i in range(1, chunks):
        for copy in load(i):
            copy.start()
    for copy in weights:
        copy.wait()

    def chunk(i, _):
        for copy in load(i):
            copy.wait()
        keys = nn(x_buf[i], w_buf[0]).astype(BF16)
        values = nn(x_buf[i], w_buf[1]).astype(BF16).astype(F32)
        for p in range(count):
            span = slice(p * rows, (p + 1) * rows)
            at = i * count + p
            for h in range(2):
                out_ref[at, h * rows : (h + 1) * rows, :] = keys[span, h * 128 : (h + 1) * 128]
            stacked = jnp.concatenate([values[span, :128], values[span, 128:]], axis=0)
            out_ref[at, 128:256, :] = stacked.T.astype(BF16)
        return 0

    lax.fori_loop(0, chunks, chunk, 0)


def project_passages(store, wk, wv, after, chunks=4):
    number, rows, depth = store.shape
    hbm = pl.BlockSpec(memory_space=pltpu.HBM)
    return pl.pallas_call(
        passages_body,
        in_specs=[hbm, hbm, hbm, pl.BlockSpec(memory_space=pl.ANY)],
        out_specs=pl.BlockSpec(memory_space=VMEM),
        out_shape=jax.ShapeDtypeStruct((number, 256, 128), BF16),
        scratch_shapes=[
            VMEM((chunks, number * rows // chunks, depth), BF16),
            VMEM((2,) + wk.shape, BF16),
            pltpu.SemaphoreType.DMA((chunks * 4 + 8,)),
        ],
        compiler_params=params(BIG),
        cost_estimate=cost(2 * number * rows * depth * 512, 2 * number * rows * depth),
        name="passages",
    )(store.reshape(number * rows, depth), wk, wv, after)


def mixer_body(
    first, qkv_ref, lg_ref, ex_ref, rate_ref, gain_ref, s_ref, after_ref, out_ref, s_out_ref
):
    ri = lax.broadcasted_iota(jnp.int32, (128, 128), 0)
    ci = lax.broadcasted_iota(jnp.int32, (128, 128), 1)
    same = (ri >= BLOCK) == (ci >= BLOCK)
    lower = same & (ri >= ci)
    strict = same & (ri > ci)
    upper = same & (ri <= ci)
    diag = ri == ci
    top = lax.broadcasted_iota(jnp.int32, (128, 1), 0) < BLOCK
    rate = jnp.where(top, rate_ref[0], rate_ref[1])
    pieces = []
    for n in range(qkv_ref.shape[1]):
        lg = lg_ref[n * BLOCK : (n + 1) * BLOCK, :]
        at = (first + n) * BLOCK
        ex = jnp.concatenate([ex_ref[0:1, at : at + BLOCK], ex_ref[1:2, at : at + BLOCK]], axis=1)
        beta = jax.nn.sigmoid(jnp.concatenate([lg[:, 0:1], lg[:, 1:2]], axis=0))
        pre = jnp.concatenate([lg[:, 2:3], lg[:, 3:4]], axis=0)
        extra = jnp.sum(jnp.where(diag, ex, 0.0), axis=1, keepdims=True)
        soft = jnp.maximum(pre, 0.0) + jnp.log1p(jnp.exp(-jnp.abs(pre)))
        g = extra - rate * soft
        g_row = jnp.sum(jnp.where(diag, g, 0.0), axis=0, keepdims=True)
        c = jnp.sum(jnp.where(lower, g_row, 0.0), axis=1, keepdims=True)
        total = jnp.sum(jnp.where(same, g_row, 0.0), axis=1, keepdims=True)
        c_row = jnp.sum(jnp.where(upper, g, 0.0), axis=0, keepdims=True)
        damping = jnp.where(lower, jnp.exp(jnp.where(lower, c - c_row, 0.0)), 0.0)
        q = qkv_ref[0, n].astype(F32)
        k = qkv_ref[1, n].astype(F32)
        v = qkv_ref[2, n].astype(F32)
        q = q * (lax.rsqrt(jnp.sum(q * q, axis=1, keepdims=True) + EPS) * 128**-0.5)
        k = k * lax.rsqrt(jnp.sum(k * k, axis=1, keepdims=True) + EPS)
        kb = k * beta
        decay = jnp.exp(c)
        k16 = k.astype(BF16)
        power = jnp.where(strict, nt(kb.astype(BF16), k16) * damping, 0.0)
        within = (nt(q.astype(BF16), k16) * damping).astype(BF16)
        inverse = jnp.where(diag, 1.0, 0.0) - power
        p16 = power.astype(BF16)

        for _ in range(5):
            p16 = nn(p16, p16).astype(BF16)
            inverse = inverse + nn(inverse.astype(BF16), p16)
        inv16 = inverse.astype(BF16)
        mix = nn(inv16, (kb * decay).astype(BF16)).astype(BF16)
        base = nn(inv16, (v * beta).astype(BF16))
        q_dec = (q * decay).astype(BF16)
        k_tail = (k * jnp.exp(total - c)).astype(BF16)
        pieces.append((mix, base, within, q_dec, k_tail, jnp.exp(total)))
    state = [s_ref[0], s_ref[1]]
    for n, (mix, base, within, q_dec, k_tail, keep) in enumerate(pieces):
        fresh, far = [], []
        for h in range(2):
            rows = slice(h * BLOCK, (h + 1) * BLOCK)
            both = nn(jnp.concatenate([mix[rows], q_dec[rows]], axis=0), state[h].astype(BF16))
            fresh.append(base[rows] - both[:BLOCK])
            far.append(both[BLOCK:])
        f16 = jnp.concatenate(fresh, axis=0).astype(BF16)
        recur = jnp.concatenate(far, axis=0) + nn(within, f16)
        for h in range(2):
            rows = slice(h * BLOCK, (h + 1) * BLOCK)
            state[h] = state[h] * keep[h * BLOCK : h * BLOCK + 1] + tn(k_tail[rows], f16[rows])
        scale = lax.rsqrt(jnp.mean(recur * recur, axis=1, keepdims=True) + EPS)
        out_ref[n] = recur * scale * gain_ref[...]
    s_out_ref[0] = state[0]
    s_out_ref[1] = state[1]


def mixer(qkv, logits, extra, rate, gain, state, after, first, number):
    at = first // number
    return pl.pallas_call(
        functools.partial(mixer_body, first),
        grid=(1,),
        in_specs=[
            pl.BlockSpec((3, number, 128, 128), lambda i: (0, at, 0, 0)),
            pl.BlockSpec((number * BLOCK, logits.shape[1]), lambda i: (at, 0)),
            pl.BlockSpec(extra.shape, lambda i: (0, 0)),
            pl.BlockSpec(memory_space=pltpu.SMEM),
            pl.BlockSpec((1, 128), lambda i: (0, 0)),
            pl.BlockSpec((2, 128, 128), lambda i: (0, 0, 0)),
            pl.BlockSpec(memory_space=pl.ANY),
        ],
        out_specs=[
            pl.BlockSpec((number, 128, 128), lambda i: (0, 0, 0)),
            pl.BlockSpec((2, 128, 128), lambda i: (0, 0, 0)),
        ],
        out_shape=[
            jax.ShapeDtypeStruct((number, 128, 128), F32),
            jax.ShapeDtypeStruct((2, 128, 128), F32),
        ],
        compiler_params=params(16),
        cost_estimate=cost(number * 1000 * MIB // 2, number * 300 * 1024),
        name="mixer",
    )(qkv, logits, extra, rate, gain, state, after)


def find_parts(count, own_ref, *refs):
    messages, refs = refs[:count], refs[count:]
    (kv_ref, mate_ref, _, sums_ref, stats_ref, codes_ref) = refs
    chip, core = own_ref[0], own_ref[1]
    rows = messages[0].shape[0]
    row = lax.broadcasted_iota(jnp.int32, (8, 128), 0)
    lane = lax.broadcasted_iota(jnp.int32, (8, 128), 1)
    before = (
        lax.broadcasted_iota(jnp.int32, (128, 128), 0) < lax.broadcasted_iota(jnp.int32, (128, 128), 1)
    )
    before = jnp.where(before, 1.0, 0.0).astype(BF16)
    blocks = (rows - 8) // 128
    left = lax.broadcasted_iota(jnp.int32, (BLOCK, 128), 1) < BLOCK
    spots = []
    for n in range(count):
        table = messages[n][rows - 8 :, :].astype(F32)
        entry = jnp.concatenate([table[4:8], table[4:8]], axis=0)
        name = table.astype(jnp.int32) - 1
        hit = ((name >> 1) == chip) & (row < 4) & (lane < blocks)
        ones = jnp.where(hit, 1.0, 0.0)
        rank = nn(ones.astype(BF16), before)
        sums = jnp.sum(ones, axis=1, keepdims=True)
        first, second, third = sums[0:1], sums[1:2], sums[2:3]
        rank = rank + jnp.where(row > 0, first, 0.0)
        rank = rank + jnp.where(row > 1, second, 0.0)
        rank = rank + jnp.where(row > 2, third, 0.0)
        far = jnp.where((name & 1) == core, 0.0, 16.0)
        code = lane.astype(F32) * 32.0 + far + entry + 1.0
        for r in range(SLOTS):
            value = jnp.where(hit & (rank == float(r)), code, 0.0)
            spots.append(jnp.sum(value).astype(jnp.int32))
    for i, spot in enumerate(spots):
        codes_ref[i] = spot

    def some(step, _):
        found = []
        for n in range(count):
            for r in range(2):
                i = n * SLOTS + step * 2 + r
                spot = jnp.maximum(codes_ref[i] - 1, 0)
                at = pl.multiple_of((spot >> 5) * 128, 128)
                q = messages[n][pl.ds(at, 128), :]
                kv = jnp.where((spot & 16) != 0, mate_ref[spot & 15], kv_ref[spot & 15])
                both = nt(kv[0:128], q)
                scores = jnp.where(left, both[:BLOCK], both[BLOCK:]) * 128**-0.5
                found.append((i, scores, kv[128:256]))
        weighed = []
        for i, scores, values in found:
            peak = jnp.max(scores, axis=0, keepdims=True)
            expo = jnp.exp(scores - peak)
            denom = jnp.sum(expo, axis=0, keepdims=True)
            split = jnp.concatenate(
                [jnp.where(left, expo, 0.0), jnp.where(left, 0.0, expo)], axis=0
            ).astype(BF16)
            stats = jnp.where(row == 0, peak, denom)
            stats = jnp.where(row == 2, codes_ref[i].astype(F32), stats)
            weighed.append((i, nn(values, split), stats))
        for i, sums, stats in weighed:
            sums_ref[i], stats_ref[i] = sums, stats
        return 0

    lax.fori_loop(0, SLOTS // 2, some, 0)


def parts(own, messages, kv, kv_mate, after):
    count = len(messages)
    total = count * SLOTS
    whole = pl.BlockSpec(memory_space=VMEM)
    scalars = pl.BlockSpec(memory_space=pltpu.SMEM)
    return pl.pallas_call(
        functools.partial(find_parts, count),
        in_specs=[scalars] + [whole] * (count + 2) + [pl.BlockSpec(memory_space=pl.ANY)],
        out_specs=[whole, whole],
        out_shape=[
            jax.ShapeDtypeStruct((total, 128, 128), F32),
            jax.ShapeDtypeStruct((total, 8, 128), F32),
        ],
        scratch_shapes=[pltpu.SMEM((total,), jnp.int32)],
        compiler_params=params(12),
        cost_estimate=cost(count * 400 * MIB, count * 500 * 1024),
        name="parts",
    )(own, *messages, kv, kv_mate, after)


def split3(x):
    high = x.astype(BF16)
    rest = x - high.astype(F32)
    mid = rest.astype(BF16)
    low = (rest - mid.astype(F32)).astype(BF16)
    return high.astype(F32), mid.astype(F32), low.astype(F32)


def begin(out_ref):
    pad = lax.broadcasted_iota(jnp.int32, (8, 128), 0)
    none = jnp.where(pad == 0, NONE, 0.0).astype(BF16)
    for b in range(out_ref.shape[0]):
        out_ref[b, 0:128, :] = jnp.zeros((128, 128), BF16)
        out_ref[b, 128:136, :] = none


def merge_into(first, sums_ref, stats_ref, out_ref, codes_ref):
    for r in range(SLOTS):
        codes_ref[r] = jnp.max(stats_ref[first + r, 2:3, :]).astype(jnp.int32)

    def one(slot, _):
        r = first + slot
        code = codes_ref[slot]

        @pl.when(code > 0)
        def _():
            b = (code - 1) >> 5
            peak, denom = stats_ref[r, 0:1, :], stats_ref[r, 1:2, :]
            stats = out_ref[b, 128:136, :].astype(F32)
            m_old = stats[0:1] + stats[1:2] + stats[2:3]
            l_old = stats[3:4] + stats[4:5] + stats[5:6]
            m_new = jnp.maximum(m_old, peak)
            keep = jnp.exp(m_old - m_new)
            gain = jnp.exp(peak - m_new)
            l_new = l_old * keep + denom * gain
            zero = jnp.zeros((2, 128), F32)
            fresh = jnp.concatenate(split3(m_new) + split3(l_new) + (zero,), axis=0)
            out_ref[b, 128:136, :] = fresh.astype(BF16)
            mixed = out_ref[b, 0:128, :].astype(F32) * keep + sums_ref[r] * gain
            out_ref[b, 0:128, :] = mixed.astype(BF16)

        return 0

    lax.fori_loop(0, SLOTS, one, 0)


def merge_body(first, start, sums_ref, stats_ref, after_ref, *refs):
    out_ref, codes_ref = refs[-2:]
    if start:
        own_ref = refs[-3]
        pl.when(own_ref[1] == 0)(lambda: begin(out_ref))
    merge_into(first, sums_ref, stats_ref, out_ref, codes_ref)


def far_body(own_ref, q_ref, kv_ref, mate_ref, after_ref, out_ref, sums_ref, stats_ref, codes_ref):
    @pl.when(own_ref[1] != 0)
    def _():
        find_parts(1, own_ref, q_ref, kv_ref, mate_ref, after_ref, sums_ref, stats_ref, codes_ref)
        begin(out_ref)
        merge_into(0, sums_ref, stats_ref, out_ref, codes_ref)


def far_message(own, q, kv, kv_mate, blocks, after):
    whole = pl.BlockSpec(memory_space=VMEM)
    return pl.pallas_call(
        far_body,
        in_specs=[pl.BlockSpec(memory_space=pltpu.SMEM), whole, whole, whole]
        + [pl.BlockSpec(memory_space=pl.ANY)],
        out_specs=whole,
        out_shape=jax.ShapeDtypeStruct((blocks, 136, 128), BF16),
        scratch_shapes=[
            VMEM((SLOTS, 128, 128), F32),
            VMEM((SLOTS, 8, 128), F32),
            pltpu.SMEM((SLOTS,), jnp.int32),
        ],
        compiler_params=params(10),
        cost_estimate=cost(500 * MIB, 500 * 1024),
        name="far",
    )(own, q, kv, kv_mate, after)


def merge(part, blocks, after, msg, start=None):
    (sums, stats), n = part
    whole = pl.BlockSpec(memory_space=VMEM)
    more = () if start is None else (start,)
    return pl.pallas_call(
        functools.partial(merge_body, n * SLOTS, start is not None),
        in_specs=[whole, whole, pl.BlockSpec(memory_space=pl.ANY), whole]
        + [pl.BlockSpec(memory_space=pltpu.SMEM)] * len(more),
        out_specs=whole,
        out_shape=jax.ShapeDtypeStruct((blocks, 136, 128), BF16),
        input_output_aliases={3: 0},
        scratch_shapes=[pltpu.SMEM((SLOTS,), jnp.int32)],
        compiler_params=params(8),
        cost_estimate=cost(100 * MIB, 900 * 1024),
        name="merge",
    )(sums, stats, after, msg, *more)


def finish_body(count, lg_ref, *refs):
    messages, normed, out_ref = refs[:count], refs[count:-1], refs[-1]
    for b in range(messages[0].shape[0]):
        peaks, denoms = [], []
        for message in messages:
            s = message[b, 128:136, :].astype(F32)
            peaks.append(s[0:1] + s[1:2] + s[2:3])
            denoms.append(s[3:4] + s[4:5] + s[5:6])
        peak = functools.reduce(jnp.maximum, peaks)
        gains = [jnp.exp(p - peak) for p in peaks]
        denom = sum(d * g for d, g in zip(denoms, gains))
        sums = sum(m[b, 0:128, :].astype(F32) * g for m, g in zip(messages, gains))
        retrieved = (sums / denom).T
        lg = lg_ref[b * BLOCK : (b + 1) * BLOCK, :]
        gate = jax.nn.sigmoid(jnp.concatenate([lg[:, 4:5], lg[:, 5:6]], axis=0))
        mixed = (normed[b][0] + gate * retrieved).astype(BF16)
        for h in range(2):
            out_ref[b * BLOCK : (b + 1) * BLOCK, h * 128 : (h + 1) * 128] = mixed[
                h * BLOCK : (h + 1) * BLOCK
            ]


def finish(messages, logits, normed):
    rows = logits.shape[0]
    return pl.pallas_call(
        functools.partial(finish_body, len(messages)),
        out_shape=jax.ShapeDtypeStruct((rows, 256), BF16),
        compiler_params=params(16),
        cost_estimate=cost(100 * MIB, 2 * MIB),
        name="finish",
    )(logits, *messages, *normed)


def per_device(
    tokens,
    owners,
    entries,
    store,
    mixer_query_weight,
    mixer_key_weight,
    mixer_value_weight,
    strength_weight,
    decay_weight,
    head_decay_rate,
    extra_forgetting_exponent,
    output_norm_gain,
    retrieval_query_weight,
    passage_key_weight,
    passage_value_weight,
    retrieval_gate_weight,
):
    devices = lax.axis_size("st")
    me = lax.axis_index("st")
    core = lax.rem(me, 2)
    reach = devices // 4
    blocks = owners.shape[0]

    step = [2 if i % 2 == 0 else -2 for i in range(devices)]

    def hops(lane, end):
        ring = [(i, (i + step[i]) % devices) for i in range(devices)]
        return [(i ^ 1, j) for i, j in ring] if lane == "other" and end else ring

    def send(x, pairs):
        return lax.ppermute(x, "st", pairs)

    def second(pairs):
        return [(i, j) for i, j in pairs if i % 2 == 1]

    def reverse(pairs):
        return [(j, i) for i, j in pairs]

    query = query_message(tokens, retrieval_query_weight, owners.T, entries.T)
    own = {0: query}
    other = {}
    gain = output_norm_gain.reshape(1, 128)
    extra = extra_forgetting_exponent.T
    where_own = jnp.stack([me >> 1, me & 1])
    part = {}

    def compute_parts(names, after):
        messages = [(own if lane == "own" else other)[h] for lane, h in names]
        result = parts(where_own, messages, kv_own, kv_mate, after)
        for n, name in enumerate(names):
            part[name] = (result, n)
        return result[1]

    lanes = {"own": own, "other": other}

    def pairs(name, h):
        hop = hops(name, h == 1)
        return second(hop) if h == reach else hop

    for h in range(1, reach + 1):
        for name, lane in lanes.items():
            lane[h] = send(lane[h - 1] if h > 1 else query, pairs(name, h))
        if h == 1:
            kv_own = project_passages(store, passage_key_weight, passage_value_weight, query)
            kv_mate = send(kv_own, [(i, i ^ 1) for i in range(devices)])
    qkv, logits = mixer_inputs(
        tokens,
        mixer_query_weight,
        mixer_key_weight,
        mixer_value_weight,
        strength_weight.T,
        decay_weight.T,
        retrieval_gate_weight.T,
        other[1],
    )
    last = compute_parts([("own", 0)], logits)
    for h in range(1, reach):
        last = compute_parts([("own", h), ("other", h)], last)

    normed = []
    state = jnp.zeros((2, 128, 128), F32)

    def mixer_step(after):
        nonlocal state
        result, state = mixer(
            qkv, logits, extra, head_decay_rate, gain, state, after, len(normed), 1
        )
        normed.append(result)
        return state

    came = {}
    for h in range(reach, 0, -1):
        for name, lane in lanes.items():
            if h == reach:
                last = far_message(where_own, lane[h], kv_own, kv_mate, blocks, last)
            else:
                start = where_own if h == reach - 1 else None
                last = merge(part[(name, h)], blocks, last, came[name], start)
            came[name] = send(last, reverse(pairs(name, h)))
        if h < reach:
            last = mixer_step(last)
    while len(normed) < blocks:
        last = mixer_step(last)
    came["own"] = merge(part[("own", 0)], blocks, last, came["own"])
    return finish((came["own"], came["other"]), logits, normed)


def solution(mesh):
    return jax.shard_map(
        per_device,
        mesh=mesh,
        in_specs=(
            P(("grp", "st"), None),
            P(("grp", "st"), None),
            P(("grp", "st"), None),
            P(("grp", "st"), None, None),
            P(None, "tp"),
            P(None, "tp"),
            P(None, "tp"),
            P(None, "tp"),
            P(None, "tp"),
            P("tp"),
            P(("grp", "st"), "tp"),
            P(),
            P(None, "tp"),
            P(None, "tp"),
            P(None, "tp"),
            P(None, "tp"),
        ),
        out_specs=P(("grp", "st"), "tp"),
        check_vma=False,
    )
```
